512 devices in a mesh: sp: 64 (over z, y), tp: 8 (over x, core).
Axes of the slice: x: 4, y: 4, z: 16, core: 2. Of those that a mesh axis runs over, the one named last changes fastest.
Arguments:
- residual: bfloat16 [8192, 2048], P('sp'), may hold values from -6 to 6
- query_nope: bfloat16 [8192, 8, 128], P('sp', 'tp'), may hold values from -6 to 6
- query_rope: bfloat16 [8192, 8, 64], P('sp', 'tp'), may hold values from -64 to 64
- latent: bfloat16 [8192, 256], P('sp'), may hold values from -6 to 6
- rope_key: bfloat16 [8192, 64], P('sp'), may hold values from -64 to 64
- kv_gain: bfloat16 [256], replicated, may hold values from 0.099609375 to 1.8984375
- key_up: bfloat16 [256, 8, 128], replicated, may hold values from -0.375 to 0.375
- value_up: bfloat16 [256, 8, 128], replicated, may hold values from -0.375 to 0.375
- out_weight: bfloat16 [1024, 2048], P('tp'), may hold values from -0.1875 to 0.1875
- post_gain: bfloat16 [2048], replicated, may hold values from 0.099609375 to 1.8984375
- pre_gain: bfloat16 [2048], replicated, may hold values from 0.099609375 to 1.8984375
- ffn_gain: bfloat16 [2048], replicated, may hold values from 0.099609375 to 1.8984375
- up_value: bfloat16 [2048, 5632], P('sp', 'tp'), may hold values from -0.125 to 0.125
- up_gate: bfloat16 [2048, 5632], P('sp', 'tp'), may hold values from -0.125 to 0.125
- conv_value: bfloat16 [3, 5632], replicated, may hold values from -3.5 to 3.5
- conv_gate: bfloat16 [3, 5632], replicated, may hold values from -3.5 to 3.5
- down_weight: bfloat16 [5632, 2048], P('tp', 'sp'), may hold values from -0.078125 to 0.078125
Outputs:
- layer_out: bfloat16 [8192, 2048], P(('sp', 'tp'))
The draws below stay inside these ranges and needn't reach their ends.
All inputs are finite; a program needn't handle non-finite values.
Results may differ from the reference program's by a relative error of at most 0.02.
Values may be sent and summed in bfloat16 or wider, within the bound.
A program may use at most 128 MiB of HBM per device.

```python
import jax
import jax.numpy as jnp
from jax import lax

D = 2048
HEADS = 8
NOPE = 128
ROPE = 64
VD = 128
KV = 256
FF = 5632
GRID = 64
TOKENS = 8192
N_TP = 8


def drawn_pair(key):
    folded = jax.random.fold_in(key, 41)
    query_key, rope_seed = jax.random.split(folded, 2)
    queries = jax.random.normal(query_key, (TOKENS, HEADS, ROPE), jnp.float32)
    rope_keys = jax.random.normal(rope_seed, (TOKENS, ROPE), jnp.float32)
    return (jnp.clip(queries, -64.0, 64.0), jnp.clip(rope_keys, -64.0, 64.0))


def draw_query_rope(key, part):
    return drawn_pair(key)[0].astype(jnp.bfloat16)


def draw_rope_key(key, part):
    return drawn_pair(key)[1].astype(jnp.bfloat16)


def level_of(key, shape, cuts, smallest, top_value):
    loudness = 1.0
    for dim, parts in cuts:
        draws = jax.random.uniform(jax.random.fold_in(jax.random.fold_in(key, 6), dim), (parts,), jnp.float32, smallest / len(cuts), top_value / len(cuts))
        loudness = loudness * jnp.repeat(jnp.exp(draws), shape[dim] // parts).reshape((-1,) + (1,) * (len(shape) - 1 - dim))
    return loudness


def bell_draw(rng, dims, scale, most, cuts=(), held_as=jnp.bfloat16):
    entries = scale * jax.random.normal(rng, dims, jnp.float32)
    if cuts:
        entries = entries * level_of(rng, dims, cuts, -0.22, 0.18)
    return jnp.clip(entries, -most, most).astype(held_as)


def setup_inputs(seed: int = 0) -> dict:
    arg_keys = jax.random.split(jax.random.key(seed), 18)
    return {
        "residual": bell_draw(arg_keys[0], (TOKENS, D), 1.0, 6.0, ((0, 64),)),
        "query_nope": bell_draw(arg_keys[1], (TOKENS, HEADS, NOPE), 1.0, 6.0, ((0, 64), (1, 8))),
        "query_rope": draw_query_rope(jax.random.fold_in(arg_keys[17], 71), 0),
        "latent": bell_draw(arg_keys[3], (TOKENS, KV), 1.0, 6.0, ((0, 64),)),
        "rope_key": draw_rope_key(jax.random.fold_in(arg_keys[17], 71), 0),
        "kv_gain": jnp.clip(1.0 + 0.18 * jax.random.normal(arg_keys[5], (KV,), jnp.float32), 0.099609375, 1.8984375).astype(jnp.bfloat16),
        "key_up": bell_draw(arg_keys[6], (KV, HEADS, NOPE), KV ** -0.5, 0.375),
        "value_up": bell_draw(arg_keys[7], (KV, HEADS, VD), KV ** -0.5, 0.375),
        "out_weight": bell_draw(arg_keys[8], (HEADS * VD, D), (HEADS * VD) ** -0.5, 0.1875, ((0, 8),)),
        "post_gain": jnp.clip(1.0 + 0.18 * jax.random.normal(arg_keys[9], (D,), jnp.float32), 0.099609375, 1.8984375).astype(jnp.bfloat16),
        "pre_gain": jnp.clip(1.0 + 0.18 * jax.random.normal(arg_keys[10], (D,), jnp.float32), 0.099609375, 1.8984375).astype(jnp.bfloat16),
        "ffn_gain": jnp.clip(1.0 + 0.18 * jax.random.normal(arg_keys[11], (D,), jnp.float32), 0.099609375, 1.8984375).astype(jnp.bfloat16),
        "up_value": bell_draw(arg_keys[12], (D, FF), D ** -0.5, 0.125, ((0, 64), (1, 8))),
        "up_gate": bell_draw(arg_keys[13], (D, FF), D ** -0.5, 0.125, ((0, 64), (1, 8))),
        "conv_value": bell_draw(arg_keys[14], (3, FF), 3 ** -0.5, 3.5),
        "conv_gate": bell_draw(arg_keys[15], (3, FF), 3 ** -0.5, 3.5),
        "down_weight": bell_draw(arg_keys[16], (FF, D), FF ** -0.5, 0.078125, ((0, 8), (1, 64))),
    }


epsilon = 1e-06
rope_base = 10000.0

def rms_norm(values, gain):
    return values * lax.rsqrt(lax.optimization_barrier(jnp.mean(values * values, axis=-1, keepdims=True)) + epsilon) * gain.astype(jnp.float32)

def widened(values):
    return lax.optimization_barrier(values.astype(jnp.bfloat16)).astype(jnp.float32)

def rotate(values, positions):
    pair_count = values.shape[-1] // 4
    frequency = rope_base ** (-jnp.arange(pair_count, dtype=jnp.float32) / pair_count)
    grid_rows = (positions // GRID).astype(jnp.float32)
    grid_cols = (positions % GRID).astype(jnp.float32)
    angles = jnp.stack([grid_rows, grid_cols], axis=-1)[:, :, None] * frequency
    table_shape = (angles.shape[0],) + (1,) * (values.ndim - 2) + angles.shape[1:]
    cosine = jnp.cos(angles).reshape(table_shape)
    sine = jnp.sin(angles).reshape(table_shape)
    halves = values.reshape(values.shape[:-1] + (2, 2, pair_count))
    leading = halves[..., 0, :]
    trailing = halves[..., 1, :]
    turned = jnp.stack([leading * cosine - trailing * sine, trailing * cosine + leading * sine], axis=-2)
    return turned.reshape(values.shape)

def reference(residual, query_nope, query_rope, latent, rope_key, kv_gain, key_up, value_up, out_weight, post_gain, pre_gain, ffn_gain, up_value, up_gate, conv_value, conv_gate, down_weight):
    token_count = residual.shape[0]
    positions = jnp.arange(token_count, dtype=jnp.int32)
    score_scale = (NOPE + ROPE) ** (-0.5)
    normed_wide = widened(rms_norm(latent.astype(jnp.float32), kv_gain))
    keys_nope = widened(jnp.einsum('nc,chd->nhd', normed_wide, key_up.astype(jnp.float32)))
    values_all = widened(jnp.einsum('nc,chd->nhd', normed_wide, value_up.astype(jnp.float32)))
    key_turn = widened(rotate(rope_key.astype(jnp.float32), positions))
    query_turn = widened(rotate(query_rope.astype(jnp.float32), positions))
    keys_all = jnp.concatenate([keys_nope, jnp.broadcast_to(key_turn[:, None, :], (token_count, HEADS, ROPE))], axis=-1)
    queries = jnp.concatenate([query_nope.astype(jnp.float32), query_turn], axis=-1)
    block_size = min(512, token_count)
    query_blocks = queries.reshape(token_count // block_size, block_size, HEADS, NOPE + ROPE)

    def attend_block(query_block):
        scores = jnp.einsum('qhd,khd->hqk', query_block, keys_all) * score_scale
        row_max = lax.optimization_barrier(jnp.max(scores, axis=-1, keepdims=True))
        weights = jnp.exp(scores - row_max)
        totals = lax.optimization_barrier(jnp.sum(weights, axis=-1))
        mixed = jnp.einsum('hqk,khd->qhd', widened(weights), values_all)
        return (mixed / jnp.transpose(totals)[:, :, None]).astype(jnp.bfloat16)
    attended = lax.map(attend_block, query_blocks).reshape(token_count, HEADS * VD)
    group_width = HEADS * VD // N_TP

    def add_heads(running, group_id):
        block_rows = lax.dynamic_slice_in_dim(attended, group_id * group_width, group_width, 1)
        weight_rows = lax.dynamic_slice_in_dim(out_weight, group_id * group_width, group_width, 0)
        partial_value = jnp.dot(block_rows, weight_rows, preferred_element_type=jnp.float32)
        return (running + widened(partial_value), None)
    summed = lax.scan(add_heads, jnp.zeros((token_count, D), jnp.float32), jnp.arange(N_TP, dtype=jnp.int32))[0]
    stream_wide = widened(residual.astype(jnp.float32) + rms_norm(widened(summed), post_gain))
    inputs = rms_norm(stream_wide, pre_gain).astype(jnp.bfloat16)
    value_rows = widened(jnp.dot(inputs, up_value, preferred_element_type=jnp.float32))
    gate_rows = widened(jnp.dot(inputs, up_gate, preferred_element_type=jnp.float32))

    def convolve(rows_wide, conv_taps):
        padded = jnp.pad(rows_wide, ((1, 1), (0, 0)))
        return padded[:-2] * conv_taps[0] + padded[1:-1] * conv_taps[1] + padded[2:] * conv_taps[2]
    value_conv = convolve(value_rows, conv_value.astype(jnp.float32))
    gate_conv = convolve(gate_rows, conv_gate.astype(jnp.float32))
    hidden = (jax.nn.silu(gate_conv) * value_conv).astype(jnp.bfloat16)
    ff_width = FF // N_TP

    def add_units(running, group_id):
        block_rows = lax.dynamic_slice_in_dim(hidden, group_id * ff_width, ff_width, 1)
        weight_rows = lax.dynamic_slice_in_dim(down_weight, group_id * ff_width, ff_width, 0)
        partial_value = jnp.dot(block_rows, weight_rows, preferred_element_type=jnp.float32)
        return (running + widened(partial_value), None)
    projected = lax.scan(add_units, jnp.zeros((token_count, D), jnp.float32), jnp.arange(N_TP, dtype=jnp.int32))[0]
    return (stream_wide + rms_norm(widened(projected), ffn_gain)).astype(jnp.bfloat16)
```

```python
import functools

import jax
import jax.numpy as jnp
from jax import lax
from jax.experimental import pallas as pl
from jax.experimental.pallas import tpu as pltpu
from jax.sharding import Mesh
from jax.sharding import PartitionSpec as P

GRID = 64
AXES = ("z", "y", "x", "c")
SP = ("z", "y")
TP = ("x", "c")
MESH_IDS = pl.DeviceIdType.MESH
F32 = jnp.float32
BF16 = jnp.bfloat16

epsilon = 1e-06
rope_base = 10000.0

NZ, NY, NX, NC = 16, 4, 4, 2
NT = NX * NC
PLANE = NY * NT
D = 2048
ROWS = 128
SHARE = 16
KEYS = NZ * NY * SHARE
QW = 256
KW = 384
WL = 640
UP = 384
TOK = 256


def rms_norm(values, gain):
    return (
        values * lax.rsqrt(jnp.mean(values * values, axis=-1, keepdims=True) + epsilon) * gain
    )


def rotate(values, positions):
    pair_count = values.shape[-1] // 4
    frequency = rope_base ** (-jnp.arange(pair_count, dtype=F32) / pair_count)
    grid_rows = (positions // GRID).astype(F32)
    grid_cols = (positions % GRID).astype(F32)
    angles = jnp.stack([grid_rows, grid_cols], axis=-1)[:, :, None] * frequency
    cosine = jnp.cos(angles)
    sine = jnp.sin(angles)
    halves = values.reshape(values.shape[:-1] + (2, 2, pair_count))
    leading = halves[..., 0, :]
    trailing = halves[..., 1, :]
    turned = jnp.stack(
        [leading * cosine - trailing * sine, trailing * cosine + leading * sine], axis=-2
    )
    return turned.reshape(values.shape)


def dot_nn(a, b):
    return jnp.dot(a, b, preferred_element_type=F32)


def dot_nt(a, b):
    return lax.dot_general(a, b, (((1,), (1,)), ((), ())), preferred_element_type=F32)


def layer_kernel(
    scale,
    kv_loc,
    q_loc,
    w_loc,
    ow,
    key_up,
    value_up,
    resid,
    gains,
    taps,
    out,
    kvbuf,
    qbuf,
    wbuf,
    owbuf,
    kvt,
    s_scr,
    ot_scr,
    stats,
    o_send,
    o_recv,
    r_send,
    r_recv,
    in_send,
    inbuf,
    up,
    p_send,
    p_recv,
    stream,
    kvs_z,
    kvs_y,
    kvr,
    qs,
    qr,
    wys,
    wyr,
    wzs,
    wps,
    wzr,
    wpr,
    ows,
    owr,
    sts,
    str_,
    os_,
    or_,
    rss,
    rsr,
    ags,
    agr,
    hs,
    hr,
    ps,
    pr,
):
    z, y, x, c = (lax.axis_index(a) for a in AXES)
    tp = x * NC + c
    plane = y * NT + tp
    half = y // 2

    def zz(k):
        return (z + k + NZ) % NZ

    def push(src, dst, ss, rs, dev):
        return pltpu.make_async_remote_copy(
            src_ref=src, dst_ref=dst, send_sem=ss, recv_sem=rs, device_id=dev,
            device_id_type=MESH_IDS,
        )

    partner = (z, y, x, 1 - c)
    right, left = (zz(1), y, x, c), (zz(-1), y, x, c)
    right2, left2 = (zz(2), y, x, c), (zz(-2), y, x, c)
    cross = ((z + 2 * c - 1 + NZ) % NZ, y, x, 1 - c)

    def on_plane(j):
        p = (plane + j) % PLANE
        return (z, p // NT, (p // NC) % NX, p % NC)

    def tp_peer(t):
        return (z, y, t // NC, t % NC)

    barrier = pltpu.get_barrier_semaphore()
    for dev in (right, left, right2, left2, cross):
        pl.semaphore_signal(barrier, inc=1, device_id=dev, device_id_type=MESH_IDS)

    @pl.loop(1, PLANE)
    def _(j):
        pl.semaphore_signal(barrier, inc=1, device_id=on_plane(j), device_id_type=MESH_IDS)

    def kv_slot(yy, k):
        start = pl.multiple_of((yy * NZ + k) * SHARE, SHARE)
        return kvbuf.at[pl.ds(start, SHARE)]

    def w_slot(core, k):
        return wbuf.at[core, pl.ds(pl.multiple_of(k * ROWS, ROWS), ROWS)]

    def w_part(k, yy):
        return wbuf.at[c, pl.ds(pl.multiple_of(k * ROWS + yy * 32, 32), 32)]

    kv_slot(y, z)[...] = kv_loc[...]
    qbuf[tp] = q_loc[...]
    w_part(z, y)[...] = w_loc[y]
    owbuf[c] = ow[...]

    pl.semaphore_wait(barrier, 5 + PLANE - 1)

    pending = []

    def go(copy):
        copy.start()
        pending.append(copy)

    def kv_to(k, sem, dev):
        slot = kv_slot(y, k)
        go(push(slot, slot, kvs_z.at[sem], kvr.at[y * NZ + k], dev))

    def kv_to_y(k, sem):
        slot = kv_slot(y, k)
        for j in range(1, NY):
            dev = (z, (y + j) % NY, x, c)
            go(push(slot, slot, kvs_y.at[sem * 3 + j - 1], kvr.at[y * NZ + k], dev))

    kv_to(z, 0, right2)
    kv_to(z, 1, left2)
    kv_to(z, 2, right)
    kv_to(z, 3, left)
    kv_to_y(z, 0)
    for j in range(1, NY):
        yy = (y + j) % NY
        go(push(w_loc.at[yy], w_part(z, y), wys.at[j - 1], wyr.at[y], (z, yy, x, c)))
    for j in range(1, NT):
        t = (tp + j) % NT
        go(push(qbuf.at[tp], qbuf.at[tp], qs.at[j - 1], qr.at[tp], tp_peer(t)))
    go(push(owbuf.at[c], owbuf.at[c], ows.at[0], owr.at[0], partner))

    def w_send(k, step, to_right, to_left):
        slot = w_slot(c, k)
        if to_right:
            go(push(slot, slot, wzs.at[step], wzr.at[k], right))
        if to_left:
            go(push(slot, slot, wzs.at[8 + step], wzr.at[k], left))

    def w_across(k, sem):
        slot = w_slot(c, k)
        go(push(slot, slot, wps.at[sem], wpr.at[k], partner))

    def w_step(step):
        if step == 0:
            for j in range(1, NY):
                yy = (y + j) % NY
                part = w_part(z, yy)
                push(part, part, wys.at[j - 1], wyr.at[yy], (z, yy, x, c)).wait_recv()
            w_send(z, 0, True, True)
            w_across(z, 0)
            return
        k = zz(-step)
        slot = w_slot(c, k)
        push(slot, slot, wzs.at[0], wzr.at[k], left).wait_recv()
        w_send(k, step, step < 8, False)
        w_across(k, 2 * step - 1)
        if step < 8:
            k = zz(step)
            slot = w_slot(c, k)
            push(slot, slot, wzs.at[0], wzr.at[k], right).wait_recv()
            w_send(k, step, False, step < 7)
            w_across(k, 2 * step)

    def kv_wait(yy, k):
        slot = kv_slot(yy, k)
        push(slot, slot, kvs_z.at[0], kvr.at[yy * NZ + k], right).wait_recv()

    for d in range(1, 9):
        k = zz(-d)
        kv_wait(y, k)
        if d + 2 <= 8:
            kv_to(k, 3 + d, right2)
        if d < 8:
            k2 = zz(d)
            kv_wait(y, k2)
            if d + 2 <= 7:
                kv_to(k2, 9 + d, left2)
        kv_to_y(k, 2 * d - 1)
        if d < 8:
            kv_to_y(k2, 2 * d)
        if d == 3:
            w_step(0)
    for j in range(1, NY):
        yy = (y + j) % NY

        @pl.loop(0, NZ)
        def _(k):
            kv_wait(yy, k)

    w_step(1)
    for j in range(1, NT):
        t = (tp + j) % NT
        push(qbuf.at[t], qbuf.at[t], qs.at[0], qr.at[t], tp_peer(t)).wait_recv()

    kvt[...] = kvbuf[:, :256].T
    for hp in range(4):
        pair = []
        for h in (2 * hp, 2 * hp + 1):
            folded = dot_nt(qbuf[h, :, :128], key_up[:, h * 128 : (h + 1) * 128])
            pair.append(jnp.concatenate([folded.astype(BF16), qbuf[h, :, 128:]], axis=1))
        q = jnp.concatenate(pair, axis=0)
        s_scr[...] = dot_nt(kvbuf[...], q)
        top = jnp.max(s_scr[...], axis=0, keepdims=True)
        weights = jnp.exp((s_scr[...] - top) * scale)
        total = jnp.sum(weights, axis=0, keepdims=True)
        ot_scr[hp] = dot_nn(kvt[...], weights.astype(BF16))
        for i in range(2):
            h = 2 * hp + i
            stats[tp, h : h + 1] = top[:, i * 128 : (i + 1) * 128]
            stats[tp, 8 + h : 9 + h] = total[:, i * 128 : (i + 1) * 128]
        if hp == 2:
            w_step(2)

    for j in range(1, NT):
        t = (tp + j) % NT
        go(push(stats.at[tp], stats.at[tp], sts.at[j - 1], str_.at[tp], tp_peer(t)))
    for j in range(1, NT):
        t = (tp + j) % NT
        push(stats.at[t], stats.at[t], sts.at[0], str_.at[t], tp_peer(t)).wait_recv()
    top_all = stats[0, 0:8]
    for t in range(1, NT):
        top_all = jnp.maximum(top_all, stats[t, 0:8])
    total_all = jnp.zeros_like(top_all)
    for t in range(NT):
        total_all += jnp.exp((stats[t, 0:8] - top_all) * scale) * stats[t, 8:16]
    factor = jnp.exp((stats[tp, 0:8] - top_all) * scale) / total_all
    for hp in range(4):
        for i in range(2):
            h = 2 * hp + i
            turned = ot_scr[hp, :, i * 128 : (i + 1) * 128] * factor[h : h + 1]
            mixed = dot_nn(turned.T.astype(BF16), value_up[:, h * 128 : (h + 1) * 128])
            blocks = mixed.astype(BF16).reshape(NX, NC, SHARE, 128)
            for core in range(NC):
                o_send[hp * NC + core, i * 64 : (i + 1) * 64] = blocks[:, core].reshape(64, 128)
    for j in range(1, NT):
        t = (tp + j) % NT
        go(push(o_send.at[t], o_recv.at[tp], os_.at[j - 1], or_.at[tp], tp_peer(t)))
    o_recv[tp] = o_send[tp]
    w_step(3)
    push(owbuf.at[1 - c], owbuf.at[1 - c], ows.at[0], owr.at[0], partner).wait_recv()
    for j in range(1, NT):
        t = (tp + j) % NT
        push(o_recv.at[t], o_recv.at[t], os_.at[0], or_.at[t], tp_peer(t)).wait_recv()
    attended = o_recv[0].astype(F32)
    for t in range(1, NT):
        attended += o_recv[t].astype(F32)
    attended = attended.astype(BF16)
    r_send[...] = (
        dot_nn(attended[:64], owbuf[0]) + dot_nn(attended[64:], owbuf[1])
    ).astype(BF16)
    for j in range(1, NX):
        xx = (x + j) % NX
        src = r_send.at[pl.ds(pl.multiple_of(xx * SHARE, SHARE), SHARE)]
        go(push(src, r_recv.at[x], rss.at[j - 1], rsr.at[x], (z, y, xx, c)))
    r_recv[x] = r_send[pl.ds(pl.multiple_of(x * SHARE, SHARE), SHARE)]
    for j in range(1, NX):
        xx = (x + j) % NX
        push(r_recv.at[xx], r_recv.at[xx], rss.at[0], rsr.at[xx], (z, y, xx, c)).wait_recv()
    summed = r_recv[0].astype(F32)
    for j in range(1, NX):
        summed += r_recv[j].astype(F32)
    summed = summed.astype(BF16).astype(F32)
    flow = (resid[...].astype(F32) + rms_norm(summed, gains[0:1])).astype(BF16).astype(F32)
    stream[...] = flow
    in_send[...] = rms_norm(flow, gains[1:2]).astype(BF16)

    def in_slot(s):
        return inbuf.at[pl.ds(pl.multiple_of(s * SHARE, SHARE), SHARE)]

    mine = (y % 2) * NT + tp

    def ag_copy(j):
        chip = (y * NX + x + j) % (NY * NX)
        dev = (z, chip // NX, chip % NX, half)
        return push(in_send, in_slot(mine), ags.at[j], agr.at[mine], dev)

    @pl.loop(1, NY * NX)
    def _(j):
        ag_copy(j).start()

    @pl.when(half == c)
    def _():
        in_slot(mine)[...] = in_send[...]

    @pl.when(half != c)
    def _():
        ag_copy(0).start()

    for step in range(4, 9):
        w_step(step)

    @pl.loop(0, NZ)
    def _(k):
        slot = w_slot(1 - c, k)
        push(slot, slot, wps.at[0], wpr.at[k], partner).wait_recv()

    own_slot = jnp.where(half == c, mine, -1)

    @pl.loop(0, 16)
    def _(s):
        @pl.when(s != own_slot)
        def _():
            push(in_slot(s), in_slot(s), ags.at[0], agr.at[s], partner).wait_recv()

    for core in range(NC):
        up[core, 8 : 8 + TOK] = dot_nn(inbuf[...], wbuf[core, :, :UP])

    low_dev = ((z + c) % NZ, y, x, 1 - c)
    high_dev = ((z + c - 1 + NZ) % NZ, y, x, 1 - c)
    go(push(up.at[:, pl.ds(TOK, 8)], up.at[:, pl.ds(0, 8)], hs.at[0], hr.at[0], low_dev))
    go(push(up.at[:, pl.ds(8, 8)], up.at[:, pl.ds(TOK + 8, 8)], hs.at[1], hr.at[1], high_dev))
    low, high = up.at[:, pl.ds(0, 8)], up.at[:, pl.ds(TOK + 8, 8)]
    push(low, low, hs.at[0], hr.at[0], low_dev).wait_recv()
    push(high, high, hs.at[1], hr.at[1], high_dev).wait_recv()

    @pl.when((z == 0) & (c == 0))
    def _():
        up[:, 0:8] = jnp.zeros((NC, 8, UP), F32)

    @pl.when((z == NZ - 1) & (c == 1))
    def _():
        up[:, TOK + 8 : TOK + 16] = jnp.zeros((NC, 8, UP), F32)

    hidden = []
    for core in range(NC):
        conv = (
            up[core, 7 : 7 + TOK] * taps[core, 0:1]
            + up[core, 8 : 8 + TOK] * taps[core, 1:2]
            + up[core, 9 : 9 + TOK] * taps[core, 2:3]
        )
        gate = conv[:, 128:256]
        first = gate / (1.0 + jnp.exp(-gate)) * conv[:, :128]
        gate = pltpu.roll(conv[:, 256:], 64, 1)
        second = gate / (1.0 + jnp.exp(-gate)) * conv[:, 256:]
        lane = lax.broadcasted_iota(jnp.int32, second.shape, 1)
        second = jnp.where(lane < 64, second, 0.0)
        hidden.append(jnp.concatenate([first.astype(BF16), second.astype(BF16)], axis=1))
    p_send[...] = (
        dot_nt(hidden[0], wbuf[0, :, UP:]) + dot_nt(hidden[1], wbuf[1, :, UP:])
    ).astype(BF16)

    chip = y * NX + x

    def p_slot(s):
        return p_send.at[pl.ds(pl.multiple_of(s * SHARE, SHARE), SHARE)]

    def rs_copy(s):
        dev = (z, 2 * c + s // NT, (s // NC) % NX, s % NC)
        return push(p_slot(s), p_recv.at[chip], ps.at[s], pr.at[chip], dev)

    @pl.loop(0, 16)
    def _(j):
        s = (mine + j) % 16

        @pl.when(s != own_slot)
        def _():
            rs_copy(s).start()

    @pl.when(half == c)
    def _():
        p_recv[chip] = p_slot(mine)[...]

    own_chip = jnp.where(half == c, chip, -1)

    @pl.loop(0, 16)
    def _(k):
        @pl.when(k != own_chip)
        def _():
            push(p_recv.at[k], p_recv.at[k], ps.at[0], pr.at[k], partner).wait_recv()

    projected = p_recv[0].astype(F32)
    for k in range(1, 16):
        projected += p_recv[k].astype(F32)
    projected = projected.astype(BF16).astype(F32)
    out[...] = (stream[...] + rms_norm(projected, gains[2:3])).astype(BF16)

    for copy in pending:
        copy.wait_send()

    @pl.loop(1, NY * NX)
    def _(j):
        ag_copy(j).wait_send()

    @pl.when(half != c)
    def _():
        ag_copy(0).wait_send()

    @pl.loop(0, 16)
    def _(s):
        @pl.when(s != own_slot)
        def _():
            rs_copy(s).wait_send()


def body(
    residual,
    query_nope,
    query_rope,
    latent,
    rope_key,
    kv_gain,
    key_up,
    value_up,
    out_weight,
    post_gain,
    pre_gain,
    ffn_gain,
    up_value,
    up_gate,
    conv_value,
    conv_gate,
    down_weight,
):
    tp = lax.axis_index(TP)
    y = lax.axis_index("y")
    sp = lax.axis_index(SP)
    scale = (query_nope.shape[2] + query_rope.shape[2]) ** (-0.5)
    positions = sp * ROWS + jnp.arange(ROWS, dtype=jnp.int32)
    key_positions = sp * ROWS + tp * SHARE + jnp.arange(SHARE, dtype=jnp.int32)

    def own_rows(a):
        return lax.dynamic_slice_in_dim(a, tp * SHARE, SHARE, 0)

    normed = rms_norm(own_rows(latent).astype(F32), kv_gain.astype(F32)).astype(BF16)
    key_turn = rotate(own_rows(rope_key).astype(F32), key_positions).astype(BF16)
    query_turn = rotate(query_rope[:, 0].astype(F32), positions).astype(BF16)
    kv_loc = jnp.concatenate([normed, key_turn, jnp.zeros((SHARE, 64), BF16)], axis=1)
    q_loc = jnp.concatenate([query_nope[:, 0], query_turn, jnp.zeros((ROWS, 64), BF16)], axis=1)

    width = up_value.shape[1] // NY
    rest = width - 128

    def by_y(a):
        return jnp.transpose(a.reshape(a.shape[0], NY, width), (1, 0, 2))

    def lanes(v, g):
        pad = jnp.zeros(v.shape[:-1] + (64 - rest,), v.dtype)
        return [v[..., :128], g[..., :128], v[..., 128:], pad, g[..., 128:], pad]

    value, gate, down = by_y(up_value), by_y(up_gate), by_y(down_weight.T)
    w_loc = jnp.concatenate(
        lanes(value, gate) + [down, jnp.zeros(down.shape[:-1] + (256 - width,), BF16)], axis=-1
    )

    def chip_taps(core):
        start = (tp // NC * NC + core) * width * NY + y * width
        v = lax.dynamic_slice_in_dim(conv_value, start, width, 1)
        g = lax.dynamic_slice_in_dim(conv_gate, start, width, 1)
        return jnp.concatenate(lanes(v, g), axis=-1)

    taps = jnp.stack([chip_taps(0), chip_taps(1)]).astype(F32)
    taps = jnp.pad(taps, ((0, 0), (0, 5), (0, 0)))
    gains = jnp.pad(jnp.stack([post_gain, pre_gain, ffn_gain]).astype(F32), ((0, 5), (0, 0)))

    dma = pltpu.SemaphoreType.DMA
    vmem = pltpu.VMEM
    return pl.pallas_call(
        functools.partial(layer_kernel, scale),
        out_shape=jax.ShapeDtypeStruct((SHARE, D), BF16),
        in_specs=[pl.BlockSpec(memory_space=vmem)] * 9,
        out_specs=pl.BlockSpec(memory_space=vmem),
        scratch_shapes=[
            vmem((KEYS, KW), BF16),
            vmem((NT, ROWS, QW), BF16),
            vmem((NC, NZ * ROWS, WL), BF16),
            vmem((NC, 128, D), BF16),
            vmem((256, KEYS), BF16),
            vmem((KEYS, 256), F32),
            vmem((4, 256, 256), F32),
            vmem((NT, 16, 128), F32),
            vmem((NT, 128, 128), BF16),
            vmem((NT, 128, 128), BF16),
            vmem((64, D), BF16),
            vmem((NX, SHARE, D), BF16),
            vmem((SHARE, D), BF16),
            vmem((TOK, D), BF16),
            vmem((NC, TOK + 16, UP), F32),
            vmem((TOK, D), BF16),
            vmem((NY * NX, SHARE, D), BF16),
            vmem((SHARE, D), F32),
        ]
        + [
            dma((n,))
            for n in (15, 48, 64, 7, 8, 3, 4, 16, 16, 16, 16, 1, 1, 7, 8, 7, 8, 3, 4, 16, 16, 2, 2, 16, 16)
        ],
        compiler_params=pltpu.CompilerParams(
            collective_id=0, has_side_effects=True, vmem_limit_bytes=60 * 1024 * 1024
        ),
        name="layer",
    )(
        kv_loc,
        q_loc,
        w_loc,
        out_weight,
        key_up.reshape(key_up.shape[0], -1),
        value_up.reshape(value_up.shape[0], -1),
        own_rows(residual),
        gains,
        taps,
    )


def solution(mesh):
    torus = Mesh(mesh.devices.reshape(NZ, NY, NX, NC), AXES)
    return jax.shard_map(
        body,
        mesh=torus,
        in_specs=(
            P(SP, None),
            P(SP, TP, None),
            P(SP, TP, None),
            P(SP, None),
            P(SP, None),
            P(),
            P(),
            P(),
            P(TP, None),
            P(),
            P(),
            P(),
            P(SP, TP),
            P(SP, TP),
            P(),
            P(),
            P(TP, SP),
        ),
        out_specs=P(SP + TP, None),
        check_vma=False,
    )
```

```python
import functools

import jax
import jax.numpy as jnp
import numpy as np
from jax import lax
from jax.experimental import pallas as pl
from jax.experimental.pallas import tpu as pltpu
from jax.sharding import Mesh
from jax.sharding import PartitionSpec as P

GRID = 64
AXES = ("z", "y", "x", "c")
SP = ("z", "y")
TP = ("x", "c")
MESH_IDS = pl.DeviceIdType.MESH
F32 = jnp.float32
BF16 = jnp.bfloat16

epsilon = 1e-06
rope_base = 10000.0

NZ, NY, NX, NC = 16, 4, 4, 2
NT = NX * NC
PLANE = NY * NT
D = 2048
ROWS = 128
SHARE = 16
KEYS = NZ * NY * SHARE
QW = 256
KW = 384
WL = 640
UP = 384
HID = 176
W_AT = {1: 0, 5: 1, 8: 2}
TOK = 256


def rms_norm(values, gain):
    return (
        values * lax.rsqrt(jnp.mean(values * values, axis=-1, keepdims=True) + epsilon) * gain
    )


def turn_tables():
    pairs = 16
    frequency = rope_base ** (-np.arange(pairs) / pairs)
    sign = np.repeat([-1.0, 1.0], pairs)

    def both(steps, at):
        angles = np.tile(np.arange(steps)[:, None] * frequency, (1, 2))
        table = np.zeros((2, steps, 128))
        table[0, :, at : at + 32] = np.cos(angles)
        table[1, :, at : at + 32] = np.sin(angles) * sign
        return table

    by_row = both(ROWS // GRID * NZ * NY, 0).reshape(2, NZ * NY, ROWS // GRID, 128)
    by_row = by_row.transpose(1, 0, 2, 3).reshape(NZ * NY, 2 * ROWS // GRID, 128)
    by_row = np.pad(by_row, ((0, 0), (0, 8 - 2 * ROWS // GRID), (0, 0)))
    return by_row.astype(np.float32), both(GRID, 32).astype(np.float32)


def turned(values, cosine, sine):
    lane = lax.broadcasted_iota(jnp.int32, values.shape, 1)
    other = jnp.where((lane & 16) == 0, pltpu.roll(values, 112, 1), pltpu.roll(values, 16, 1))
    return values * cosine + other * sine


def widen64(values):
    return jnp.concatenate([values.astype(F32), jnp.zeros(values.shape, F32)], axis=1)


def dot_nn(a, b):
    return jnp.dot(a, b, preferred_element_type=F32)


def dot_nt(a, b):
    return lax.dot_general(a, b, (((1,), (1,)), ((), ())), preferred_element_type=F32)


def side_lanes(v, g):
    rest = HID - 128
    pad = jnp.zeros(v.shape[:-1] + (64 - rest,), v.dtype)
    return [v[:, :128], g[:, :128], v[:, 128:], pad, g[:, 128:], pad]


def layer_kernel(
    scale,
    latent,
    rope_key,
    kv_gain,
    q_nope,
    q_rope,
    by_row,
    by_col,
    up_value,
    up_gate,
    down,
    ow,
    key_up,
    value_up,
    resid,
    post_gain,
    pre_gain,
    ffn_gain,
    conv_value,
    conv_gate,
    out,
    kvbuf,
    qbuf,
    wbuf,
    owbuf,
    kvt,
    s_scr,
    ot_scr,
    stats,
    o_send,
    o_recv,
    r_send,
    r_recv,
    in_send,
    inbuf,
    up,
    p_send,
    p_recv,
    stream,
    latent_v,
    rope_key_v,
    kv_gain_v,
    q_nope_v,
    q_rope_v,
    by_row_v,
    by_col_v,
    up_value_v,
    up_gate_v,
    down_v,
    key_up_v,
    value_up_v,
    resid_v,
    gains,
    conv_v,
    turns,
    w_loc,
    wide,
    qf,
    vu,
    taps,
    loads,
    kvs_z,
    kvs_y,
    kvr,
    qs,
    qr,
    wys,
    wyr,
    wzs,
    wps,
    wzr,
    wpr,
    ows,
    owr,
    sts,
    str_,
    os_,
    or_,
    rss,
    rsr,
    ags,
    agr,
    hs,
    hr,
    ps,
    pr,
):
    z, y, x, c = (lax.axis_index(a) for a in AXES)
    tp = x * NC + c
    plane = y * NT + tp
    half = y // 2

    def zz(k):
        return (z + k + NZ) % NZ

    def push(src, dst, ss, rs, dev):
        return pltpu.make_async_remote_copy(
            src_ref=src, dst_ref=dst, send_sem=ss, recv_sem=rs, device_id=dev,
            device_id_type=MESH_IDS,
        )

    partner = (z, y, x, 1 - c)
    right, left = (zz(1), y, x, c), (zz(-1), y, x, c)
    right2, left2 = (zz(2), y, x, c), (zz(-2), y, x, c)
    cross = ((z + 2 * c - 1 + NZ) % NZ, y, x, 1 - c)

    def on_plane(j):
        p = (plane + j) % PLANE
        return (z, p // NT, (p // NC) % NX, p % NC)

    def tp_peer(t):
        return (z, y, t // NC, t % NC)

    def own(ref):
        return ref.at[pl.ds(pl.multiple_of(tp * SHARE, SHARE), SHARE)]

    local = {}

    def load(name, src, dst):
        local[name] = pltpu.make_async_copy(src, dst, loads.at[len(local)])
        local[name].start()

    load("latent", own(latent), latent_v)
    load("rope_key", own(rope_key), rope_key_v)
    load("by_row", by_row.at[z * NY + y], by_row_v)
    load("by_col", by_col, by_col_v)
    load("kv_gain", kv_gain, kv_gain_v)
    load("q_nope", q_nope, q_nope_v)
    load("q_rope", q_rope, q_rope_v)
    load("up_value", up_value, up_value_v)
    load("up_gate", up_gate, up_gate_v)
    load("down", down, down_v)
    load("ow", ow, owbuf.at[c])
    load("key_up", key_up, key_up_v)
    load("value_up", value_up, value_up_v)
    load("resid", own(resid), resid_v)
    load("post", post_gain, gains.at[0])
    load("pre", pre_gain, gains.at[1])
    load("ffn", ffn_gain, gains.at[2])
    load("conv_value", conv_value, conv_v.at[0])
    load("conv_gate", conv_gate, conv_v.at[1])

    def ready(*names):
        for name in names:
            local[name].wait()

    barrier = pltpu.get_barrier_semaphore()
    for dev in (right, left, right2, left2, cross):
        pl.semaphore_signal(barrier, inc=1, device_id=dev, device_id_type=MESH_IDS)

    @pl.loop(1, PLANE)
    def _(j):
        pl.semaphore_signal(barrier, inc=1, device_id=on_plane(j), device_id_type=MESH_IDS)

    def kv_slot(yy, k):
        start = pl.multiple_of((yy * NZ + k) * SHARE, SHARE)
        return kvbuf.at[pl.ds(start, SHARE)]

    def w_slot(core, k):
        return wbuf.at[core, pl.ds(pl.multiple_of(k * ROWS, ROWS), ROWS)]

    def w_part(k, yy):
        return wbuf.at[c, pl.ds(pl.multiple_of(k * ROWS + yy * 32, 32), 32)]

    ready("latent", "rope_key", "by_row", "by_col", "kv_gain")
    for i in range(2):
        grid_rows = [
            by_row_v[2 * i + j : 2 * i + j + 1] + by_col_v[i] for j in range(ROWS // GRID)
        ]
        turns[i] = jnp.concatenate(grid_rows, axis=0)
    rows = pl.ds(pl.multiple_of(tp * SHARE, SHARE), SHARE)
    kv_slot(y, z)[:, :256] = rms_norm(
        latent_v[...].astype(F32), kv_gain_v[...].astype(F32)
    ).astype(BF16)
    kv_slot(y, z)[:, 256:] = turned(
        widen64(rope_key_v[...]), turns[0, rows], turns[1, rows]
    ).astype(BF16)

    pl.semaphore_wait(barrier, 5 + PLANE - 1)

    pending = []

    def go(copy):
        copy.start()
        pending.append(copy)

    def kv_to(k, sem, dev):
        slot = kv_slot(y, k)
        go(push(slot, slot, kvs_z.at[sem], kvr.at[y * NZ + k], dev))

    def kv_to_y(k, sem):
        slot = kv_slot(y, k)
        for j in range(1, NY):
            dev = (z, (y + j) % NY, x, c)
            go(push(slot, slot, kvs_y.at[sem * 3 + j - 1], kvr.at[y * NZ + k], dev))

    kv_to(z, 0, right2)
    kv_to(z, 1, left2)
    kv_to(z, 2, right)
    kv_to(z, 3, left)
    kv_to_y(z, 0)
    ready("q_nope", "q_rope")
    qbuf[tp, :, :128] = q_nope_v[...]
    qbuf[tp, :, 128:] = turned(widen64(q_rope_v[...]), turns[0], turns[1]).astype(BF16)
    for j in range(1, NT):
        t = (tp + j) % NT
        go(push(qbuf.at[tp], qbuf.at[tp], qs.at[j - 1], qr.at[tp], tp_peer(t)))

    ready("up_value", "up_gate", "down")
    eye = (
        lax.broadcasted_iota(jnp.int32, (32, 32), 0) == lax.broadcasted_iota(jnp.int32, (32, 32), 1)
    ).astype(BF16)
    value, gate = up_value_v[...].astype(F32), up_gate_v[...].astype(F32)
    across = dot_nt(eye, down_v[...])
    for yy in range(NY):
        at = slice(yy * HID, (yy + 1) * HID)
        parts = side_lanes(value[:, at], gate[:, at])
        parts += [across[:, at], jnp.zeros((32, 256 - HID), F32)]
        w_loc[yy] = jnp.concatenate(parts, axis=1).astype(BF16)
    for j in range(1, NY):
        yy = (y + j) % NY
        go(push(w_loc.at[yy], w_part(z, y), wys.at[j - 1], wyr.at[y], (z, yy, x, c)))
    w_part(z, y)[...] = w_loc[y]
    ready("ow")
    go(push(owbuf.at[c], owbuf.at[c], ows.at[0], owr.at[0], partner))

    def w_send(k, step, to_right, to_left):
        slot = w_slot(c, k)
        if to_right:
            go(push(slot, slot, wzs.at[step], wzr.at[k], right))
        if to_left:
            go(push(slot, slot, wzs.at[8 + step], wzr.at[k], left))

    def w_across(k, sem):
        slot = w_slot(c, k)
        go(push(slot, slot, wps.at[sem], wpr.at[k], partner))

    def w_step(step):
        if step == 0:
            for j in range(1, NY):
                yy = (y + j) % NY
                part = w_part(z, yy)
                push(part, part, wys.at[j - 1], wyr.at[yy], (z, yy, x, c)).wait_recv()
            w_send(z, 0, True, True)
            w_across(z, 0)
            return
        k = zz(-step)
        slot = w_slot(c, k)
        push(slot, slot, wzs.at[0], wzr.at[k], left).wait_recv()
        w_send(k, step, step < 8, False)
        w_across(k, 2 * step - 1)
        if step < 8:
            k = zz(step)
            slot = w_slot(c, k)
            push(slot, slot, wzs.at[0], wzr.at[k], right).wait_recv()
            w_send(k, step, False, step < 7)
            w_across(k, 2 * step)

    def kv_wait(yy, k):
        slot = kv_slot(yy, k)
        push(slot, slot, kvs_z.at[0], kvr.at[yy * NZ + k], right).wait_recv()

    def fold_queries():
        for j in range(1, NT):
            t = (tp + j) % NT
            push(qbuf.at[t], qbuf.at[t], qs.at[0], qr.at[t], tp_peer(t)).wait_recv()
        ready("key_up")
        wide[...] = key_up_v[...].astype(F32)
        for h in range(NT):
            up_h = wide[pl.ds(h, 256, stride=NT)].astype(BF16)
            r = slice(h % 2 * 128, h % 2 * 128 + 128)
            qf[h // 2, r, :256] = dot_nt(qbuf[h, :, :128], up_h).astype(BF16)
            qf[h // 2, r, 256:] = qbuf[h, :, 128:]

    def split_values():
        ready("value_up")
        wide[...] = value_up_v[...].astype(F32)
        for h in range(NT):
            vu[h] = wide[pl.ds(h, 256, stride=NT)].astype(BF16)

    for d in range(1, 9):
        if d == 4:
            fold_queries()
        if d == 6:
            split_values()
        k = zz(-d)
        kv_wait(y, k)
        if d + 2 <= 8:
            kv_to(k, 3 + d, right2)
        if d < 8:
            k2 = zz(d)
            kv_wait(y, k2)
            if d + 2 <= 7:
                kv_to(k2, 9 + d, left2)
        kv_to_y(k, 2 * d - 1)
        if d < 8:
            kv_to_y(k2, 2 * d)
        if d in W_AT:
            w_step(W_AT[d])
    for j in range(1, NY):
        yy = (y + j) % NY

        @pl.loop(0, NZ)
        def _(k):
            kv_wait(yy, k)

    kvt[...] = kvbuf[:, :256].T
    for hp in range(4):
        s_now = s_scr.at[hp % 2]
        s_now[...] = dot_nt(kvbuf[...], qf[hp])
        top = jnp.max(s_now[...], axis=0, keepdims=True)
        weights = jnp.exp((s_now[...] - top) * scale)
        total = jnp.sum(weights, axis=0, keepdims=True)
        ot_scr[hp] = dot_nn(kvt[...], weights.astype(BF16))
        for i in range(2):
            h = 2 * hp + i
            stats[tp, h : h + 1] = top[:, i * 128 : (i + 1) * 128]
            stats[tp, 8 + h : 9 + h] = total[:, i * 128 : (i + 1) * 128]
        if hp == 1:
            w_step(3)

    for j in range(1, NT):
        t = (tp + j) % NT
        go(push(stats.at[tp], stats.at[tp], sts.at[j - 1], str_.at[tp], tp_peer(t)))
    w_step(4)
    for j in range(1, NT):
        t = (tp + j) % NT
        push(stats.at[t], stats.at[t], sts.at[0], str_.at[t], tp_peer(t)).wait_recv()
    top_all = stats[0, 0:8]
    for t in range(1, NT):
        top_all = jnp.maximum(top_all, stats[t, 0:8])
    total_all = jnp.zeros_like(top_all)
    for t in range(NT):
        total_all += jnp.exp((stats[t, 0:8] - top_all) * scale) * stats[t, 8:16]
    factor = jnp.exp((stats[tp, 0:8] - top_all) * scale) / total_all
    for hp in range(4):
        for i in range(2):
            h = 2 * hp + i
            scaled = ot_scr[hp, :, i * 128 : (i + 1) * 128] * factor[h : h + 1]
            mixed = dot_nn(scaled.T.astype(BF16), vu[h])
            blocks = mixed.astype(BF16).reshape(NX, NC, SHARE, 128)
            for core in range(NC):
                o_send[hp * NC + core, i * 64 : (i + 1) * 64] = blocks[:, core].reshape(64, 128)
    for j in range(1, NT):
        t = (tp + j) % NT
        go(push(o_send.at[t], o_recv.at[tp], os_.at[j - 1], or_.at[tp], tp_peer(t)))
    o_recv[tp] = o_send[tp]
    w_step(5)
    push(owbuf.at[1 - c], owbuf.at[1 - c], ows.at[0], owr.at[0], partner).wait_recv()
    for j in range(1, NT):
        t = (tp + j) % NT
        push(o_recv.at[t], o_recv.at[t], os_.at[0], or_.at[t], tp_peer(t)).wait_recv()
    attended = o_recv[0].astype(F32)
    for t in range(1, NT):
        attended += o_recv[t].astype(F32)
    attended = attended.astype(BF16)
    r_send[...] = (
        dot_nn(attended[:64], owbuf[0]) + dot_nn(attended[64:], owbuf[1])
    ).astype(BF16)
    for j in range(1, NX):
        xx = (x + j) % NX
        src = r_send.at[pl.ds(pl.multiple_of(xx * SHARE, SHARE), SHARE)]
        go(push(src, r_recv.at[x], rss.at[j - 1], rsr.at[x], (z, y, xx, c)))
    r_recv[x] = r_send[pl.ds(pl.multiple_of(x * SHARE, SHARE), SHARE)]
    for j in range(1, NX):
        xx = (x + j) % NX
        push(r_recv.at[xx], r_recv.at[xx], rss.at[0], rsr.at[xx], (z, y, xx, c)).wait_recv()
    ready("resid", "post", "pre", "ffn")
    summed = r_recv[0].astype(F32)
    for j in range(1, NX):
        summed += r_recv[j].astype(F32)
    summed = summed.astype(BF16).astype(F32)
    flow = (resid_v[...].astype(F32) + rms_norm(summed, gains[0].astype(F32))).astype(BF16).astype(F32)
    stream[...] = flow
    in_send[...] = rms_norm(flow, gains[1].astype(F32)).astype(BF16)

    def in_slot(s):
        return inbuf.at[pl.ds(pl.multiple_of(s * SHARE, SHARE), SHARE)]

    mine = (y % 2) * NT + tp

    def ag_copy(j):
        chip = (y * NX + x + j) % (NY * NX)
        dev = (z, chip // NX, chip % NX, half)
        return push(in_send, in_slot(mine), ags.at[j], agr.at[mine], dev)

    @pl.loop(1, NY * NX)
    def _(j):
        ag_copy(j).start()

    @pl.when(half == c)
    def _():
        in_slot(mine)[...] = in_send[...]

    @pl.when(half != c)
    def _():
        ag_copy(0).start()

    for step in range(6, 9):
        w_step(step)

    ready("conv_value", "conv_gate")
    last = conv_v.shape[2] - UP
    for core in range(NC):
        first = (x * NC + core) * NY * HID + y * HID
        base = jnp.minimum(first // 128 * 128, last)
        lanes = pl.ds(pl.multiple_of(base, 128), UP)
        back = UP - (first - base)
        v = pltpu.roll(conv_v[0, :, lanes].astype(F32), back, 1)
        g = pltpu.roll(conv_v[1, :, lanes].astype(F32), back, 1)
        taps[core, 0:3] = jnp.concatenate(side_lanes(v[:, :HID], g[:, :HID]), axis=1)

    @pl.loop(0, NZ)
    def _(k):
        slot = w_slot(1 - c, k)
        push(slot, slot, wps.at[0], wpr.at[k], partner).wait_recv()

    own_slot = jnp.where(half == c, mine, -1)

    @pl.loop(0, 16)
    def _(s):
        @pl.when(s != own_slot)
        def _():
            push(in_slot(s), in_slot(s), ags.at[0], agr.at[s], partner).wait_recv()

    for core in range(NC):
        up[core, 8 : 8 + TOK] = dot_nn(inbuf[...], wbuf[core, :, :UP])

    low_dev = ((z + c) % NZ, y, x, 1 - c)
    high_dev = ((z + c - 1 + NZ) % NZ, y, x, 1 - c)
    go(push(up.at[:, pl.ds(TOK, 8)], up.at[:, pl.ds(0, 8)], hs.at[0], hr.at[0], low_dev))
    go(push(up.at[:, pl.ds(8, 8)], up.at[:, pl.ds(TOK + 8, 8)], hs.at[1], hr.at[1], high_dev))
    low, high = up.at[:, pl.ds(0, 8)], up.at[:, pl.ds(TOK + 8, 8)]
    push(low, low, hs.at[0], hr.at[0], low_dev).wait_recv()
    push(high, high, hs.at[1], hr.at[1], high_dev).wait_recv()

    @pl.when((z == 0) & (c == 0))
    def _():
        up[:, 0:8] = jnp.zeros((NC, 8, UP), F32)

    @pl.when((z == NZ - 1) & (c == 1))
    def _():
        up[:, TOK + 8 : TOK + 16] = jnp.zeros((NC, 8, UP), F32)

    hidden = []
    for core in range(NC):
        conv = (
            up[core, 7 : 7 + TOK] * taps[core, 0:1]
            + up[core, 8 : 8 + TOK] * taps[core, 1:2]
            + up[core, 9 : 9 + TOK] * taps[core, 2:3]
        )
        gate = conv[:, 128:256]
        first = gate / (1.0 + jnp.exp(-gate)) * conv[:, :128]
        gate = pltpu.roll(conv[:, 256:], 64, 1)
        second = gate / (1.0 + jnp.exp(-gate)) * conv[:, 256:]
        lane = lax.broadcasted_iota(jnp.int32, second.shape, 1)
        second = jnp.where(lane < 64, second, 0.0)
        hidden.append(jnp.concatenate([first.astype(BF16), second.astype(BF16)], axis=1))
    p_send[...] = (
        dot_nt(hidden[0], wbuf[0, :, UP:]) + dot_nt(hidden[1], wbuf[1, :, UP:])
    ).astype(BF16)

    chip = y * NX + x

    def p_slot(s):
        return p_send.at[pl.ds(pl.multiple_of(s * SHARE, SHARE), SHARE)]

    def rs_copy(s):
        dev = (z, 2 * c + s // NT, (s // NC) % NX, s % NC)
        return push(p_slot(s), p_recv.at[chip], ps.at[s], pr.at[chip], dev)

    @pl.loop(0, 16)
    def _(j):
        s = (mine + j) % 16

        @pl.when(s != own_slot)
        def _():
            rs_copy(s).start()

    @pl.when(half == c)
    def _():
        p_recv[chip] = p_slot(mine)[...]

    own_chip = jnp.where(half == c, chip, -1)

    @pl.loop(0, 16)
    def _(k):
        @pl.when(k != own_chip)
        def _():
            push(p_recv.at[k], p_recv.at[k], ps.at[0], pr.at[k], partner).wait_recv()

    projected = p_recv[0].astype(F32)
    for k in range(1, 16):
        projected += p_recv[k].astype(F32)
    projected = projected.astype(BF16).astype(F32)
    out[...] = (stream[...] + rms_norm(projected, gains[2].astype(F32))).astype(BF16)

    for copy in pending:
        copy.wait_send()

    @pl.loop(1, NY * NX)
    def _(j):
        ag_copy(j).wait_send()

    @pl.when(half != c)
    def _():
        ag_copy(0).wait_send()

    @pl.loop(0, 16)
    def _(s):
        @pl.when(s != own_slot)
        def _():
            rs_copy(s).wait_send()


def body(
    residual,
    query_nope,
    query_rope,
    latent,
    rope_key,
    kv_gain,
    key_up,
    value_up,
    out_weight,
    post_gain,
    pre_gain,
    ffn_gain,
    up_value,
    up_gate,
    conv_value,
    conv_gate,
    down_weight,
):
    scale = (query_nope.shape[2] + query_rope.shape[2]) ** (-0.5)
    by_row, by_col = turn_tables()
    dma = pltpu.SemaphoreType.DMA
    vmem = pltpu.VMEM
    return pl.pallas_call(
        functools.partial(layer_kernel, scale),
        out_shape=jax.ShapeDtypeStruct((SHARE, D), BF16),
        in_specs=[pl.BlockSpec(memory_space=pl.ANY)] * 19,
        out_specs=pl.BlockSpec(memory_space=vmem),
        scratch_shapes=[
            vmem((KEYS, KW), BF16),
            vmem((NT, ROWS, QW), BF16),
            vmem((NC, NZ * ROWS, WL), BF16),
            vmem((NC, 128, D), BF16),
            vmem((256, KEYS), BF16),
            vmem((2, KEYS, 256), F32),
            vmem((4, 256, 256), F32),
            vmem((NT, 16, 128), F32),
            vmem((NT, 128, 128), BF16),
            vmem((NT, 128, 128), BF16),
            vmem((64, D), BF16),
            vmem((NX, SHARE, D), BF16),
            vmem((SHARE, D), BF16),
            vmem((TOK, D), BF16),
            vmem((NC, TOK + 16, UP), F32),
            vmem((TOK, D), BF16),
            vmem((NY * NX, SHARE, D), BF16),
            vmem((SHARE, D), F32),
            vmem((SHARE, 256), BF16),
            vmem((SHARE, 64), BF16),
            vmem((1, 256), BF16),
            vmem((ROWS, 128), BF16),
            vmem((ROWS, 64), BF16),
            vmem((8, 128), F32),
            vmem((2, GRID, 128), F32),
            vmem(up_value.shape, BF16),
            vmem(up_gate.shape, BF16),
            vmem(down_weight.shape, BF16),
            vmem((256 * NT, 128), BF16),
            vmem((256 * NT, 128), BF16),
            vmem((SHARE, D), BF16),
            vmem((3, 1, D), BF16),
            vmem((2,) + conv_value.shape, BF16),
            vmem((2, ROWS, 128), F32),
            vmem((NY, 32, WL), BF16),
            vmem((256 * NT, 128), F32),
            vmem((4, 256, KW), BF16),
            vmem((NT, 256, 128), BF16),
            vmem((NC, 8, UP), F32),
        ]
        + [
            dma((n,))
            for n in (19, 15, 48, 64, 7, 8, 3, 4, 16, 16, 16, 16, 1, 1, 7, 8, 7, 8, 3, 4, 16, 16, 2, 2, 16, 16)
        ],
        compiler_params=pltpu.CompilerParams(
            collective_id=0, has_side_effects=True, vmem_limit_bytes=60 * 1024 * 1024
        ),
        name="layer",
    )(
        latent,
        rope_key,
        kv_gain[None],
        query_nope[:, 0],
        query_rope[:, 0],
        by_row,
        by_col,
        up_value,
        up_gate,
        down_weight,
        out_weight,
        key_up.reshape(-1, key_up.shape[2]),
        value_up.reshape(-1, value_up.shape[2]),
        residual,
        post_gain[None],
        pre_gain[None],
        ffn_gain[None],
        conv_value,
        conv_gate,
    )


def solution(mesh):
    torus = Mesh(mesh.devices.reshape(NZ, NY, NX, NC), AXES)
    return jax.shard_map(
        body,
        mesh=torus,
        in_specs=(
            P(SP, None),
            P(SP, TP, None),
            P(SP, TP, None),
            P(SP, None),
            P(SP, None),
            P(),
            P(),
            P(),
            P(TP, None),
            P(),
            P(),
            P(),
            P(SP, TP),
            P(SP, TP),
            P(),
            P(),
            P(TP, SP),
        ),
        out_specs=P(SP + TP, None),
        check_vma=False,
    )
```

```python
import functools

import jax
import jax.numpy as jnp
import numpy as np
from jax import lax
from jax.experimental import pallas as pl
from jax.experimental.pallas import tpu as pltpu
from jax.sharding import Mesh
from jax.sharding import PartitionSpec as P

GRID = 64
AXES = ("z", "y", "x", "c")
SP = ("z", "y")
TP = ("x", "c")
MESH_IDS = pl.DeviceIdType.MESH
F32 = jnp.float32
BF16 = jnp.bfloat16

epsilon = 1e-06
rope_base = 10000.0

NZ, NY, NX, NC = 16, 4, 4, 2
NT = NX * NC
PLANE = NY * NT
D = 2048
ROWS = 128
SHARE = 16
KEYS = NZ * NY * SHARE
QW = 256
KW = 384
UP = 384
HID = 176
W_AT = {2: [0], 6: [1], 8: [2]}
W_KVY = {1: [3], 2: [4]}
W_ATTN = {1: [5], 3: [6]}
W_MORE = ([7, 8], [9, 10], [11, 12, 13, 14, 15, 16])
TOK = 256


def rms_norm(values, gain):
    return (
        values * lax.rsqrt(jnp.mean(values * values, axis=-1, keepdims=True) + epsilon) * gain
    )


def turn_tables():
    pairs = 16
    frequency = rope_base ** (-np.arange(pairs) / pairs)
    sign = np.repeat([-1.0, 1.0], pairs)

    def both(steps, at):
        angles = np.tile(np.arange(steps)[:, None] * frequency, (1, 2))
        table = np.zeros((2, steps, 128))
        table[0, :, at : at + 32] = np.cos(angles)
        table[1, :, at : at + 32] = np.sin(angles) * sign
        return table

    by_row = both(ROWS // GRID * NZ * NY, 0).reshape(2, NZ * NY, ROWS // GRID, 128)
    by_row = by_row.transpose(1, 0, 2, 3).reshape(NZ * NY, 2 * ROWS // GRID, 128)
    by_row = np.pad(by_row, ((0, 0), (0, 8 - 2 * ROWS // GRID), (0, 0)))
    return by_row.astype(np.float32), both(GRID, 32).astype(np.float32)


def turned(values, cosine, sine):
    lane = lax.broadcasted_iota(jnp.int32, values.shape, 1)
    other = jnp.where((lane & 16) == 0, pltpu.roll(values, 112, 1), pltpu.roll(values, 16, 1))
    return values * cosine + other * sine


def in_one_row(ref):
    folded = ref[...].astype(F32)
    return jnp.concatenate([folded[i : i + 1] for i in range(folded.shape[0])], axis=1)


def as_rows(columns):
    both = jnp.concatenate([columns.astype(F32), jnp.zeros(columns.shape, F32)], axis=0)
    return both.T


def dot_nn(a, b):
    return jnp.dot(a, b, preferred_element_type=F32)


def dot_nt(a, b):
    return lax.dot_general(a, b, (((1,), (1,)), ((), ())), preferred_element_type=F32)


def side_lanes(v, g):
    rest = HID - 128
    pad = jnp.zeros(v.shape[:-1] + (64 - rest,), v.dtype)
    return [v[:, :128], g[:, :128], v[:, 128:], pad, g[:, 128:], pad]


def layer_kernel(
    scale,
    latent,
    rope_key,
    q_nope,
    q_rope,
    by_row,
    by_col,
    up_value,
    up_gate,
    down,
    ow,
    key_up,
    value_up,
    resid,
    kv_gain,
    post_gain,
    pre_gain,
    ffn_gain,
    conv_value,
    conv_gate,
    out,
    kvbuf,
    qbuf,
    wbuf,
    dbuf,
    d_stage,
    owbuf,
    kvt,
    s_scr,
    st_send,
    stats,
    o_send,
    o_recv,
    r_send,
    r_recv,
    in_send,
    inbuf,
    up,
    p_send,
    p_recv,
    stream,
    latent_v,
    rope_key_v,
    q_nope_v,
    q_rope_v,
    by_row_v,
    by_col_v,
    up_value_v,
    up_gate_v,
    down_v,
    key_up_v,
    value_up_v,
    resid_v,
    kv_gain_v,
    gains,
    conv_v,
    turns,
    key_rows,
    w_loc,
    d_loc,
    wide,
    qf,
    vu,
    taps,
    loads,
    kvs_z,
    kvs_y,
    kvr,
    qs,
    qr,
    wys,
    wyr,
    wzs,
    wps,
    wzr,
    wpr,
    ows,
    owr,
    sts,
    str_,
    os_,
    or_,
    rss,
    rsr,
    ags,
    agr,
    hs,
    hr,
    ps,
    pr,
):
    z, y, x, c = (lax.axis_index(a) for a in AXES)
    tp = x * NC + c
    plane = y * NT + tp
    half = y // 2

    def zz(k):
        return (z + k + NZ) % NZ

    def push(src, dst, ss, rs, dev):
        return pltpu.make_async_remote_copy(
            src_ref=src, dst_ref=dst, send_sem=ss, recv_sem=rs, device_id=dev,
            device_id_type=MESH_IDS,
        )

    partner = (z, y, x, 1 - c)
    right, left = (zz(1), y, x, c), (zz(-1), y, x, c)
    right2, left2 = (zz(2), y, x, c), (zz(-2), y, x, c)
    cross = ((z + 2 * c - 1 + NZ) % NZ, y, x, 1 - c)

    def on_plane(j):
        p = (plane + j) % PLANE
        return (z, p // NT, (p // NC) % NX, p % NC)

    def tp_peer(t):
        return (z, y, t // NC, t % NC)

    def own(ref):
        return ref.at[pl.ds(pl.multiple_of(tp * SHARE, SHARE), SHARE)]

    local = {}

    def load(name, src, dst):
        local[name] = pltpu.make_async_copy(src, dst, loads.at[len(local)])
        local[name].start()

    load("latent", own(latent), latent_v)
    load("rope_key", rope_key, rope_key_v)
    load("by_row", by_row.at[z * NY + y], by_row_v)
    load("by_col", by_col, by_col_v)
    load("kv_gain", kv_gain, kv_gain_v)
    load("post", post_gain, gains.at[0])
    load("pre", pre_gain, gains.at[1])
    load("ffn", ffn_gain, gains.at[2])
    load("q_nope", q_nope, q_nope_v)
    load("q_rope", q_rope, q_rope_v)
    load("up_value", up_value, up_value_v)
    load("up_gate", up_gate, up_gate_v)
    load("down", down, down_v)
    load("ow", ow, owbuf.at[c])
    load("key_up", key_up, key_up_v)
    load("value_up", value_up, value_up_v)
    load("resid", own(resid), resid_v)
    load("conv_value", conv_value, conv_v.at[0])
    load("conv_gate", conv_gate, conv_v.at[1])

    def ready(*names):
        for name in names:
            local[name].wait()

    barrier = pltpu.get_barrier_semaphore()
    for dev in (right, left, right2, left2, cross):
        pl.semaphore_signal(barrier, inc=1, device_id=dev, device_id_type=MESH_IDS)

    @pl.loop(1, PLANE)
    def _(j):
        pl.semaphore_signal(barrier, inc=1, device_id=on_plane(j), device_id_type=MESH_IDS)

    def kv_slot(yy, k):
        start = pl.multiple_of((yy * NZ + k) * SHARE, SHARE)
        return kvbuf.at[pl.ds(start, SHARE)]

    def w_slot(kind, core, k):
        at = pl.ds(pl.multiple_of(k * ROWS, ROWS), ROWS)
        if kind == 0:
            return wbuf.at[core, at]
        return dbuf.at[core, pl.ds(0, HID), at]

    def w_part(kind, yy):
        if kind == 0:
            return wbuf.at[c, pl.ds(pl.multiple_of(z * ROWS + yy * 32, 32), 32)]
        return d_stage.at[pl.ds(pl.multiple_of(yy * 32, 32), 32)]

    ready("latent", "rope_key", "by_row", "by_col", "kv_gain")
    for i in range(2):
        grid_rows = [
            by_row_v[2 * i + j : 2 * i + j + 1] + by_col_v[i] for j in range(ROWS // GRID)
        ]
        turns[i] = jnp.concatenate(grid_rows, axis=0)
    rows = pl.ds(pl.multiple_of(tp * SHARE, SHARE), SHARE)
    kv_slot(y, z)[:, :256] = rms_norm(
        latent_v[...].astype(F32), in_one_row(kv_gain_v)
    ).astype(BF16)
    key_rows[...] = as_rows(rope_key_v[...])
    kv_slot(y, z)[:, 256:] = turned(key_rows[rows], turns[0, rows], turns[1, rows]).astype(BF16)

    pl.semaphore_wait(barrier, 5 + PLANE - 1)

    pending = []

    def go(copy):
        copy.start()
        pending.append(copy)

    def kv_to(k, sem, dev):
        slot = kv_slot(y, k)
        go(push(slot, slot, kvs_z.at[sem], kvr.at[y * NZ + k], dev))

    def kv_to_y(k, sem):
        slot = kv_slot(y, k)
        for j in range(1, NY):
            dev = (z, (y + j) % NY, x, c)
            go(push(slot, slot, kvs_y.at[sem * 3 + j - 1], kvr.at[y * NZ + k], dev))

    kv_to(z, 0, right2)
    kv_to(z, 1, left2)
    kv_to(z, 2, right)
    kv_to(z, 3, left)
    kv_to_y(z, 0)
    ready("q_nope", "q_rope")
    qbuf[tp, :, :128] = q_nope_v[...]
    qbuf[tp, :, 128:] = turned(as_rows(q_rope_v[...]), turns[0], turns[1]).astype(BF16)
    for j in range(1, NT):
        t = (tp + j) % NT
        go(push(qbuf.at[tp], qbuf.at[tp], qs.at[j - 1], qr.at[tp], tp_peer(t)))

    ready("up_value", "up_gate", "down")
    value, gate = up_value_v[...].astype(F32), up_gate_v[...].astype(F32)
    across = down_v[...].astype(F32)
    for yy in range(NY):
        at = slice(yy * HID, (yy + 1) * HID)
        parts = side_lanes(value[:, at], gate[:, at])
        w_loc[yy] = jnp.concatenate(parts, axis=1).astype(BF16)
        parts = [across[:, at], jnp.zeros((32, 256 - HID), F32)]
        d_loc[yy] = jnp.concatenate(parts, axis=1).astype(BF16)
    for j in range(1, NY):
        yy = (y + j) % NY
        dev = (z, yy, x, c)
        go(push(w_loc.at[yy], w_part(0, y), wys.at[j - 1], wyr.at[y], dev))
        go(push(d_loc.at[yy], w_part(1, y), wys.at[j + 2], wyr.at[NY + y], dev))
    w_part(0, y)[...] = w_loc[y]
    w_part(1, y)[...] = d_loc[y]
    dbuf[:, HID:] = jnp.zeros((NC, 256 - HID, D), BF16)
    ready("ow")
    go(push(owbuf.at[c], owbuf.at[c], ows.at[0], owr.at[0], partner))

    def w_send(kind, k, step, to_right, to_left):
        slot = w_slot(kind, c, k)
        if to_right:
            go(push(slot, slot, wzs.at[kind, step], wzr.at[kind, k], right))
        if to_left:
            go(push(slot, slot, wzs.at[kind, 8 + step], wzr.at[kind, k], left))

    def w_across(kind, k, sem):
        slot = w_slot(kind, c, k)
        go(push(slot, slot, wps.at[kind, sem], wpr.at[kind, k], partner))

    def w_wait(kind, k, dev):
        slot = w_slot(kind, c, k)
        push(slot, slot, wzs.at[kind, 0], wzr.at[kind, k], dev).wait_recv()

    def w_start():
        for kind in range(2):
            for j in range(1, NY):
                yy = (y + j) % NY
                part = w_part(kind, yy)
                sem = wyr.at[kind * NY + yy]
                push(part, part, wys.at[0], sem, (z, yy, x, c)).wait_recv()
            if kind == 1:
                columns = pl.ds(pl.multiple_of(z * ROWS, ROWS), ROWS)
                dbuf[c, :HID, columns] = d_stage[...].astype(F32).T[:HID].astype(BF16)
            w_send(kind, z, 0, True, True)
            w_across(kind, z, 0)

    def w_go(steps):
        for event in steps:
            if event == 0:
                w_start()
                continue
            step, kind = (event + 1) // 2, (event + 1) % 2
            k = zz(-step)
            w_wait(kind, k, left)
            w_send(kind, k, step, step < 8, False)
            w_across(kind, k, 2 * step - 1)
            if step < 8:
                k = zz(step)
                w_wait(kind, k, right)
                w_send(kind, k, step, False, step < 7)
                w_across(kind, k, 2 * step)

    def kv_wait(yy, k):
        slot = kv_slot(yy, k)
        push(slot, slot, kvs_z.at[0], kvr.at[yy * NZ + k], right).wait_recv()

    def fold_queries():
        for j in range(1, NT):
            t = (tp + j) % NT
            push(qbuf.at[t], qbuf.at[t], qs.at[0], qr.at[t], tp_peer(t)).wait_recv()
        ready("key_up")
        wide[...] = key_up_v[...].astype(F32)
        for h in range(NT):
            up_h = wide[pl.ds(h, 256, stride=NT)].astype(BF16)
            folded = dot_nt(qbuf[h, :, :128], up_h).astype(BF16)
            folded = folded.reshape(NX, NC, SHARE, 256)
            rope = qbuf[h, :, 128:].reshape(NX, NC, SHARE, 128)
            for core in range(NC):
                r = slice(core * 128 + h % 2 * 64, core * 128 + h % 2 * 64 + 64)
                qf[h // 2, r, :256] = folded[:, core].reshape(64, 256)
                qf[h // 2, r, 256:] = rope[:, core].reshape(64, 128)

    def split_values():
        ready("value_up")
        wide[...] = value_up_v[...].astype(F32)
        for h in range(NT):
            vu[h // 2, h % 2 * 128 : h % 2 * 128 + 128] = wide[pl.ds(h, 256, stride=NT)].T.astype(BF16)

    for d in range(1, 9):
        if d == 4:
            fold_queries()
        if d == 6:
            split_values()
        k = zz(-d)
        kv_wait(y, k)
        if d + 2 <= 8:
            kv_to(k, 3 + d, right2)
        if d < 8:
            k2 = zz(d)
            kv_wait(y, k2)
            if d + 2 <= 7:
                kv_to(k2, 9 + d, left2)
        kv_to_y(k, 2 * d - 1)
        if d < 8:
            kv_to_y(k2, 2 * d)
        if d in W_AT:
            w_go(W_AT[d])
    for j in range(1, NY):
        yy = (y + j) % NY

        @pl.loop(0, NZ)
        def _(k):
            kv_wait(yy, k)

        if j in W_KVY:
            w_go(W_KVY[j])

    kvt[...] = kvbuf[:, :256].T
    lane = lax.broadcasted_iota(jnp.int32, (128, 256), 1)
    for i in range(NX):
        hp = (x + 1 + i) % NX
        s_now = s_scr.at[i % 2]
        s_now[...] = dot_nt(kvbuf[...], qf[hp])
        top = jnp.max(s_now[...], axis=0, keepdims=True)
        weights = jnp.exp((s_now[...] - top) * scale)
        total = jnp.sum(weights, axis=0, keepdims=True)
        mixed = dot_nn(kvt[...], weights.astype(BF16))
        mixed = dot_nn(vu[hp], mixed.astype(BF16))
        mixed = jnp.where((lane & 64) == 0, mixed[:128], mixed[128:]).astype(BF16)
        for core in range(NC):
            t = hp * NC + core
            at = slice(core * 128, core * 128 + 128)
            o_send[t] = mixed[:, at]
            st_send[t, 0:1] = top[:, at]
            st_send[t, 1:2] = total[:, at]
        if i < NX - 1:
            for core in range(NC):
                t = hp * NC + core
                j = i * NC + core
                go(push(st_send.at[t], stats.at[tp], sts.at[j], str_.at[tp], tp_peer(t)))
                go(push(o_send.at[t], o_recv.at[tp], os_.at[j], or_.at[tp], tp_peer(t)))
        else:
            t = x * NC + 1 - c
            go(push(st_send.at[t], stats.at[tp], sts.at[6], str_.at[tp], partner))
            go(push(o_send.at[t], o_recv.at[tp], os_.at[6], or_.at[tp], partner))
            o_recv[tp] = o_send[tp]
            stats[tp] = st_send[tp]
        if i in W_ATTN:
            w_go(W_ATTN[i])
    w_go(W_MORE[0])
    push(owbuf.at[1 - c], owbuf.at[1 - c], ows.at[0], owr.at[0], partner).wait_recv()
    for j in range(1, NT):
        t = (tp + j) % NT
        push(stats.at[t], stats.at[t], sts.at[0], str_.at[t], tp_peer(t)).wait_recv()
        push(o_recv.at[t], o_recv.at[t], os_.at[0], or_.at[t], tp_peer(t)).wait_recv()
    top_all = stats[0, 0:1]
    for t in range(1, NT):
        top_all = jnp.maximum(top_all, stats[t, 0:1])
    total_all = jnp.zeros_like(top_all)
    attended = jnp.zeros((128, 128), F32)
    for t in range(NT):
        factor = jnp.exp((stats[t, 0:1] - top_all) * scale)
        total_all += factor * stats[t, 1:2]
        attended += factor * o_recv[t].astype(F32)
    attended = (attended / total_all).T.astype(BF16)
    r_send[...] = (
        dot_nn(attended[:64], owbuf[0]) + dot_nn(attended[64:], owbuf[1])
    ).astype(BF16)
    for j in range(1, NX):
        xx = (x + j) % NX
        src = r_send.at[pl.ds(pl.multiple_of(xx * SHARE, SHARE), SHARE)]
        go(push(src, r_recv.at[x], rss.at[j - 1], rsr.at[x], (z, y, xx, c)))
    r_recv[x] = r_send[pl.ds(pl.multiple_of(x * SHARE, SHARE), SHARE)]
    w_go(W_MORE[1])
    for j in range(1, NX):
        xx = (x + j) % NX
        push(r_recv.at[xx], r_recv.at[xx], rss.at[0], rsr.at[xx], (z, y, xx, c)).wait_recv()
    ready("resid", "post", "pre", "ffn")
    summed = r_recv[0].astype(F32)
    for j in range(1, NX):
        summed += r_recv[j].astype(F32)
    summed = summed.astype(BF16).astype(F32)
    flow = (resid_v[...].astype(F32) + rms_norm(summed, in_one_row(gains.at[0]))).astype(BF16).astype(F32)
    stream[...] = flow
    in_send[...] = rms_norm(flow, in_one_row(gains.at[1])).astype(BF16)

    def in_slot(s):
        return inbuf.at[pl.ds(pl.multiple_of(s * SHARE, SHARE), SHARE)]

    mine = (y % 2) * NT + tp

    def ag_copy(j):
        chip = (y * NX + x + j) % (NY * NX)
        dev = (z, chip // NX, chip % NX, half)
        return push(in_send, in_slot(mine), ags.at[j], agr.at[mine], dev)

    @pl.loop(1, NY * NX)
    def _(j):
        ag_copy(j).start()

    @pl.when(half == c)
    def _():
        in_slot(mine)[...] = in_send[...]

    @pl.when(half != c)
    def _():
        ag_copy(0).start()

    w_go(W_MORE[2])

    ready("conv_value", "conv_gate")
    last = conv_v.shape[2] - UP
    for core in range(NC):
        first = (x * NC + core) * NY * HID + y * HID
        base = jnp.minimum(first // 128 * 128, last)
        lanes = pl.ds(pl.multiple_of(base, 128), UP)
        back = UP - (first - base)
        v = pltpu.roll(conv_v[0, :, lanes].astype(F32), back, 1)
        g = pltpu.roll(conv_v[1, :, lanes].astype(F32), back, 1)
        taps[core, 0:3] = jnp.concatenate(side_lanes(v[:, :HID], g[:, :HID]), axis=1)

    @pl.loop(0, NZ)
    def _(k):
        slot = w_slot(0, 1 - c, k)
        push(slot, slot, wps.at[0, 0], wpr.at[0, k], partner).wait_recv()

    own_slot = jnp.where(half == c, mine, -1)

    @pl.loop(0, 16)
    def _(s):
        @pl.when(s != own_slot)
        def _():
            push(in_slot(s), in_slot(s), ags.at[0], agr.at[s], partner).wait_recv()

    for core in range(NC):
        up[core, 8 : 8 + TOK] = dot_nn(inbuf[...], wbuf[core])

    low_dev = ((z + c) % NZ, y, x, 1 - c)
    high_dev = ((z + c - 1 + NZ) % NZ, y, x, 1 - c)
    go(push(up.at[:, pl.ds(TOK, 8)], up.at[:, pl.ds(0, 8)], hs.at[0], hr.at[0], low_dev))
    go(push(up.at[:, pl.ds(8, 8)], up.at[:, pl.ds(TOK + 8, 8)], hs.at[1], hr.at[1], high_dev))
    def hidden_rows(core, first, count):
        conv = (
            up[core, first + 7 : first + 7 + count] * taps[core, 0:1]
            + up[core, first + 8 : first + 8 + count] * taps[core, 1:2]
            + up[core, first + 9 : first + 9 + count] * taps[core, 2:3]
        )
        gate = conv[:, 128:256]
        near = gate / (1.0 + jnp.exp(-gate)) * conv[:, :128]
        gate = pltpu.roll(conv[:, 256:], 64, 1)
        far = gate / (1.0 + jnp.exp(-gate)) * conv[:, 256:]
        lane = lax.broadcasted_iota(jnp.int32, far.shape, 1)
        far = jnp.where(lane < 64, far, 0.0)
        return jnp.concatenate([near.astype(BF16), far.astype(BF16)], axis=1)

    def down_rows(hidden):
        return (dot_nn(hidden[0], dbuf[0]) + dot_nn(hidden[1], dbuf[1])).astype(BF16)

    inner = [hidden_rows(core, SHARE, TOK - 2 * SHARE) for core in range(NC)]
    @pl.loop(0, NZ)
    def _(k):
        slot = w_slot(1, 1 - c, k)
        push(slot, slot, wps.at[1, 0], wpr.at[1, k], partner).wait_recv()

    p_send[SHARE : TOK - SHARE] = down_rows(inner)

    chip = y * NX + x

    def p_slot(s):
        return p_send.at[pl.ds(pl.multiple_of(s * SHARE, SHARE), SHARE)]

    def rs_copy(s):
        dev = (z, 2 * c + s // NT, (s // NC) % NX, s % NC)
        return push(p_slot(s), p_recv.at[chip], ps.at[s], pr.at[chip], dev)

    @pl.loop(0, 16)
    def _(j):
        s = (mine + j) % 16

        @pl.when((s != own_slot) & (s > 0) & (s < 15))
        def _():
            rs_copy(s).start()

    low, high = up.at[:, pl.ds(0, 8)], up.at[:, pl.ds(TOK + 8, 8)]
    push(low, low, hs.at[0], hr.at[0], low_dev).wait_recv()
    push(high, high, hs.at[1], hr.at[1], high_dev).wait_recv()

    @pl.when((z == 0) & (c == 0))
    def _():
        up[:, 0:8] = jnp.zeros((NC, 8, UP), F32)

    @pl.when((z == NZ - 1) & (c == 1))
    def _():
        up[:, TOK + 8 : TOK + 16] = jnp.zeros((NC, 8, UP), F32)

    outer = [
        jnp.concatenate(
            [hidden_rows(core, 0, SHARE), hidden_rows(core, TOK - SHARE, SHARE)], axis=0
        )
        for core in range(NC)
    ]
    edges = down_rows(outer)
    p_send[:SHARE] = edges[:SHARE]
    p_send[TOK - SHARE :] = edges[SHARE:]
    for s in (0, 15):

        @pl.when(s != own_slot)
        def _():
            rs_copy(s).start()


    @pl.when(half == c)
    def _():
        p_recv[chip] = p_slot(mine)[...]

    own_chip = jnp.where(half == c, chip, -1)

    @pl.loop(0, 16)
    def _(k):
        @pl.when(k != own_chip)
        def _():
            push(p_recv.at[k], p_recv.at[k], ps.at[0], pr.at[k], partner).wait_recv()

    projected = p_recv[0].astype(F32)
    for k in range(1, 16):
        projected += p_recv[k].astype(F32)
    projected = projected.astype(BF16).astype(F32)
    out[...] = (stream[...] + rms_norm(projected, in_one_row(gains.at[2]))).astype(BF16)

    for copy in pending:
        copy.wait_send()

    @pl.loop(1, NY * NX)
    def _(j):
        ag_copy(j).wait_send()

    @pl.when(half != c)
    def _():
        ag_copy(0).wait_send()

    @pl.loop(0, 16)
    def _(s):
        @pl.when(s != own_slot)
        def _():
            rs_copy(s).wait_send()


def body(
    residual,
    query_nope,
    query_rope,
    latent,
    rope_key,
    kv_gain,
    key_up,
    value_up,
    out_weight,
    post_gain,
    pre_gain,
    ffn_gain,
    up_value,
    up_gate,
    conv_value,
    conv_gate,
    down_weight,
):
    scale = (query_nope.shape[2] + query_rope.shape[2]) ** (-0.5)
    by_row, by_col = turn_tables()

    dma = pltpu.SemaphoreType.DMA
    vmem = pltpu.VMEM
    return pl.pallas_call(
        functools.partial(layer_kernel, scale),
        out_shape=jax.ShapeDtypeStruct((SHARE, D), BF16),
        in_specs=[pl.BlockSpec(memory_space=pl.ANY)] * 19,
        out_specs=pl.BlockSpec(memory_space=vmem),
        scratch_shapes=[
            vmem((KEYS, KW), BF16),
            vmem((NT, ROWS, QW), BF16),
            vmem((NC, NZ * ROWS, UP), BF16),
            vmem((NC, 256, D), BF16),
            vmem((ROWS, 256), BF16),
            vmem((NC, 128, D), BF16),
            vmem((256, KEYS), BF16),
            vmem((2, KEYS, 256), F32),
            vmem((NT, 8, 128), F32),
            vmem((NT, 8, 128), F32),
            vmem((NT, 128, 128), BF16),
            vmem((NT, 128, 128), BF16),
            vmem((64, D), BF16),
            vmem((NX, SHARE, D), BF16),
            vmem((SHARE, D), BF16),
            vmem((TOK, D), BF16),
            vmem((NC, TOK + 16, UP), F32),
            vmem((TOK, D), BF16),
            vmem((NY * NX, SHARE, D), BF16),
            vmem((SHARE, D), F32),
            vmem((SHARE, 256), BF16),
            vmem((64, ROWS), BF16),
            vmem((ROWS, 128), BF16),
            vmem((64, ROWS), BF16),
            vmem((8, 128), F32),
            vmem((2, GRID, 128), F32),
            vmem(up_value.shape, BF16),
            vmem(up_gate.shape, BF16),
            vmem(down_weight.shape[::-1], BF16),
            vmem((256 * NT, 128), BF16),
            vmem((256 * NT, 128), BF16),
            vmem((SHARE, D), BF16),
            vmem((2, 128), BF16),
            vmem((3, D // 128, 128), BF16),
            vmem((2,) + conv_value.shape, BF16),
            vmem((2, ROWS, 128), F32),
            vmem((ROWS, 128), F32),
            vmem((NY, 32, UP), BF16),
            vmem((NY, 32, 256), BF16),
            vmem((256 * NT, 128), F32),
            vmem((4, 256, KW), BF16),
            vmem((4, 256, 256), BF16),
            vmem((NC, 8, UP), F32),
        ]
        + [dma((n,)) for n in (19, 15, 48, 64, 7, 8, 6, 8)]
        + [dma((2, 16))] * 4
        + [
            dma((n,))
            for n in (1, 1, 7, 8, 7, 8, 3, 4, 16, 16, 2, 2, 16, 16)
        ],
        compiler_params=pltpu.CompilerParams(
            collective_id=0, has_side_effects=True, vmem_limit_bytes=60 * 1024 * 1024
        ),
        name="layer",
    )(
        latent,
        rope_key.T,
        query_nope[:, 0],
        query_rope[:, 0].T,
        by_row,
        by_col,
        up_value,
        up_gate,
        down_weight.T,
        out_weight,
        key_up.reshape(-1, key_up.shape[2]),
        value_up.reshape(-1, value_up.shape[2]),
        residual,
        kv_gain.reshape(-1, 128),
        post_gain.reshape(-1, 128),
        pre_gain.reshape(-1, 128),
        ffn_gain.reshape(-1, 128),
        conv_value,
        conv_gate,
    )


def solution(mesh):
    torus = Mesh(mesh.devices.reshape(NZ, NY, NX, NC), AXES)
    return jax.shard_map(
        body,
        mesh=torus,
        in_specs=(
            P(SP, None),
            P(SP, TP, None),
            P(SP, TP, None),
            P(SP, None),
            P(SP, None),
            P(),
            P(),
            P(),
            P(TP, None),
            P(),
            P(),
            P(),
            P(SP, TP),
            P(SP, TP),
            P(),
            P(),
            P(TP, SP),
        ),
        out_specs=P(SP + TP, None),
        check_vma=False,
    )
```

```python
import functools

import jax
import jax.numpy as jnp
import numpy as np
from jax import lax
from jax.experimental import pallas as pl
from jax.experimental.pallas import tpu as pltpu
from jax.sharding import Mesh
from jax.sharding import PartitionSpec as P

GRID = 64
AXES = ("z", "y", "x", "c")
SP = ("z", "y")
TP = ("x", "c")
MESH_IDS = pl.DeviceIdType.MESH
F32 = jnp.float32
BF16 = jnp.bfloat16

epsilon = 1e-06
rope_base = 10000.0

NZ, NY, NX, NC = 16, 4, 4, 2
NT = NX * NC
PLANE = NY * NT
D = 2048
ROWS = 128
SHARE = 16
KEYS = NZ * NY * SHARE
QW = 256
KW = 384
UP = 384
HID = 176
W_AT = {2: [0], 6: [1], 8: [2]}
W_NEAR = {1: [3], 3: [4]}
W_ATTN = {1: [5], 3: [6]}
W_MORE = ([7, 8], [9, 10], [11, 12, 13, 14, 15, 16])
NEAR = (-4, 6)
TOK = 256


def rms_norm(values, gain):
    return (
        values * lax.rsqrt(jnp.mean(values * values, axis=-1, keepdims=True) + epsilon) * gain
    )


def turn_tables():
    pairs = 16
    frequency = rope_base ** (-np.arange(pairs) / pairs)
    sign = np.repeat([-1.0, 1.0], pairs)

    def both(steps, at):
        angles = np.tile(np.arange(steps)[:, None] * frequency, (1, 2))
        table = np.zeros((2, steps, 128))
        table[0, :, at : at + 32] = np.cos(angles)
        table[1, :, at : at + 32] = np.sin(angles) * sign
        return table

    by_row = both(ROWS // GRID * NZ * NY, 0).reshape(2, NZ * NY, ROWS // GRID, 128)
    by_row = by_row.transpose(1, 0, 2, 3).reshape(NZ * NY, 2 * ROWS // GRID, 128)
    by_row = np.pad(by_row, ((0, 0), (0, 8 - 2 * ROWS // GRID), (0, 0)))
    return by_row.astype(np.float32), both(GRID, 32).astype(np.float32)


def turned(values, cosine, sine):
    lane = lax.broadcasted_iota(jnp.int32, values.shape, 1)
    other = jnp.where((lane & 16) == 0, pltpu.roll(values, 112, 1), pltpu.roll(values, 16, 1))
    return values * cosine + other * sine


def in_one_row(ref):
    folded = ref[...].astype(F32)
    return jnp.concatenate([folded[i : i + 1] for i in range(folded.shape[0])], axis=1)


def as_rows(columns):
    both = jnp.concatenate([columns.astype(F32), jnp.zeros(columns.shape, F32)], axis=0)
    return both.T


def dot_nn(a, b):
    return jnp.dot(a, b, preferred_element_type=F32)


def dot_nt(a, b):
    return lax.dot_general(a, b, (((1,), (1,)), ((), ())), preferred_element_type=F32)


def side_lanes(v, g):
    rest = HID - 128
    pad = jnp.zeros(v.shape[:-1] + (64 - rest,), v.dtype)
    return [v[:, :128], g[:, :128], v[:, 128:], pad, g[:, 128:], pad]


def layer_kernel(
    scale,
    latent,
    rope_key,
    q_nope,
    q_rope,
    by_row,
    by_col,
    up_value,
    up_gate,
    down,
    ow,
    key_up,
    value_up,
    resid,
    kv_gain,
    post_gain,
    pre_gain,
    ffn_gain,
    conv_value,
    conv_gate,
    out,
    kvbuf,
    qbuf,
    wbuf,
    dbuf,
    d_stage,
    owbuf,
    kvt,
    s_scr,
    near_stats,
    near_mixed,
    st_send,
    stats,
    o_send,
    o_recv,
    r_send,
    r_recv,
    in_send,
    inbuf,
    up,
    p_send,
    p_recv,
    stream,
    latent_v,
    rope_key_v,
    q_nope_v,
    q_rope_v,
    by_row_v,
    by_col_v,
    up_value_v,
    up_gate_v,
    down_v,
    key_up_v,
    value_up_v,
    resid_v,
    kv_gain_v,
    gains,
    conv_v,
    turns,
    key_rows,
    w_loc,
    d_loc,
    wide,
    qf,
    vu,
    taps,
    loads,
    unused,
    kvs,
    kvr,
    qs,
    qr,
    wys,
    wyr,
    wzs,
    wps,
    wzr,
    wpr,
    ows,
    owr,
    sts,
    str_,
    os_,
    or_,
    rss,
    rsr,
    ags,
    agr,
    hs,
    hr,
    ps,
    pr,
):
    z, y, x, c = (lax.axis_index(a) for a in AXES)
    tp = x * NC + c
    plane = y * NT + tp
    half = y // 2

    def zz(k):
        return (z + k + NZ) % NZ

    def push(src, dst, ss, rs, dev):
        return pltpu.make_async_remote_copy(
            src_ref=src, dst_ref=dst, send_sem=ss, recv_sem=rs, device_id=dev,
            device_id_type=MESH_IDS,
        )

    partner = (z, y, x, 1 - c)
    right, left = (zz(1), y, x, c), (zz(-1), y, x, c)
    right2, left2 = (zz(2), y, x, c), (zz(-2), y, x, c)
    cross = ((z + 2 * c - 1 + NZ) % NZ, y, x, 1 - c)

    def on_plane(j):
        p = (plane + j) % PLANE
        return (z, p // NT, (p // NC) % NX, p % NC)

    def tp_peer(t):
        return (z, y, t // NC, t % NC)

    def own(ref):
        return ref.at[pl.ds(pl.multiple_of(tp * SHARE, SHARE), SHARE)]

    local = {}

    def load(name, src, dst):
        local[name] = pltpu.make_async_copy(src, dst, loads.at[len(local)])
        local[name].start()

    load("latent", own(latent), latent_v)
    load("rope_key", rope_key, rope_key_v)
    load("by_row", by_row.at[z * NY + y], by_row_v)
    load("by_col", by_col, by_col_v)
    load("kv_gain", kv_gain, kv_gain_v)
    load("post", post_gain, gains.at[0])
    load("pre", pre_gain, gains.at[1])
    load("ffn", ffn_gain, gains.at[2])
    load("q_nope", q_nope, q_nope_v)
    load("q_rope", q_rope, q_rope_v)
    load("up_value", up_value, up_value_v)
    load("up_gate", up_gate, up_gate_v)
    load("down", down, down_v)
    load("ow", ow, owbuf.at[c])
    load("key_up", key_up, key_up_v)
    load("value_up", value_up, value_up_v)
    load("resid", own(resid), resid_v)
    load("conv_value", conv_value, conv_v.at[0])
    load("conv_gate", conv_gate, conv_v.at[1])

    def ready(*names):
        for name in names:
            local[name].wait()

    barrier = pltpu.get_barrier_semaphore()
    for dev in (right, left, right2, left2, cross):
        pl.semaphore_signal(barrier, inc=1, device_id=dev, device_id_type=MESH_IDS)

    @pl.loop(1, PLANE)
    def _(j):
        pl.semaphore_signal(barrier, inc=1, device_id=on_plane(j), device_id_type=MESH_IDS)

    def kv_slot(yy, d):
        start = pl.multiple_of(((d + 8) * NY + yy) * SHARE, SHARE)
        return kvbuf.at[pl.ds(start, SHARE)]

    def w_slot(kind, core, k):
        at = pl.ds(pl.multiple_of(k * ROWS, ROWS), ROWS)
        if kind == 0:
            return wbuf.at[core, at]
        return dbuf.at[core, pl.ds(0, HID), at]

    def w_part(kind, yy):
        if kind == 0:
            return wbuf.at[c, pl.ds(pl.multiple_of(z * ROWS + yy * 32, 32), 32)]
        return d_stage.at[pl.ds(pl.multiple_of(yy * 32, 32), 32)]

    ready("latent", "rope_key", "by_row", "by_col", "kv_gain")
    for i in range(2):
        grid_rows = [
            by_row_v[2 * i + j : 2 * i + j + 1] + by_col_v[i] for j in range(ROWS // GRID)
        ]
        turns[i] = jnp.concatenate(grid_rows, axis=0)
    rows = pl.ds(pl.multiple_of(tp * SHARE, SHARE), SHARE)
    kv_slot(y, 0)[:, :256] = rms_norm(
        latent_v[...].astype(F32), in_one_row(kv_gain_v)
    ).astype(BF16)
    key_rows[...] = as_rows(rope_key_v[...])
    kv_slot(y, 0)[:, 256:] = turned(key_rows[rows], turns[0, rows], turns[1, rows]).astype(BF16)

    pl.semaphore_wait(barrier, 5 + PLANE - 1)

    def go(copy):
        copy.start()

    def kv_to(d, hop, dev):
        seen = d - hop
        go(push(kv_slot(y, d), kv_slot(y, seen), kvs.at[0], kvr.at[seen + 8], dev))

    def kv_to_y(d):
        slot = kv_slot(y, d)
        for j in range(1, NY):
            dev = (z, (y + j) % NY, x, c)
            go(push(slot, slot, kvs.at[0], kvr.at[16 if NEAR[0] <= d < NEAR[1] else 17], dev))

    kv_to(0, 2, right2)
    kv_to(0, -2, left2)
    kv_to(0, 1, right)
    kv_to(0, -1, left)
    kv_to_y(0)
    ready("q_nope", "q_rope")
    qbuf[tp, :, :128] = q_nope_v[...]
    qbuf[tp, :, 128:] = turned(as_rows(q_rope_v[...]), turns[0], turns[1]).astype(BF16)
    for j in range(1, NT):
        t = (tp + j) % NT
        go(push(qbuf.at[tp], qbuf.at[tp], qs.at[0], qr.at[0], tp_peer(t)))

    ready("up_value", "up_gate", "down")
    value, gate = up_value_v[...].astype(F32), up_gate_v[...].astype(F32)
    across = down_v[...].astype(F32)
    for yy in range(NY):
        at = slice(yy * HID, (yy + 1) * HID)
        parts = side_lanes(value[:, at], gate[:, at])
        w_loc[yy] = jnp.concatenate(parts, axis=1).astype(BF16)
        parts = [across[:, at], jnp.zeros((32, 256 - HID), F32)]
        d_loc[yy] = jnp.concatenate(parts, axis=1).astype(BF16)
    for j in range(1, NY):
        yy = (y + j) % NY
        dev = (z, yy, x, c)
        go(push(w_loc.at[yy], w_part(0, y), wys.at[0], wyr.at[0], dev))
        go(push(d_loc.at[yy], w_part(1, y), wys.at[1], wyr.at[1], dev))
    w_part(0, y)[...] = w_loc[y]
    w_part(1, y)[...] = d_loc[y]
    dbuf[:, HID:] = jnp.zeros((NC, 256 - HID, D), BF16)
    ready("ow")
    go(push(owbuf.at[c], owbuf.at[c], ows.at[0], owr.at[0], partner))

    def w_send(kind, k, to_right, to_left):
        slot = w_slot(kind, c, k)
        if to_right:
            go(push(slot, slot, wzs.at[kind], wzr.at[kind, k], right))
        if to_left:
            go(push(slot, slot, wzs.at[kind], wzr.at[kind, k], left))

    def w_across(kind, k):
        slot = w_slot(kind, c, k)
        go(push(slot, slot, wps.at[kind], wpr.at[kind], partner))

    def w_wait(kind, k, dev):
        slot = w_slot(kind, c, k)
        push(slot, slot, wzs.at[kind], wzr.at[kind, k], dev).wait_recv()

    def w_start():
        for kind in range(2):
            landed((wbuf.at[c] if kind == 0 else d_stage).at[pl.ds(0, 96)], wyr.at[kind])
            if kind == 1:
                columns = pl.ds(pl.multiple_of(z * ROWS, ROWS), ROWS)
                dbuf[c, :HID, columns] = d_stage[...].astype(F32).T[:HID].astype(BF16)
            w_send(kind, z, True, True)
            w_across(kind, z)

    def w_go(steps):
        for event in steps:
            if event == 0:
                w_start()
                continue
            step, kind = (event + 1) // 2, (event + 1) % 2
            k = zz(-step)
            w_wait(kind, k, left)
            w_send(kind, k, step < 8, False)
            w_across(kind, k)
            if step < 8:
                k = zz(step)
                w_wait(kind, k, right)
                w_send(kind, k, False, step < 7)
                w_across(kind, k)

    def kv_wait(d):
        slot = kv_slot(y, d)
        push(slot, slot, kvs.at[0], kvr.at[d + 8], right).wait_recv()

    def landed(ref, sem):
        push(ref, ref, unused.at[0], sem, partner).wait_recv()

    def left_here(ref, sem):
        push(ref, ref, sem, unused.at[0], partner).wait_send()

    def fold_queries():
        landed(qbuf.at[pl.ds(0, NT - 1)], qr.at[0])
        ready("key_up")
        wide[...] = key_up_v[...].astype(F32)
        for h in range(NT):
            up_h = wide[pl.ds(h, 256, stride=NT)].astype(BF16)
            folded = dot_nt(qbuf[h, :, :128], up_h).astype(BF16)
            folded = folded.reshape(NX, NC, SHARE, 256)
            rope = qbuf[h, :, 128:].reshape(NX, NC, SHARE, 128)
            for core in range(NC):
                r = slice(core * 128 + h % 2 * 64, core * 128 + h % 2 * 64 + 64)
                qf[h // 2, r, :256] = folded[:, core].reshape(64, 256)
                qf[h // 2, r, 256:] = rope[:, core].reshape(64, 128)

    def split_values():
        ready("value_up")
        wide[...] = value_up_v[...].astype(F32)
        for h in range(NT):
            vu[h // 2, h % 2 * 128 : h % 2 * 128 + 128] = wide[pl.ds(h, 256, stride=NT)].T.astype(BF16)

    for d in range(1, 9):
        if d == 4:
            fold_queries()
        if d == 6:
            split_values()
        kv_wait(-d)
        if d + 2 <= 8:
            kv_to(-d, 2, right2)
        if d < 8:
            kv_wait(d)
            if d + 2 <= 7:
                kv_to(d, -2, left2)
        kv_to_y(-d)
        if d < 8:
            kv_to_y(d)
        if d in W_AT:
            w_go(W_AT[d])
    def weigh(hp, i, spans, top):
        s_now = s_scr.at[i % 2]
        for at in spans:
            s_now[at] = dot_nt(kvbuf[at], qf[hp])
            here = jnp.max(s_now[at], axis=0, keepdims=True)
            top = here if top is None else jnp.maximum(top, here)
        total, mixed = 0.0, 0.0
        for at in spans:
            weights = jnp.exp((s_now[at] - top) * scale)
            total += jnp.sum(weights, axis=0, keepdims=True)
            mixed += dot_nn(kvt[:, at], weights.astype(BF16))
        return top, total, mixed

    near, far = [slice(256, 896)], [slice(0, 256), slice(896, KEYS)]
    landed(kvbuf.at[pl.ds(0, (NEAR[1] - NEAR[0]) * 3 * SHARE)], kvr.at[16])
    for at in near:
        kvt[:, at] = kvbuf[at, :256].T
    for i in range(NX):
        hp = (x + 1 + i) % NX
        top, total, mixed = weigh(hp, i, near, None)
        near_stats[i, 0:1] = top
        near_stats[i, 1:2] = total
        near_mixed[i] = mixed
        if i in W_NEAR:
            w_go(W_NEAR[i])
    landed(kvbuf.at[pl.ds(0, (NZ - NEAR[1] + NEAR[0]) * 3 * SHARE)], kvr.at[17])
    for at in far:
        kvt[:, at] = kvbuf[at, :256].T
    lane = lax.broadcasted_iota(jnp.int32, (128, 256), 1)
    for i in range(NX):
        hp = (x + 1 + i) % NX
        top_near = near_stats[i, 0:1]
        top, total, mixed = weigh(hp, i, far, top_near)
        factor = jnp.exp((top_near - top) * scale)
        total += factor * near_stats[i, 1:2]
        mixed += factor * near_mixed[i]
        mixed = dot_nn(vu[hp], mixed.astype(BF16))
        mixed = jnp.where((lane & 64) == 0, mixed[:128], mixed[128:]).astype(BF16)
        for core in range(NC):
            t = hp * NC + core
            at = slice(core * 128, core * 128 + 128)
            o_send[t] = mixed[:, at]
            st_send[t, 0:1] = top[:, at]
            st_send[t, 1:2] = total[:, at]
        if i < NX - 1:
            for core in range(NC):
                t = hp * NC + core
                go(push(st_send.at[t], stats.at[tp], sts.at[0], str_.at[0], tp_peer(t)))
                go(push(o_send.at[t], o_recv.at[tp], os_.at[0], or_.at[0], tp_peer(t)))
        else:
            t = x * NC + 1 - c
            go(push(st_send.at[t], stats.at[tp], sts.at[0], str_.at[0], partner))
            go(push(o_send.at[t], o_recv.at[tp], os_.at[0], or_.at[0], partner))
            o_recv[tp] = o_send[tp]
            stats[tp] = st_send[tp]
        if i in W_ATTN:
            w_go(W_ATTN[i])
    w_go(W_MORE[0])
    push(owbuf.at[1 - c], owbuf.at[1 - c], ows.at[0], owr.at[0], partner).wait_recv()
    landed(stats.at[pl.ds(0, NT - 1)], str_.at[0])
    landed(o_recv.at[pl.ds(0, NT - 1)], or_.at[0])
    top_all = stats[0, 0:1]
    for t in range(1, NT):
        top_all = jnp.maximum(top_all, stats[t, 0:1])
    total_all = jnp.zeros_like(top_all)
    attended = jnp.zeros((128, 128), F32)
    for t in range(NT):
        factor = jnp.exp((stats[t, 0:1] - top_all) * scale)
        total_all += factor * stats[t, 1:2]
        attended += factor * o_recv[t].astype(F32)
    attended = (attended / total_all).T.astype(BF16)
    r_send[...] = (
        dot_nn(attended[:64], owbuf[0]) + dot_nn(attended[64:], owbuf[1])
    ).astype(BF16)
    for j in range(1, NX):
        xx = (x + j) % NX
        src = r_send.at[pl.ds(pl.multiple_of(xx * SHARE, SHARE), SHARE)]
        go(push(src, r_recv.at[x], rss.at[0], rsr.at[0], (z, y, xx, c)))
    r_recv[x] = r_send[pl.ds(pl.multiple_of(x * SHARE, SHARE), SHARE)]
    w_go(W_MORE[1])
    landed(r_recv.at[pl.ds(0, NX - 1)], rsr.at[0])
    ready("resid", "post", "pre", "ffn")
    summed = r_recv[0].astype(F32)
    for j in range(1, NX):
        summed += r_recv[j].astype(F32)
    summed = summed.astype(BF16).astype(F32)
    flow = (resid_v[...].astype(F32) + rms_norm(summed, in_one_row(gains.at[0]))).astype(BF16).astype(F32)
    stream[...] = flow
    in_send[...] = rms_norm(flow, in_one_row(gains.at[1])).astype(BF16)

    def in_slot(s):
        return inbuf.at[pl.ds(pl.multiple_of(s * SHARE, SHARE), SHARE)]

    mine = (y % 2) * NT + tp

    def ag_copy(j):
        chip = (y * NX + x + j) % (NY * NX)
        dev = (z, chip // NX, chip % NX, half)
        return push(in_send, in_slot(mine), ags.at[0], agr.at[0], dev)

    @pl.loop(1, NY * NX)
    def _(j):
        ag_copy(j).start()

    @pl.when(half == c)
    def _():
        in_slot(mine)[...] = in_send[...]

    @pl.when(half != c)
    def _():
        ag_copy(0).start()

    w_go(W_MORE[2])

    ready("conv_value", "conv_gate")
    last = conv_v.shape[2] - UP
    for core in range(NC):
        first = (x * NC + core) * NY * HID + y * HID
        base = jnp.minimum(first // 128 * 128, last)
        lanes = pl.ds(pl.multiple_of(base, 128), UP)
        back = UP - (first - base)
        v = pltpu.roll(conv_v[0, :, lanes].astype(F32), back, 1)
        g = pltpu.roll(conv_v[1, :, lanes].astype(F32), back, 1)
        taps[core, 0:3] = jnp.concatenate(side_lanes(v[:, :HID], g[:, :HID]), axis=1)

    landed(wbuf.at[1 - c], wpr.at[0])

    own_slot = jnp.where(half == c, mine, -1)

    @pl.when(half == c)
    def _():
        landed(inbuf.at[pl.ds(0, 15 * SHARE)], agr.at[0])

    @pl.when(half != c)
    def _():
        landed(inbuf, agr.at[0])

    for core in range(NC):
        up[core, 8 : 8 + TOK] = dot_nn(inbuf[...], wbuf[core])

    low_dev = ((z + c) % NZ, y, x, 1 - c)
    high_dev = ((z + c - 1 + NZ) % NZ, y, x, 1 - c)
    go(push(up.at[:, pl.ds(TOK, 8)], up.at[:, pl.ds(0, 8)], hs.at[0], hr.at[0], low_dev))
    go(push(up.at[:, pl.ds(8, 8)], up.at[:, pl.ds(TOK + 8, 8)], hs.at[1], hr.at[1], high_dev))
    def hidden_rows(core, first, count):
        conv = (
            up[core, first + 7 : first + 7 + count] * taps[core, 0:1]
            + up[core, first + 8 : first + 8 + count] * taps[core, 1:2]
            + up[core, first + 9 : first + 9 + count] * taps[core, 2:3]
        )
        gate = conv[:, 128:256]
        near = gate / (1.0 + jnp.exp(-gate)) * conv[:, :128]
        gate = pltpu.roll(conv[:, 256:], 64, 1)
        far = gate / (1.0 + jnp.exp(-gate)) * conv[:, 256:]
        lane = lax.broadcasted_iota(jnp.int32, far.shape, 1)
        far = jnp.where(lane < 64, far, 0.0)
        return jnp.concatenate([near.astype(BF16), far.astype(BF16)], axis=1)

    def down_rows(hidden):
        return (dot_nn(hidden[0], dbuf[0]) + dot_nn(hidden[1], dbuf[1])).astype(BF16)

    inner = [hidden_rows(core, SHARE, TOK - 2 * SHARE) for core in range(NC)]
    landed(dbuf.at[1 - c, pl.ds(0, HID)], wpr.at[1])

    p_send[SHARE : TOK - SHARE] = down_rows(inner)

    chip = y * NX + x

    def p_slot(s):
        return p_send.at[pl.ds(pl.multiple_of(s * SHARE, SHARE), SHARE)]

    def rs_copy(s):
        dev = (z, 2 * c + s // NT, (s // NC) % NX, s % NC)
        return push(p_slot(s), p_recv.at[chip], ps.at[0], pr.at[0], dev)

    @pl.loop(0, 16)
    def _(j):
        s = (mine + j) % 16

        @pl.when((s != own_slot) & (s > 0) & (s < 15))
        def _():
            rs_copy(s).start()

    low, high = up.at[:, pl.ds(0, 8)], up.at[:, pl.ds(TOK + 8, 8)]
    push(low, low, hs.at[0], hr.at[0], low_dev).wait_recv()
    push(high, high, hs.at[1], hr.at[1], high_dev).wait_recv()

    @pl.when((z == 0) & (c == 0))
    def _():
        up[:, 0:8] = jnp.zeros((NC, 8, UP), F32)

    @pl.when((z == NZ - 1) & (c == 1))
    def _():
        up[:, TOK + 8 : TOK + 16] = jnp.zeros((NC, 8, UP), F32)

    outer = [
        jnp.concatenate(
            [hidden_rows(core, 0, SHARE), hidden_rows(core, TOK - SHARE, SHARE)], axis=0
        )
        for core in range(NC)
    ]
    edges = down_rows(outer)
    p_send[:SHARE] = edges[:SHARE]
    p_send[TOK - SHARE :] = edges[SHARE:]
    for s in (0, 15):

        @pl.when(s != own_slot)
        def _():
            rs_copy(s).start()


    @pl.when(half == c)
    def _():
        p_recv[chip] = p_slot(mine)[...]

    @pl.when(half == c)
    def _():
        landed(p_recv.at[pl.ds(0, 15)], pr.at[0])

    @pl.when(half != c)
    def _():
        landed(p_recv, pr.at[0])

    projected = p_recv[0].astype(F32)
    for k in range(1, 16):
        projected += p_recv[k].astype(F32)
    projected = projected.astype(BF16).astype(F32)
    out[...] = (stream[...] + rms_norm(projected, in_one_row(gains.at[2]))).astype(BF16)

    left_here(kvbuf.at[pl.ds(0, 63 * SHARE)], kvs.at[0])
    left_here(qbuf.at[pl.ds(0, NT - 1)], qs.at[0])
    left_here(wbuf.at[0, pl.ds(0, 96)], wys.at[0])
    left_here(d_stage.at[pl.ds(0, 96)], wys.at[1])
    left_here(owbuf.at[0], ows.at[0])
    left_here(wbuf.at[0, pl.ds(0, 15 * ROWS)], wzs.at[0])
    left_here(dbuf.at[0, pl.ds(0, HID), pl.ds(0, 15 * ROWS)], wzs.at[1])
    left_here(wbuf.at[0], wps.at[0])
    left_here(dbuf.at[0, pl.ds(0, HID)], wps.at[1])
    left_here(stats.at[pl.ds(0, NT - 1)], sts.at[0])
    left_here(o_recv.at[pl.ds(0, NT - 1)], os_.at[0])
    left_here(r_recv.at[pl.ds(0, NX - 1)], rss.at[0])
    both = up.at[:, pl.ds(0, 8)]
    left_here(both, hs.at[0])
    left_here(both, hs.at[1])

    @pl.when(half == c)
    def _():
        left_here(inbuf.at[pl.ds(0, 15 * SHARE)], ags.at[0])
        left_here(p_send.at[pl.ds(0, 15 * SHARE)], ps.at[0])

    @pl.when(half != c)
    def _():
        left_here(inbuf, ags.at[0])
        left_here(p_send, ps.at[0])


def body(
    residual,
    query_nope,
    query_rope,
    latent,
    rope_key,
    kv_gain,
    key_up,
    value_up,
    out_weight,
    post_gain,
    pre_gain,
    ffn_gain,
    up_value,
    up_gate,
    conv_value,
    conv_gate,
    down_weight,
):
    scale = (query_nope.shape[2] + query_rope.shape[2]) ** (-0.5)
    by_row, by_col = turn_tables()

    dma = pltpu.SemaphoreType.DMA
    vmem = pltpu.VMEM
    return pl.pallas_call(
        functools.partial(layer_kernel, scale),
        out_shape=jax.ShapeDtypeStruct((SHARE, D), BF16),
        in_specs=[pl.BlockSpec(memory_space=pl.ANY)] * 19,
        out_specs=pl.BlockSpec(memory_space=vmem),
        scratch_shapes=[
            vmem((KEYS, KW), BF16),
            vmem((NT, ROWS, QW), BF16),
            vmem((NC, NZ * ROWS, UP), BF16),
            vmem((NC, 256, D), BF16),
            vmem((ROWS, 256), BF16),
            vmem((NC, 128, D), BF16),
            vmem((256, KEYS), BF16),
            vmem((2, KEYS, 256), F32),
            vmem((NX, 8, 256), F32),
            vmem((NX, 256, 256), F32),
            vmem((NT, 8, 128), F32),
            vmem((NT, 8, 128), F32),
            vmem((NT, 128, 128), BF16),
            vmem((NT, 128, 128), BF16),
            vmem((64, D), BF16),
            vmem((NX, SHARE, D), BF16),
            vmem((SHARE, D), BF16),
            vmem((TOK, D), BF16),
            vmem((NC, TOK + 16, UP), F32),
            vmem((TOK, D), BF16),
            vmem((NY * NX, SHARE, D), BF16),
            vmem((SHARE, D), F32),
            vmem((SHARE, 256), BF16),
            vmem((64, ROWS), BF16),
            vmem((ROWS, 128), BF16),
            vmem((64, ROWS), BF16),
            vmem((8, 128), F32),
            vmem((2, GRID, 128), F32),
            vmem(up_value.shape, BF16),
            vmem(up_gate.shape, BF16),
            vmem(down_weight.shape[::-1], BF16),
            vmem((256 * NT, 128), BF16),
            vmem((256 * NT, 128), BF16),
            vmem((SHARE, D), BF16),
            vmem((2, 128), BF16),
            vmem((3, D // 128, 128), BF16),
            vmem((2,) + conv_value.shape, BF16),
            vmem((2, ROWS, 128), F32),
            vmem((ROWS, 128), F32),
            vmem((NY, 32, UP), BF16),
            vmem((NY, 32, 256), BF16),
            vmem((256 * NT, 128), F32),
            vmem((4, 256, KW), BF16),
            vmem((4, 256, 256), BF16),
            vmem((NC, 8, UP), F32),
        ]
        + [dma((n,)) for n in (19, 1, 1, 18, 1, 1, 2, 2, 2, 2)]
        + [dma((2, NZ))]
        + [dma((n,)) for n in (2, 1, 1, 1, 1, 1, 1, 1, 1, 1, 1, 2, 2, 1, 1)],
        compiler_params=pltpu.CompilerParams(
            collective_id=0, has_side_effects=True, vmem_limit_bytes=60 * 1024 * 1024
        ),
        name="layer",
    )(
        latent,
        rope_key.T,
        query_nope[:, 0],
        query_rope[:, 0].T,
        by_row,
        by_col,
        up_value,
        up_gate,
        down_weight.T,
        out_weight,
        key_up.reshape(-1, key_up.shape[2]),
        value_up.reshape(-1, value_up.shape[2]),
        residual,
        kv_gain.reshape(-1, 128),
        post_gain.reshape(-1, 128),
        pre_gain.reshape(-1, 128),
        ffn_gain.reshape(-1, 128),
        conv_value,
        conv_gate,
    )


def solution(mesh):
    torus = Mesh(mesh.devices.reshape(NZ, NY, NX, NC), AXES)
    return jax.shard_map(
        body,
        mesh=torus,
        in_specs=(
            P(SP, None),
            P(SP, TP, None),
            P(SP, TP, None),
            P(SP, None),
            P(SP, None),
            P(),
            P(),
            P(),
            P(TP, None),
            P(),
            P(),
            P(),
            P(SP, TP),
            P(SP, TP),
            P(),
            P(),
            P(TP, SP),
        ),
        out_specs=P(SP + TP, None),
        check_vma=False,
    )
```

```python
import functools

import jax
import jax.numpy as jnp
import numpy as np
from jax import lax
from jax.experimental import pallas as pl
from jax.experimental.pallas import tpu as pltpu
from jax.sharding import Mesh
from jax.sharding import PartitionSpec as P

GRID = 64
AXES = ("z", "y", "x", "c")
SP = ("z", "y")
TP = ("x", "c")
MESH_IDS = pl.DeviceIdType.MESH
F32 = jnp.float32
BF16 = jnp.bfloat16

epsilon = 1e-06
rope_base = 10000.0

NZ, NY, NX, NC = 16, 4, 4, 2
NT = NX * NC
PLANE = NY * NT
D = 2048
ROWS = 128
SHARE = 16
KEYS = NZ * NY * SHARE
QW = 256
KW = 384
UP = 384
HID = 176
W_AT = {2: [0], 6: [1]}
W_NEAR = {0: [2], 1: [3]}
W_ATTN = {0: [4], 1: [5]}
W_MORE = ([6, 7], [8, 9], [10, 11, 12, 13, 14, 15, 16])
HOP = 3
QG = 512
NEAR_AT = 9
NEAR = (-4, 6)
TOK = 256


def rms_norm(values, gain):
    return (
        values * lax.rsqrt(jnp.mean(values * values, axis=-1, keepdims=True) + epsilon) * gain
    )


def turn_tables():
    pairs = 16
    frequency = rope_base ** (-np.arange(pairs) / pairs)
    sign = np.repeat([-1.0, 1.0], pairs)

    def both(steps, at):
        angles = np.tile(np.arange(steps)[:, None] * frequency, (1, 2))
        table = np.zeros((2, steps, 128))
        table[0, :, at : at + 32] = np.cos(angles)
        table[1, :, at : at + 32] = np.sin(angles) * sign
        return table

    by_row = both(ROWS // GRID * NZ * NY, 0).reshape(2, NZ * NY, ROWS // GRID, 128)
    by_row = by_row.transpose(1, 0, 2, 3).reshape(NZ * NY, 2 * ROWS // GRID, 128)
    by_row = np.pad(by_row, ((0, 0), (0, 8 - 2 * ROWS // GRID), (0, 0)))
    return by_row.astype(np.float32), both(GRID, 32).astype(np.float32)


def turned(values, cosine, sine):
    lane = lax.broadcasted_iota(jnp.int32, values.shape, 1)
    other = jnp.where((lane & 16) == 0, pltpu.roll(values, 112, 1), pltpu.roll(values, 16, 1))
    return values * cosine + other * sine


def in_one_row(ref):
    folded = ref[...].astype(F32)
    return jnp.concatenate([folded[i : i + 1] for i in range(folded.shape[0])], axis=1)


def as_rows(columns):
    both = jnp.concatenate([columns.astype(F32), jnp.zeros(columns.shape, F32)], axis=0)
    return both.T


def dot_nn(a, b):
    return jnp.dot(a, b, preferred_element_type=F32)


def dot_nt(a, b):
    return lax.dot_general(a, b, (((1,), (1,)), ((), ())), preferred_element_type=F32)


def side_lanes(v, g):
    rest = HID - 128
    pad = jnp.zeros(v.shape[:-1] + (64 - rest,), v.dtype)
    return [v[:, :128], g[:, :128], v[:, 128:], pad, g[:, 128:], pad]


def layer_kernel(
    scale,
    latent,
    rope_key,
    q_nope,
    q_rope,
    by_row,
    by_col,
    up_value,
    up_gate,
    down,
    ow,
    key_up,
    value_up,
    resid,
    kv_gain,
    post_gain,
    pre_gain,
    ffn_gain,
    conv_value,
    conv_gate,
    out,
    kvbuf,
    qbuf,
    wbuf,
    dbuf,
    d_stage,
    owbuf,
    kvt,
    s_scr,
    near_stats,
    near_mixed,
    st_send,
    stats,
    o_send,
    o_recv,
    r_send,
    r_recv,
    in_send,
    inbuf,
    up,
    p_send,
    p_recv,
    stream,
    latent_v,
    rope_key_v,
    q_nope_v,
    q_rope_v,
    by_row_v,
    by_col_v,
    up_value_v,
    up_gate_v,
    down_v,
    key_up_v,
    value_up_v,
    resid_v,
    kv_gain_v,
    gains,
    conv_v,
    turns,
    key_rows,
    w_loc,
    d_loc,
    wide,
    qf,
    vu,
    taps,
    loads,
    unused,
    kvs,
    kvr,
    qs,
    qr,
    wys,
    wyr,
    wzs,
    wps,
    wzr,
    wpr,
    ows,
    owr,
    sts,
    str_,
    os_,
    or_,
    rss,
    rsr,
    ags,
    agr,
    hs,
    hr,
    ps,
    pr,
):
    z, y, x, c = (lax.axis_index(a) for a in AXES)
    tp = x * NC + c
    plane = y * NT + tp
    half = lax.div(y, 2)

    def zz(k):
        return lax.rem(z + k + NZ, NZ)

    def push(src, dst, ss, rs, dev):
        return pltpu.make_async_remote_copy(
            src_ref=src, dst_ref=dst, send_sem=ss, recv_sem=rs, device_id=dev,
            device_id_type=MESH_IDS,
        )

    partner = (z, y, x, 1 - c)
    right, left = (zz(1), y, x, c), (zz(-1), y, x, c)
    cross = ((z + 2 * c - 1 + NZ) % NZ, y, x, 1 - c)

    def on_plane(j):
        p = lax.rem(plane + j, PLANE)
        return (z, lax.div(p, NT), lax.rem(lax.div(p, NC), NX), lax.rem(p, NC))

    def tp_peer(t):
        return (z, y, lax.div(t, NC), lax.rem(t, NC))

    def own(ref):
        return ref.at[pl.ds(pl.multiple_of(tp * SHARE, SHARE), SHARE)]

    local = {}

    def load(name, src, dst):
        local[name] = pltpu.make_async_copy(src, dst, loads.at[len(local)])
        local[name].start()

    load("latent", own(latent), latent_v)
    load("rope_key", rope_key, rope_key_v)
    load("by_row", by_row.at[z * NY + y], by_row_v)
    load("by_col", by_col, by_col_v)
    load("kv_gain", kv_gain, kv_gain_v)
    load("post", post_gain, gains.at[0])
    load("pre", pre_gain, gains.at[1])
    load("ffn", ffn_gain, gains.at[2])
    load("q_nope", q_nope, q_nope_v)
    load("q_rope", q_rope, q_rope_v)
    load("up_value", up_value, up_value_v)
    load("up_gate", up_gate, up_gate_v)
    load("down", down, down_v)
    load("ow", ow, owbuf.at[c])
    load("key_up", key_up, key_up_v)
    load("value_up", value_up, value_up_v)
    load("resid", own(resid), resid_v)
    load("conv_value", conv_value, conv_v.at[0])
    load("conv_gate", conv_gate, conv_v.at[1])

    def ready(*names):
        for name in names:
            local[name].wait()

    barrier = pltpu.get_barrier_semaphore()
    for hop in range(1, HOP + 1):
        for dev in ((zz(hop), y, x, c), (zz(-hop), y, x, c)):
            pl.semaphore_signal(barrier, inc=1, device_id=dev, device_id_type=MESH_IDS)
    pl.semaphore_signal(barrier, inc=1, device_id=cross, device_id_type=MESH_IDS)

    @pl.loop(1, PLANE)
    def _(j):
        pl.semaphore_signal(barrier, inc=1, device_id=on_plane(j), device_id_type=MESH_IDS)

    def kv_slot(yy, d):
        start = pl.multiple_of(((d + 8) * NY + yy) * SHARE, SHARE)
        return kvbuf.at[pl.ds(start, SHARE)]

    def w_slot(kind, core, k):
        at = pl.ds(pl.multiple_of(k * ROWS, ROWS), ROWS)
        if kind == 0:
            return wbuf.at[core, at]
        return dbuf.at[core, pl.ds(0, HID), at]

    def w_part(kind, yy):
        if kind == 0:
            return wbuf.at[c, pl.ds(pl.multiple_of(z * ROWS + yy * 32, 32), 32)]
        return d_stage.at[pl.ds(pl.multiple_of(yy * 32, 32), 32)]

    ready("latent", "rope_key", "by_row", "by_col", "kv_gain")
    for i in range(2):
        grid_rows = [
            by_row_v[2 * i + j : 2 * i + j + 1] + by_col_v[i] for j in range(ROWS // GRID)
        ]
        turns[i] = jnp.concatenate(grid_rows, axis=0)
    rows = pl.ds(pl.multiple_of(tp * SHARE, SHARE), SHARE)
    kv_slot(y, 0)[:, :256] = rms_norm(
        latent_v[...].astype(F32), in_one_row(kv_gain_v)
    ).astype(BF16)
    key_rows[...] = as_rows(rope_key_v[...])
    kv_slot(y, 0)[:, 256:] = turned(key_rows[rows], turns[0, rows], turns[1, rows]).astype(BF16)

    pl.semaphore_wait(barrier, 2 * HOP + PLANE)

    def go(copy):
        copy.start()

    def kv_to(d, hop, dev):
        seen = d - hop
        go(push(kv_slot(y, d), kv_slot(y, seen), kvs.at[0], kvr.at[seen + 8], dev))

    def kv_to_y(d):
        slot = kv_slot(y, d)
        for j in range(1, NY):
            dev = (z, lax.rem(y + j, NY), x, c)
            go(push(slot, slot, kvs.at[0], kvr.at[16 if NEAR[0] <= d < NEAR[1] else 17], dev))

    for hop in range(HOP, 0, -1):
        kv_to(0, hop, (zz(hop), y, x, c))
        kv_to(0, -hop, (zz(-hop), y, x, c))
    kv_to_y(0)
    ready("q_nope", "q_rope")
    qbuf[tp, :, :128] = q_nope_v[...]
    qbuf[tp, :, 128:] = turned(as_rows(q_rope_v[...]), turns[0], turns[1]).astype(BF16)
    for j in range(1, NT):
        t = lax.rem(tp + j, NT)
        go(push(qbuf.at[tp], qbuf.at[tp], qs.at[0], qr.at[0], tp_peer(t)))

    ready("up_value", "up_gate", "down")
    value, gate = up_value_v[...].astype(F32), up_gate_v[...].astype(F32)
    across = down_v[...].astype(F32)
    for yy in range(NY):
        at = slice(yy * HID, (yy + 1) * HID)
        parts = side_lanes(value[:, at], gate[:, at])
        w_loc[yy] = jnp.concatenate(parts, axis=1).astype(BF16)
        parts = [across[:, at], jnp.zeros((32, 256 - HID), F32)]
        d_loc[yy] = jnp.concatenate(parts, axis=1).astype(BF16)
    for j in range(1, NY):
        yy = lax.rem(y + j, NY)
        dev = (z, yy, x, c)
        go(push(w_loc.at[yy], w_part(0, y), wys.at[0], wyr.at[0], dev))
        go(push(d_loc.at[yy], w_part(1, y), wys.at[1], wyr.at[1], dev))
    w_part(0, y)[...] = w_loc[y]
    w_part(1, y)[...] = d_loc[y]
    dbuf[:, HID:] = jnp.zeros((NC, 256 - HID, D), BF16)
    ready("ow")
    go(push(owbuf.at[c], owbuf.at[c], ows.at[0], owr.at[0], partner))

    def w_send(kind, k, to_right, to_left):
        slot = w_slot(kind, c, k)
        if to_right:
            go(push(slot, slot, wzs.at[kind], wzr.at[kind, k], right))
        if to_left:
            go(push(slot, slot, wzs.at[kind], wzr.at[kind, k], left))

    def w_across(kind, k):
        slot = w_slot(kind, c, k)
        go(push(slot, slot, wps.at[kind], wpr.at[kind], partner))

    def w_wait(kind, k, dev):
        slot = w_slot(kind, c, k)
        push(slot, slot, wzs.at[kind], wzr.at[kind, k], dev).wait_recv()

    def w_start():
        for kind in range(2):
            landed((wbuf.at[c] if kind == 0 else d_stage).at[pl.ds(0, 96)], wyr.at[kind])
            if kind == 1:
                columns = pl.ds(pl.multiple_of(z * ROWS, ROWS), ROWS)
                dbuf[c, :HID, columns] = d_stage[...].astype(F32).T[:HID].astype(BF16)
            w_send(kind, z, True, True)
            w_across(kind, z)

    def w_go(steps):
        for event in steps:
            if event == 0:
                w_start()
                continue
            step, kind = (event + 1) // 2, (event + 1) % 2
            k = zz(-step)
            w_wait(kind, k, left)
            w_send(kind, k, step < 8, False)
            w_across(kind, k)
            if step < 8:
                k = zz(step)
                w_wait(kind, k, right)
                w_send(kind, k, False, step < 7)
                w_across(kind, k)

    def kv_wait(d):
        slot = kv_slot(y, d)
        push(slot, slot, kvs.at[0], kvr.at[d + 8], right).wait_recv()

    def landed(ref, sem):
        push(ref, ref, unused.at[0], sem, partner).wait_recv()

    def left_here(ref, sem):
        push(ref, ref, sem, unused.at[0], partner).wait_send()

    def fold_queries():
        landed(qbuf.at[pl.ds(0, NT - 1)], qr.at[0])
        ready("key_up")
        wide[...] = key_up_v[...].astype(F32)
        for h in range(NT):
            up_h = wide[pl.ds(h, 256, stride=NT)].astype(BF16)
            folded = dot_nt(qbuf[h, :, :128], up_h).astype(BF16)
            folded = folded.reshape(NX, NC, SHARE, 256)
            rope = qbuf[h, :, 128:].reshape(NX, NC, SHARE, 128)
            for core in range(NC):
                first = (h // 2 * NC + core) * 128 + h % 2 * 64
                r = slice(first, first + 64)
                qf[r, :256] = folded[:, core].reshape(64, 256)
                qf[r, 256:] = rope[:, core].reshape(64, 128)

    def split_values():
        ready("value_up")
        wide[...] = value_up_v[...].astype(F32)
        for h in range(NT):
            vu[h // 2, h % 2 * 128 : h % 2 * 128 + 128] = wide[pl.ds(h, 256, stride=NT)].T.astype(BF16)

    def weigh(queries, spans, top):
        for at in spans:
            s_scr[at, queries] = dot_nt(kvbuf[at], qf[queries])
            here = jnp.max(s_scr[at, queries], axis=0, keepdims=True)
            top = here if top is None else jnp.maximum(top, here)
        total, mixed = 0.0, 0.0
        for at in spans:
            weights = jnp.exp2((s_scr[at, queries] - top) * scale2)
            total += jnp.sum(weights, axis=0, keepdims=True)
            mixed += dot_nn(kvt[:, at], weights.astype(BF16))
        return top, total, mixed

    scale2 = scale * 1.4426950408889634
    first, last = ((d + 8) * NY * SHARE for d in NEAR)
    near, far = [slice(first, last)], [slice(0, first), slice(last, KEYS)]
    groups = [slice(i * QG, (i + 1) * QG) for i in range(1024 // QG)]

    def weigh_near():
        landed(kvbuf.at[pl.ds(0, (NEAR[1] - NEAR[0]) * 3 * SHARE)], kvr.at[16])
        for at in near:
            kvt[:, at] = kvbuf[at, :256].T
        for i, queries in enumerate(groups):
            top, total, mixed = weigh(queries, near, None)
            near_stats[0:1, queries] = top
            near_stats[1:2, queries] = total
            near_mixed[:, queries] = mixed
            if i in W_NEAR:
                w_go(W_NEAR[i])

    for d in range(1, 9):
        if d == 4:
            fold_queries()
        if d == 6:
            split_values()
        if d == NEAR_AT:
            weigh_near()
        kv_wait(-d)
        if d + HOP <= 8:
            kv_to(-d, HOP, (zz(HOP), y, x, c))
        if d < 8:
            kv_wait(d)
            if d + HOP <= 7:
                kv_to(d, -HOP, (zz(-HOP), y, x, c))
        kv_to_y(-d)
        if d < 8:
            kv_to_y(d)
        if d in W_AT:
            w_go(W_AT[d])
    if NEAR_AT == 9:
        weigh_near()
    landed(kvbuf.at[pl.ds(0, (NZ - NEAR[1] + NEAR[0]) * 3 * SHARE)], kvr.at[17])
    for at in far:
        kvt[:, at] = kvbuf[at, :256].T
    lane = lax.broadcasted_iota(jnp.int32, (128, 256), 1)
    for i in range(2):
        pair = (x // 2 + 1 + i) % 2
        queries = pl.ds(pl.multiple_of(pair * QG, QG), QG)
        top_near = near_stats[0:1, queries]
        top, total, mixed = weigh(queries, far, top_near)
        factor = jnp.exp2((top_near - top) * scale2)
        total += factor * near_stats[1:2, queries]
        mixed += factor * near_mixed[:, queries]
        for k in range(2):
            cut = slice(k * 256, k * 256 + 256)
            part = dot_nn(vu[2 * pair + k], mixed[:, cut].astype(BF16))
            part = jnp.where((lane & 64) == 0, part[:128], part[128:]).astype(BF16)
            for core in range(NC):
                t = pair * 4 + k * NC + core
                at = slice(core * 128, core * 128 + 128)
                o_send[t] = part[:, at]
                st_send[t, 0:1] = top[:, cut][:, at]
                st_send[t, 1:2] = total[:, cut][:, at]
        for k in range(4):
            t = pair * 4 + (k + tp) % 4

            @pl.when(t != tp)
            def _():
                go(push(st_send.at[t], stats.at[tp], sts.at[0], str_.at[0], tp_peer(t)))
                go(push(o_send.at[t], o_recv.at[tp], os_.at[0], or_.at[0], tp_peer(t)))

        if i in W_ATTN:
            w_go(W_ATTN[i])
    o_recv[tp] = o_send[tp]
    stats[tp] = st_send[tp]
    w_go(W_MORE[0])
    push(owbuf.at[1 - c], owbuf.at[1 - c], ows.at[0], owr.at[0], partner).wait_recv()
    landed(stats.at[pl.ds(0, NT - 1)], str_.at[0])
    landed(o_recv.at[pl.ds(0, NT - 1)], or_.at[0])
    top_all = stats[0, 0:1]
    for t in range(1, NT):
        top_all = jnp.maximum(top_all, stats[t, 0:1])
    total_all = jnp.zeros_like(top_all)
    attended = jnp.zeros((128, 128), F32)
    for t in range(NT):
        factor = jnp.exp2((stats[t, 0:1] - top_all) * scale2)
        total_all += factor * stats[t, 1:2]
        attended += factor * o_recv[t].astype(F32)
    attended = (attended / total_all).T.astype(BF16)
    r_send[...] = (
        dot_nn(attended[:64], owbuf[0]) + dot_nn(attended[64:], owbuf[1])
    ).astype(BF16)
    for j in range(1, NX):
        xx = lax.rem(x + j, NX)
        src = r_send.at[pl.ds(pl.multiple_of(xx * SHARE, SHARE), SHARE)]
        go(push(src, r_recv.at[x], rss.at[0], rsr.at[0], (z, y, xx, c)))
    r_recv[x] = r_send[pl.ds(pl.multiple_of(x * SHARE, SHARE), SHARE)]
    w_go(W_MORE[1])
    landed(r_recv.at[pl.ds(0, NX - 1)], rsr.at[0])
    ready("resid", "post", "pre", "ffn")
    summed = r_recv[0].astype(F32)
    for j in range(1, NX):
        summed += r_recv[j].astype(F32)
    summed = summed.astype(BF16).astype(F32)
    flow = (resid_v[...].astype(F32) + rms_norm(summed, in_one_row(gains.at[0]))).astype(BF16).astype(F32)
    stream[...] = flow
    in_send[...] = rms_norm(flow, in_one_row(gains.at[1])).astype(BF16)

    def in_slot(s):
        return inbuf.at[pl.ds(pl.multiple_of(s * SHARE, SHARE), SHARE)]

    mine = (y % 2) * NT + tp

    def ag_copy(j):
        chip = lax.rem(y * NX + x + j, NY * NX)
        dev = (z, lax.div(chip, NX), lax.rem(chip, NX), half)
        return push(in_send, in_slot(mine), ags.at[0], agr.at[0], dev)

    @pl.loop(1, NY * NX)
    def _(j):
        ag_copy(j).start()

    @pl.when(half == c)
    def _():
        in_slot(mine)[...] = in_send[...]

    @pl.when(half != c)
    def _():
        ag_copy(0).start()

    w_go(W_MORE[2])

    ready("conv_value", "conv_gate")
    last = conv_v.shape[2] - UP
    for core in range(NC):
        first = (x * NC + core) * NY * HID + y * HID
        base = jnp.minimum(first // 128 * 128, last)
        lanes = pl.ds(pl.multiple_of(base, 128), UP)
        back = UP - (first - base)
        v = pltpu.roll(conv_v[0, :, lanes].astype(F32), back, 1)
        g = pltpu.roll(conv_v[1, :, lanes].astype(F32), back, 1)
        taps[core, 0:3] = jnp.concatenate(side_lanes(v[:, :HID], g[:, :HID]), axis=1)

    landed(wbuf.at[1 - c], wpr.at[0])

    own_slot = jnp.where(half == c, mine, -1)

    @pl.when(half == c)
    def _():
        landed(inbuf.at[pl.ds(0, 15 * SHARE)], agr.at[0])

    @pl.when(half != c)
    def _():
        landed(inbuf, agr.at[0])

    for core in range(NC):
        up[core, 8 : 8 + TOK] = dot_nn(inbuf[...], wbuf[core])

    low_dev = ((z + c) % NZ, y, x, 1 - c)
    high_dev = ((z + c - 1 + NZ) % NZ, y, x, 1 - c)
    go(push(up.at[:, pl.ds(TOK, 8)], up.at[:, pl.ds(0, 8)], hs.at[0], hr.at[0], low_dev))
    go(push(up.at[:, pl.ds(8, 8)], up.at[:, pl.ds(TOK + 8, 8)], hs.at[1], hr.at[1], high_dev))
    def hidden_rows(core, first, count):
        conv = (
            up[core, first + 7 : first + 7 + count] * taps[core, 0:1]
            + up[core, first + 8 : first + 8 + count] * taps[core, 1:2]
            + up[core, first + 9 : first + 9 + count] * taps[core, 2:3]
        )
        gate = conv[:, 128:256]
        near = gate / (1.0 + jnp.exp(-gate)) * conv[:, :128]
        gate = pltpu.roll(conv[:, 256:], 64, 1)
        far = gate / (1.0 + jnp.exp(-gate)) * conv[:, 256:]
        lane = lax.broadcasted_iota(jnp.int32, far.shape, 1)
        far = jnp.where(lane < 64, far, 0.0)
        return jnp.concatenate([near.astype(BF16), far.astype(BF16)], axis=1)

    def down_rows(hidden):
        return (dot_nn(hidden[0], dbuf[0]) + dot_nn(hidden[1], dbuf[1])).astype(BF16)

    inner = [hidden_rows(core, SHARE, TOK - 2 * SHARE) for core in range(NC)]
    landed(dbuf.at[1 - c, pl.ds(0, HID)], wpr.at[1])

    p_send[SHARE : TOK - SHARE] = down_rows(inner)

    chip = y * NX + x

    def p_slot(s):
        return p_send.at[pl.ds(pl.multiple_of(s * SHARE, SHARE), SHARE)]

    def rs_copy(s):
        dev = (z, 2 * c + lax.div(s, NT), lax.rem(lax.div(s, NC), NX), lax.rem(s, NC))
        return push(p_slot(s), p_recv.at[chip], ps.at[0], pr.at[0], dev)

    @pl.loop(0, 16)
    def _(j):
        s = lax.rem(mine + j, 16)

        @pl.when((s != own_slot) & (s > 0) & (s < 15))
        def _():
            rs_copy(s).start()

    low, high = up.at[:, pl.ds(0, 8)], up.at[:, pl.ds(TOK + 8, 8)]
    push(low, low, hs.at[0], hr.at[0], low_dev).wait_recv()
    push(high, high, hs.at[1], hr.at[1], high_dev).wait_recv()

    @pl.when((z == 0) & (c == 0))
    def _():
        up[:, 0:8] = jnp.zeros((NC, 8, UP), F32)

    @pl.when((z == NZ - 1) & (c == 1))
    def _():
        up[:, TOK + 8 : TOK + 16] = jnp.zeros((NC, 8, UP), F32)

    outer = [
        jnp.concatenate(
            [hidden_rows(core, 0, SHARE), hidden_rows(core, TOK - SHARE, SHARE)], axis=0
        )
        for core in range(NC)
    ]
    edges = down_rows(outer)
    p_send[:SHARE] = edges[:SHARE]
    p_send[TOK - SHARE :] = edges[SHARE:]
    for s in (0, 15):

        @pl.when(s != own_slot)
        def _():
            rs_copy(s).start()


    @pl.when(half == c)
    def _():
        p_recv[chip] = p_slot(mine)[...]

    @pl.when(half == c)
    def _():
        landed(p_recv.at[pl.ds(0, 15)], pr.at[0])

    @pl.when(half != c)
    def _():
        landed(p_recv, pr.at[0])

    projected = p_recv[0].astype(F32)
    for k in range(1, 16):
        projected += p_recv[k].astype(F32)
    projected = projected.astype(BF16).astype(F32)
    out[...] = (stream[...] + rms_norm(projected, in_one_row(gains.at[2]))).astype(BF16)

    left_here(kvbuf.at[pl.ds(0, 63 * SHARE)], kvs.at[0])
    left_here(qbuf.at[pl.ds(0, NT - 1)], qs.at[0])
    left_here(wbuf.at[0, pl.ds(0, 96)], wys.at[0])
    left_here(d_stage.at[pl.ds(0, 96)], wys.at[1])
    left_here(owbuf.at[0], ows.at[0])
    left_here(wbuf.at[0, pl.ds(0, 15 * ROWS)], wzs.at[0])
    left_here(dbuf.at[0, pl.ds(0, HID), pl.ds(0, 15 * ROWS)], wzs.at[1])
    left_here(wbuf.at[0], wps.at[0])
    left_here(dbuf.at[0, pl.ds(0, HID)], wps.at[1])
    left_here(stats.at[pl.ds(0, NT - 1)], sts.at[0])
    left_here(o_recv.at[pl.ds(0, NT - 1)], os_.at[0])
    left_here(r_recv.at[pl.ds(0, NX - 1)], rss.at[0])
    both = up.at[:, pl.ds(0, 8)]
    left_here(both, hs.at[0])
    left_here(both, hs.at[1])

    @pl.when(half == c)
    def _():
        left_here(inbuf.at[pl.ds(0, 15 * SHARE)], ags.at[0])
        left_here(p_send.at[pl.ds(0, 15 * SHARE)], ps.at[0])

    @pl.when(half != c)
    def _():
        left_here(inbuf, ags.at[0])
        left_here(p_send, ps.at[0])


def body(
    residual,
    query_nope,
    query_rope,
    latent,
    rope_key,
    kv_gain,
    key_up,
    value_up,
    out_weight,
    post_gain,
    pre_gain,
    ffn_gain,
    up_value,
    up_gate,
    conv_value,
    conv_gate,
    down_weight,
):
    scale = (query_nope.shape[2] + query_rope.shape[2]) ** (-0.5)
    by_row, by_col = turn_tables()

    dma = pltpu.SemaphoreType.DMA
    vmem = pltpu.VMEM
    return pl.pallas_call(
        functools.partial(layer_kernel, scale),
        out_shape=jax.ShapeDtypeStruct((SHARE, D), BF16),
        in_specs=[pl.BlockSpec(memory_space=pl.ANY)] * 19,
        out_specs=pl.BlockSpec(memory_space=vmem),
        scratch_shapes=[
            vmem((KEYS, KW), BF16),
            vmem((NT, ROWS, QW), BF16),
            vmem((NC, NZ * ROWS, UP), BF16),
            vmem((NC, 256, D), BF16),
            vmem((ROWS, 256), BF16),
            vmem((NC, 128, D), BF16),
            vmem((256, KEYS), BF16),
            vmem((KEYS, 1024), F32),
            vmem((8, 1024), F32),
            vmem((256, 1024), F32),
            vmem((NT, 8, 128), F32),
            vmem((NT, 8, 128), F32),
            vmem((NT, 128, 128), BF16),
            vmem((NT, 128, 128), BF16),
            vmem((64, D), BF16),
            vmem((NX, SHARE, D), BF16),
            vmem((SHARE, D), BF16),
            vmem((TOK, D), BF16),
            vmem((NC, TOK + 16, UP), F32),
            vmem((TOK, D), BF16),
            vmem((NY * NX, SHARE, D), BF16),
            vmem((SHARE, D), F32),
            vmem((SHARE, 256), BF16),
            vmem((64, ROWS), BF16),
            vmem((ROWS, 128), BF16),
            vmem((64, ROWS), BF16),
            vmem((8, 128), F32),
            vmem((2, GRID, 128), F32),
            vmem(up_value.shape, BF16),
            vmem(up_gate.shape, BF16),
            vmem(down_weight.shape[::-1], BF16),
            vmem((256 * NT, 128), BF16),
            vmem((256 * NT, 128), BF16),
            vmem((SHARE, D), BF16),
            vmem((2, 128), BF16),
            vmem((3, D // 128, 128), BF16),
            vmem((2,) + conv_value.shape, BF16),
            vmem((2, ROWS, 128), F32),
            vmem((ROWS, 128), F32),
            vmem((NY, 32, UP), BF16),
            vmem((NY, 32, 256), BF16),
            vmem((256 * NT, 128), F32),
            vmem((NX * 256, KW), BF16),
            vmem((4, 256, 256), BF16),
            vmem((NC, 8, UP), F32),
        ]
        + [dma((n,)) for n in (19, 1, 1, 18, 1, 1, 2, 2, 2, 2)]
        + [dma((2, NZ))]
        + [dma((n,)) for n in (2, 1, 1, 1, 1, 1, 1, 1, 1, 1, 1, 2, 2, 1, 1)],
        compiler_params=pltpu.CompilerParams(
            collective_id=0, has_side_effects=True, vmem_limit_bytes=60 * 1024 * 1024
        ),
        name="layer",
    )(
        latent,
        rope_key.T,
        query_nope[:, 0],
        query_rope[:, 0].T,
        by_row,
        by_col,
        up_value,
        up_gate,
        down_weight.T,
        out_weight,
        key_up.reshape(-1, key_up.shape[2]),
        value_up.reshape(-1, value_up.shape[2]),
        residual,
        kv_gain.reshape(-1, 128),
        post_gain.reshape(-1, 128),
        pre_gain.reshape(-1, 128),
        ffn_gain.reshape(-1, 128),
        conv_value,
        conv_gate,
    )


def solution(mesh):
    torus = Mesh(mesh.devices.reshape(NZ, NY, NX, NC), AXES)
    return jax.shard_map(
        body,
        mesh=torus,
        in_specs=(
            P(SP, None),
            P(SP, TP, None),
            P(SP, TP, None),
            P(SP, None),
            P(SP, None),
            P(),
            P(),
            P(),
            P(TP, None),
            P(),
            P(),
            P(),
            P(SP, TP),
            P(SP, TP),
            P(),
            P(),
            P(TP, SP),
        ),
        out_specs=P(SP + TP, None),
        check_vma=False,
    )
```

```python
import functools

import jax
import jax.numpy as jnp
import numpy as np
from jax import lax
from jax.experimental import pallas as pl
from jax.experimental.pallas import tpu as pltpu
from jax.sharding import Mesh
from jax.sharding import PartitionSpec as P

GRID = 64
AXES = ("z", "y", "x", "c")
SP = ("z", "y")
TP = ("x", "c")
MESH_IDS = pl.DeviceIdType.MESH
F32 = jnp.float32
BF16 = jnp.bfloat16

epsilon = 1e-06
rope_base = 10000.0

NZ, NY, NX, NC = 16, 4, 4, 2
NT = NX * NC
PLANE = NY * NT
D = 2048
ROWS = 128
SHARE = 16
KEYS = NZ * NY * SHARE
QW = 256
KW = 384
UP = 384
HID = 176
W_AT = {2: [0], 6: [1]}
W_NEAR = {0: [2], 1: [3]}
W_ATTN = {0: [4], 1: [5]}
W_MORE = ([6, 7], [8, 9], [10, 11, 12, 13, 14, 15, 16])
HOP = 3
QG = 512
NEAR_AT = 9
NEAR = (-4, 6)
TOK = 256


def rms_norm(values, gain):
    return (
        values * lax.rsqrt(jnp.mean(values * values, axis=-1, keepdims=True) + epsilon) * gain
    )


def turn_tables():
    pairs = 16
    frequency = rope_base ** (-np.arange(pairs) / pairs)
    sign = np.repeat([-1.0, 1.0], pairs)

    def both(steps, at):
        angles = np.tile(np.arange(steps)[:, None] * frequency, (1, 2))
        table = np.zeros((2, steps, 128))
        table[0, :, at : at + 32] = np.cos(angles)
        table[1, :, at : at + 32] = np.sin(angles) * sign
        return table

    by_row = both(ROWS // GRID * NZ * NY, 0).reshape(2, NZ * NY, ROWS // GRID, 128)
    by_row = by_row.transpose(1, 0, 2, 3).reshape(NZ * NY, 2 * ROWS // GRID, 128)
    by_row = np.pad(by_row, ((0, 0), (0, 8 - 2 * ROWS // GRID), (0, 0)))
    return by_row.astype(np.float32), both(GRID, 32).astype(np.float32)


def turned(values, cosine, sine):
    lane = lax.broadcasted_iota(jnp.int32, values.shape, 1)
    other = jnp.where((lane & 16) == 0, pltpu.roll(values, 112, 1), pltpu.roll(values, 16, 1))
    return values * cosine + other * sine


def in_one_row(ref):
    folded = ref[...].astype(F32)
    return jnp.concatenate([folded[i : i + 1] for i in range(folded.shape[0])], axis=1)


def as_rows(columns):
    both = jnp.concatenate([columns.astype(F32), jnp.zeros(columns.shape, F32)], axis=0)
    return both.T


def dot_nn(a, b):
    return jnp.dot(a, b, preferred_element_type=F32)


def dot_nt(a, b):
    return lax.dot_general(a, b, (((1,), (1,)), ((), ())), preferred_element_type=F32)


def side_lanes(v, g):
    rest = HID - 128
    pad = jnp.zeros(v.shape[:-1] + (64 - rest,), v.dtype)
    return [v[:, :128], g[:, :128], v[:, 128:], pad, g[:, 128:], pad]


def layer_kernel(
    scale,
    latent,
    rope_key,
    q_nope,
    q_rope,
    by_row,
    by_col,
    up_value,
    up_gate,
    down,
    ow,
    key_up,
    value_up,
    resid,
    kv_gain,
    post_gain,
    pre_gain,
    ffn_gain,
    conv_value,
    conv_gate,
    out,
    kvbuf,
    qbuf,
    wbuf,
    dbuf,
    d_stage,
    owbuf,
    kvt,
    s_scr,
    near_stats,
    near_mixed,
    st_send,
    stats,
    o_send,
    o_recv,
    r_send,
    r_recv,
    in_send,
    inbuf,
    up,
    p_send,
    a_recv,
    b_recv,
    a_send,
    b_send,
    fin,
    stream,
    latent_v,
    rope_key_v,
    q_nope_v,
    q_rope_v,
    by_row_v,
    by_col_v,
    up_value_v,
    up_gate_v,
    down_v,
    key_up_v,
    value_up_v,
    resid_v,
    kv_gain_v,
    gains,
    conv_v,
    turns,
    key_rows,
    w_loc,
    d_loc,
    wide,
    qf,
    vu,
    taps,
    loads,
    unused,
    kvs,
    kvr,
    qs,
    qr,
    wys,
    wyr,
    wzs,
    wps,
    wzr,
    wpr,
    ows,
    owr,
    sts,
    str_,
    os_,
    or_,
    rss,
    rsr,
    ags,
    agr,
    hs,
    hr,
    ps,
    pr,
):
    z, y, x, c = (lax.axis_index(a) for a in AXES)
    tp = x * NC + c
    plane = y * NT + tp
    half = lax.div(y, 2)

    def zz(k):
        return lax.rem(z + k + NZ, NZ)

    def push(src, dst, ss, rs, dev):
        return pltpu.make_async_remote_copy(
            src_ref=src, dst_ref=dst, send_sem=ss, recv_sem=rs, device_id=dev,
            device_id_type=MESH_IDS,
        )

    partner = (z, y, x, 1 - c)
    right, left = (zz(1), y, x, c), (zz(-1), y, x, c)
    cross = ((z + 2 * c - 1 + NZ) % NZ, y, x, 1 - c)

    def on_plane(j):
        p = lax.rem(plane + j, PLANE)
        return (z, lax.div(p, NT), lax.rem(lax.div(p, NC), NX), lax.rem(p, NC))

    def tp_peer(t):
        return (z, y, lax.div(t, NC), lax.rem(t, NC))

    def own(ref):
        return ref.at[pl.ds(pl.multiple_of(tp * SHARE, SHARE), SHARE)]

    local = {}

    def load(name, src, dst):
        local[name] = pltpu.make_async_copy(src, dst, loads.at[len(local)])
        local[name].start()

    load("latent", own(latent), latent_v)
    load("rope_key", rope_key, rope_key_v)
    load("by_row", by_row.at[z * NY + y], by_row_v)
    load("by_col", by_col, by_col_v)
    load("post", post_gain, gains.at[0])
    load("pre", pre_gain, gains.at[1])
    load("ffn", ffn_gain, gains.at[2])
    load("kv_gain", kv_gain, kv_gain_v)

    def ready(*names):
        for name in names:
            local[name].wait()

    barrier = pltpu.get_barrier_semaphore()
    for hop in range(1, HOP + 1):
        for dev in ((zz(hop), y, x, c), (zz(-hop), y, x, c)):
            pl.semaphore_signal(barrier, inc=1, device_id=dev, device_id_type=MESH_IDS)
    pl.semaphore_signal(barrier, inc=1, device_id=cross, device_id_type=MESH_IDS)

    @pl.loop(1, PLANE)
    def _(j):
        pl.semaphore_signal(barrier, inc=1, device_id=on_plane(j), device_id_type=MESH_IDS)

    def kv_slot(yy, d):
        start = pl.multiple_of(((d + 8) * NY + yy) * SHARE, SHARE)
        return kvbuf.at[pl.ds(start, SHARE)]

    def w_slot(kind, core, k):
        at = pl.ds(pl.multiple_of(k * ROWS, ROWS), ROWS)
        if kind == 0:
            return wbuf.at[core, at]
        return dbuf.at[core, pl.ds(0, HID), at]

    def w_part(kind, yy):
        if kind == 0:
            return wbuf.at[c, pl.ds(pl.multiple_of(z * ROWS + yy * 32, 32), 32)]
        return d_stage.at[pl.ds(pl.multiple_of(yy * 32, 32), 32)]

    load("q_nope", q_nope, q_nope_v)
    load("q_rope", q_rope, q_rope_v)
    load("up_value", up_value, up_value_v)
    load("up_gate", up_gate, up_gate_v)
    load("down", down, down_v)
    load("ow", ow, owbuf.at[c])
    load("key_up", key_up, key_up_v)
    load("value_up", value_up, value_up_v)
    load("resid", own(resid), resid_v)
    load("conv_value", conv_value, conv_v.at[0])
    load("conv_gate", conv_gate, conv_v.at[1])

    ready("latent", "rope_key", "by_row", "by_col", "kv_gain")
    for i in range(2):
        grid_rows = [
            by_row_v[2 * i + j : 2 * i + j + 1] + by_col_v[i] for j in range(ROWS // GRID)
        ]
        turns[i] = jnp.concatenate(grid_rows, axis=0)
    rows = pl.ds(pl.multiple_of(tp * SHARE, SHARE), SHARE)
    kv_slot(y, 0)[:, :256] = rms_norm(
        latent_v[...].astype(F32), in_one_row(kv_gain_v)
    ).astype(BF16)
    key_rows[...] = as_rows(rope_key_v[...])
    kv_slot(y, 0)[:, 256:] = turned(key_rows[rows], turns[0, rows], turns[1, rows]).astype(BF16)

    pl.semaphore_wait(barrier, 2 * HOP + PLANE)

    def go(copy):
        copy.start()

    def kv_to(d, hop, dev):
        seen = d - hop
        go(push(kv_slot(y, d), kv_slot(y, seen), kvs.at[0], kvr.at[seen + 8], dev))

    def kv_to_y(d):
        slot = kv_slot(y, d)
        for j in range(1, NY):
            dev = (z, lax.rem(y + j, NY), x, c)
            go(push(slot, slot, kvs.at[0], kvr.at[16 if NEAR[0] <= d < NEAR[1] else 17], dev))

    for hop in range(HOP, 0, -1):
        kv_to(0, hop, (zz(hop), y, x, c))
        kv_to(0, -hop, (zz(-hop), y, x, c))
    kv_to_y(0)
    ready("q_nope", "q_rope")
    qbuf[tp, :, :128] = q_nope_v[...]
    qbuf[tp, :, 128:] = turned(as_rows(q_rope_v[...]), turns[0], turns[1]).astype(BF16)
    for j in range(1, NT):
        t = lax.rem(tp + j, NT)
        go(push(qbuf.at[tp], qbuf.at[tp], qs.at[0], qr.at[0], tp_peer(t)))

    ready("up_value", "up_gate", "down")
    value, gate = up_value_v[...].astype(F32), up_gate_v[...].astype(F32)
    across = down_v[...].astype(F32)
    for yy in range(NY):
        at = slice(yy * HID, (yy + 1) * HID)
        parts = side_lanes(value[:, at], gate[:, at])
        w_loc[yy] = jnp.concatenate(parts, axis=1).astype(BF16)
        parts = [across[:, at], jnp.zeros((32, 256 - HID), F32)]
        d_loc[yy] = jnp.concatenate(parts, axis=1).astype(BF16)
    for j in range(1, NY):
        yy = lax.rem(y + j, NY)
        dev = (z, yy, x, c)
        go(push(w_loc.at[yy], w_part(0, y), wys.at[0], wyr.at[0], dev))
        go(push(d_loc.at[yy], w_part(1, y), wys.at[1], wyr.at[1], dev))
    w_part(0, y)[...] = w_loc[y]
    w_part(1, y)[...] = d_loc[y]
    dbuf[:, HID:] = jnp.zeros((NC, 256 - HID, D), BF16)
    ready("ow")
    go(push(owbuf.at[c], owbuf.at[c], ows.at[0], owr.at[0], partner))

    def w_send(kind, k, to_right, to_left):
        slot = w_slot(kind, c, k)
        if to_right:
            go(push(slot, slot, wzs.at[kind], wzr.at[kind, k], right))
        if to_left:
            go(push(slot, slot, wzs.at[kind], wzr.at[kind, k], left))

    def w_across(kind, k):
        slot = w_slot(kind, c, k)
        go(push(slot, slot, wps.at[kind], wpr.at[kind], partner))

    def w_wait(kind, k, dev):
        slot = w_slot(kind, c, k)
        push(slot, slot, wzs.at[kind], wzr.at[kind, k], dev).wait_recv()

    def w_start():
        for kind in range(2):
            landed((wbuf.at[c] if kind == 0 else d_stage).at[pl.ds(0, 96)], wyr.at[kind])
            if kind == 1:
                columns = pl.ds(pl.multiple_of(z * ROWS, ROWS), ROWS)
                dbuf[c, :HID, columns] = d_stage[...].astype(F32).T[:HID].astype(BF16)
            w_send(kind, z, True, True)
            w_across(kind, z)

    def w_go(steps):
        for event in steps:
            if event == 0:
                w_start()
                continue
            step, kind = (event + 1) // 2, (event + 1) % 2
            k = zz(-step)
            w_wait(kind, k, left)
            w_send(kind, k, step < 8, False)
            w_across(kind, k)
            if step < 8:
                k = zz(step)
                w_wait(kind, k, right)
                w_send(kind, k, False, step < 7)
                w_across(kind, k)

    def kv_wait(d):
        slot = kv_slot(y, d)
        push(slot, slot, kvs.at[0], kvr.at[d + 8], right).wait_recv()

    def landed(ref, sem):
        push(ref, ref, unused.at[0], sem, partner).wait_recv()

    def left_here(ref, sem):
        push(ref, ref, sem, unused.at[0], partner).wait_send()

    def fold_queries():
        landed(qbuf.at[pl.ds(0, NT - 1)], qr.at[0])
        ready("key_up")
        wide[...] = key_up_v[...].astype(F32)
        for h in range(NT):
            up_h = wide[pl.ds(h, 256, stride=NT)].astype(BF16)
            folded = dot_nt(qbuf[h, :, :128], up_h).astype(BF16)
            folded = folded.reshape(NX, NC, SHARE, 256)
            rope = qbuf[h, :, 128:].reshape(NX, NC, SHARE, 128)
            for core in range(NC):
                first = (h // 2 * NC + core) * 128 + h % 2 * 64
                r = slice(first, first + 64)
                qf[r, :256] = folded[:, core].reshape(64, 256)
                qf[r, 256:] = rope[:, core].reshape(64, 128)

    def split_values():
        ready("value_up")
        wide[...] = value_up_v[...].astype(F32)
        for h in range(NT):
            vu[h // 2, h % 2 * 128 : h % 2 * 128 + 128] = wide[pl.ds(h, 256, stride=NT)].T.astype(BF16)

    def weigh(queries, spans, top):
        for at in spans:
            s_scr[at, queries] = dot_nt(kvbuf[at], qf[queries])
            here = jnp.max(s_scr[at, queries], axis=0, keepdims=True)
            top = here if top is None else jnp.maximum(top, here)
        total, mixed = 0.0, 0.0
        for at in spans:
            weights = jnp.exp2((s_scr[at, queries] - top) * scale2)
            total += jnp.sum(weights, axis=0, keepdims=True)
            mixed += dot_nn(kvt[:, at], weights.astype(BF16))
        return top, total, mixed

    scale2 = scale * 1.4426950408889634
    first, last = ((d + 8) * NY * SHARE for d in NEAR)
    near, far = [slice(first, last)], [slice(0, first), slice(last, KEYS)]
    groups = [slice(i * QG, (i + 1) * QG) for i in range(1024 // QG)]

    def weigh_near():
        landed(kvbuf.at[pl.ds(0, (NEAR[1] - NEAR[0]) * 3 * SHARE)], kvr.at[16])
        for at in near:
            kvt[:, at] = kvbuf[at, :256].T
        for i, queries in enumerate(groups):
            top, total, mixed = weigh(queries, near, None)
            near_stats[0:1, queries] = top
            near_stats[1:2, queries] = total
            near_mixed[:, queries] = mixed
            if i in W_NEAR:
                w_go(W_NEAR[i])

    for d in range(1, 9):
        if d == 4:
            fold_queries()
        if d == 6:
            split_values()
        if d == NEAR_AT:
            weigh_near()
        kv_wait(-d)
        if d + HOP <= 8:
            kv_to(-d, HOP, (zz(HOP), y, x, c))
        if d < 8:
            kv_wait(d)
            if d + HOP <= 7:
                kv_to(d, -HOP, (zz(-HOP), y, x, c))
        kv_to_y(-d)
        if d < 8:
            kv_to_y(d)
        if d in W_AT:
            w_go(W_AT[d])
    if NEAR_AT == 9:
        weigh_near()
    landed(kvbuf.at[pl.ds(0, (NZ - NEAR[1] + NEAR[0]) * 3 * SHARE)], kvr.at[17])
    for at in far:
        kvt[:, at] = kvbuf[at, :256].T
    lane = lax.broadcasted_iota(jnp.int32, (128, 256), 1)
    for i in range(2):
        pair = (x // 2 + 1 + i) % 2
        queries = pl.ds(pl.multiple_of(pair * QG, QG), QG)
        top_near = near_stats[0:1, queries]
        top, total, mixed = weigh(queries, far, top_near)
        factor = jnp.exp2((top_near - top) * scale2)
        total += factor * near_stats[1:2, queries]
        mixed += factor * near_mixed[:, queries]
        for k in range(2):
            cut = slice(k * 256, k * 256 + 256)
            part = dot_nn(vu[2 * pair + k], mixed[:, cut].astype(BF16))
            part = jnp.where((lane & 64) == 0, part[:128], part[128:]).astype(BF16)
            for core in range(NC):
                t = pair * 4 + k * NC + core
                at = slice(core * 128, core * 128 + 128)
                o_send[t] = part[:, at]
                st_send[t, 0:1] = top[:, cut][:, at]
                st_send[t, 1:2] = total[:, cut][:, at]
        for k in range(4):
            t = pair * 4 + (k + tp) % 4

            @pl.when(t != tp)
            def _():
                go(push(st_send.at[t], stats.at[tp], sts.at[0], str_.at[0], tp_peer(t)))
                go(push(o_send.at[t], o_recv.at[tp], os_.at[0], or_.at[0], tp_peer(t)))

        if i in W_ATTN:
            w_go(W_ATTN[i])
    o_recv[tp] = o_send[tp]
    stats[tp] = st_send[tp]
    w_go(W_MORE[0])
    push(owbuf.at[1 - c], owbuf.at[1 - c], ows.at[0], owr.at[0], partner).wait_recv()
    landed(stats.at[pl.ds(0, NT - 1)], str_.at[0])
    landed(o_recv.at[pl.ds(0, NT - 1)], or_.at[0])
    top_all = stats[0, 0:1]
    for t in range(1, NT):
        top_all = jnp.maximum(top_all, stats[t, 0:1])
    total_all = jnp.zeros_like(top_all)
    attended = jnp.zeros((128, 128), F32)
    for t in range(NT):
        factor = jnp.exp2((stats[t, 0:1] - top_all) * scale2)
        total_all += factor * stats[t, 1:2]
        attended += factor * o_recv[t].astype(F32)
    attended = (attended / total_all).T.astype(BF16)
    r_send[...] = (
        dot_nn(attended[:64], owbuf[0]) + dot_nn(attended[64:], owbuf[1])
    ).astype(BF16)
    for j in range(1, NX):
        xx = lax.rem(x + j, NX)
        src = r_send.at[pl.ds(pl.multiple_of(xx * SHARE, SHARE), SHARE)]
        go(push(src, r_recv.at[x], rss.at[0], rsr.at[0], (z, y, xx, c)))
    r_recv[x] = r_send[pl.ds(pl.multiple_of(x * SHARE, SHARE), SHARE)]
    w_go(W_MORE[1])
    landed(r_recv.at[pl.ds(0, NX - 1)], rsr.at[0])
    ready("resid", "post", "pre", "ffn")
    summed = r_recv[0].astype(F32)
    for j in range(1, NX):
        summed += r_recv[j].astype(F32)
    summed = summed.astype(BF16).astype(F32)
    flow = (resid_v[...].astype(F32) + rms_norm(summed, in_one_row(gains.at[0]))).astype(BF16).astype(F32)
    stream[...] = flow
    in_send[...] = rms_norm(flow, in_one_row(gains.at[1])).astype(BF16)

    def in_slot(s):
        return inbuf.at[pl.ds(pl.multiple_of(s * SHARE, SHARE), SHARE)]

    mine = (y % 2) * NT + tp

    def ag_copy(j):
        chip = lax.rem(y * NX + x + j, NY * NX)
        dev = (z, lax.div(chip, NX), lax.rem(chip, NX), half)
        return push(in_send, in_slot(mine), ags.at[0], agr.at[0], dev)

    @pl.loop(1, NY * NX)
    def _(j):
        ag_copy(j).start()

    @pl.when(half == c)
    def _():
        in_slot(mine)[...] = in_send[...]

    @pl.when(half != c)
    def _():
        ag_copy(0).start()

    w_go(W_MORE[2])

    ready("conv_value", "conv_gate")
    last = conv_v.shape[2] - UP
    for core in range(NC):
        first = (x * NC + core) * NY * HID + y * HID
        base = jnp.minimum(first // 128 * 128, last)
        lanes = pl.ds(pl.multiple_of(base, 128), UP)
        back = UP - (first - base)
        v = pltpu.roll(conv_v[0, :, lanes].astype(F32), back, 1)
        g = pltpu.roll(conv_v[1, :, lanes].astype(F32), back, 1)
        taps[core, 0:3] = jnp.concatenate(side_lanes(v[:, :HID], g[:, :HID]), axis=1)

    landed(wbuf.at[1 - c], wpr.at[0])


    @pl.when(half == c)
    def _():
        landed(inbuf.at[pl.ds(0, 15 * SHARE)], agr.at[0])

    @pl.when(half != c)
    def _():
        landed(inbuf, agr.at[0])

    for core in range(NC):
        up[core, 8 : 8 + TOK] = dot_nn(inbuf[...], wbuf[core])

    low_dev = ((z + c) % NZ, y, x, 1 - c)
    high_dev = ((z + c - 1 + NZ) % NZ, y, x, 1 - c)
    go(push(up.at[:, pl.ds(TOK, 8)], up.at[:, pl.ds(0, 8)], hs.at[0], hr.at[0], low_dev))
    go(push(up.at[:, pl.ds(8, 8)], up.at[:, pl.ds(TOK + 8, 8)], hs.at[1], hr.at[1], high_dev))
    def hidden_rows(core, first, count):
        conv = (
            up[core, first + 7 : first + 7 + count] * taps[core, 0:1]
            + up[core, first + 8 : first + 8 + count] * taps[core, 1:2]
            + up[core, first + 9 : first + 9 + count] * taps[core, 2:3]
        )
        gate = conv[:, 128:256]
        near = gate / (1.0 + jnp.exp(-gate)) * conv[:, :128]
        gate = pltpu.roll(conv[:, 256:], 64, 1)
        far = gate / (1.0 + jnp.exp(-gate)) * conv[:, 256:]
        lane = lax.broadcasted_iota(jnp.int32, far.shape, 1)
        far = jnp.where(lane < 64, far, 0.0)
        return jnp.concatenate([near.astype(BF16), far.astype(BF16)], axis=1)

    def down_rows(hidden):
        return (dot_nn(hidden[0], dbuf[0]) + dot_nn(hidden[1], dbuf[1])).astype(BF16)

    inner = [hidden_rows(core, SHARE, TOK - 2 * SHARE) for core in range(NC)]
    landed(dbuf.at[1 - c, pl.ds(0, HID)], wpr.at[1])

    p_send[SHARE : TOK - SHARE] = down_rows(inner)

    left_cols, right_cols = pl.ds(0, D // 2), pl.ds(D // 2, D // 2)
    yl = lax.rem(y, 2)

    def along_x(s):
        to = lax.rem(lax.div(s, NC), NX)
        src = p_send.at[pl.ds(pl.multiple_of(s * SHARE, SHARE), SHARE), left_cols]
        at = pl.multiple_of((lax.div(s, NT) * NC + lax.rem(s, NC)) * SHARE, SHARE)
        dst = a_recv.at[x, pl.ds(at, SHARE)]
        return to, push(src, dst, ps.at[0], pr.at[0], (z, y, to, c))

    def along_y(k, first, count):
        at = pl.ds(pl.multiple_of(k * ROWS + first, SHARE), count)
        dst = b_recv.at[y, pl.ds(first, count)]
        dev = (z, 2 * c + k, x, c)
        return push(p_send.at[at, right_cols], dst, ps.at[1], pr.at[1], dev)

    for k, first in ((0, SHARE), (1, 0)):

        @pl.when(2 * c + k != y)
        def _():
            along_y(k, first, ROWS - SHARE).start()

    @pl.loop(0, 16)
    def _(j):
        s = lax.rem(mine + 2 + j, 16)
        to, copy = along_x(s)

        @pl.when((to != x) & (s > 0) & (s < 15))
        def _():
            copy.start()

    low, high = up.at[:, pl.ds(0, 8)], up.at[:, pl.ds(TOK + 8, 8)]
    push(low, low, hs.at[0], hr.at[0], low_dev).wait_recv()
    push(high, high, hs.at[1], hr.at[1], high_dev).wait_recv()

    @pl.when((z == 0) & (c == 0))
    def _():
        up[:, 0:8] = jnp.zeros((NC, 8, UP), F32)

    @pl.when((z == NZ - 1) & (c == 1))
    def _():
        up[:, TOK + 8 : TOK + 16] = jnp.zeros((NC, 8, UP), F32)

    outer = [
        jnp.concatenate(
            [hidden_rows(core, 0, SHARE), hidden_rows(core, TOK - SHARE, SHARE)], axis=0
        )
        for core in range(NC)
    ]
    edges = down_rows(outer)
    p_send[:SHARE] = edges[:SHARE]
    p_send[TOK - SHARE :] = edges[SHARE:]
    for k, first, s in ((0, 0, 0), (1, ROWS - SHARE, 15)):

        @pl.when(2 * c + k != y)
        def _():
            along_y(k, first, SHARE).start()

        to, copy = along_x(jnp.int32(s))

        @pl.when(to != x)
        def _():
            copy.start()

    def own_part(k, first, count, cols):
        at = pl.multiple_of(k * ROWS + first, SHARE)
        return p_send[pl.ds(at, count), cols].astype(F32)

    landed(a_recv.at[pl.ds(0, NX - 1)], pr.at[0])
    total = jnp.concatenate([own_part(k, x * 32, 32, left_cols) for k in range(2)], axis=0)
    for j in range(1, NX):
        total += a_recv[lax.rem(x + j, NX)].astype(F32)
    a_send[...] = total.astype(BF16)

    def a_owner(k, core):
        at = (k * NC + core) * SHARE
        dev = (z, 2 * c + k, x, core)
        return push(a_send.at[pl.ds(at, SHARE)], fin.at[0, y], ps.at[2], pr.at[2], dev)

    for k in range(2):
        for core in range(NC):

            @pl.when((2 * c + k != y) | (c != core))
            def _():
                a_owner(k, core).start()

    def b_owner(j):
        t = lax.rem(tp + j, NT)
        at = pl.multiple_of(t * SHARE, SHARE)
        return push(b_send.at[pl.ds(at, SHARE)], fin.at[1, x], ps.at[3], pr.at[3], tp_peer(t))

    @pl.when(half == c)
    def _():
        landed(b_recv.at[pl.ds(0, NY - 1)], pr.at[1])
        total = own_part(yl, 0, ROWS, right_cols)
        for j in range(1, NY):
            total += b_recv[lax.rem(y + j, NY)].astype(F32)
        b_send[...] = total.astype(BF16)
        for j in range(1, NT):
            b_owner(j).start()
        fin[1, x] = b_send[pl.ds(pl.multiple_of(tp * SHARE, SHARE), SHARE)]
        fin[0, y] = a_send[pl.ds(pl.multiple_of((yl * NC + c) * SHARE, SHARE), SHARE)]

    for kind in range(2):

        @pl.when(half == c)
        def _():
            landed(fin.at[kind, pl.ds(0, 3)], pr.at[2 + kind])

        @pl.when(half != c)
        def _():
            landed(fin.at[kind], pr.at[2 + kind])

    sums = []
    for kind in range(2):
        part = fin[kind, 0].astype(F32)
        for k in range(1, 4):
            part += fin[kind, k].astype(F32)
        sums.append(part)
    projected = jnp.concatenate(sums, axis=1).astype(BF16).astype(F32)
    out[...] = (stream[...] + rms_norm(projected, in_one_row(gains.at[2]))).astype(BF16)

    left_here(kvbuf.at[pl.ds(0, 63 * SHARE)], kvs.at[0])
    left_here(qbuf.at[pl.ds(0, NT - 1)], qs.at[0])
    left_here(wbuf.at[0, pl.ds(0, 96)], wys.at[0])
    left_here(d_stage.at[pl.ds(0, 96)], wys.at[1])
    left_here(owbuf.at[0], ows.at[0])
    left_here(wbuf.at[0, pl.ds(0, 15 * ROWS)], wzs.at[0])
    left_here(dbuf.at[0, pl.ds(0, HID), pl.ds(0, 15 * ROWS)], wzs.at[1])
    left_here(wbuf.at[0], wps.at[0])
    left_here(dbuf.at[0, pl.ds(0, HID)], wps.at[1])
    left_here(stats.at[pl.ds(0, NT - 1)], sts.at[0])
    left_here(o_recv.at[pl.ds(0, NT - 1)], os_.at[0])
    left_here(r_recv.at[pl.ds(0, NX - 1)], rss.at[0])
    left_here(a_recv.at[pl.ds(0, NX - 1)], ps.at[0])
    both = up.at[:, pl.ds(0, 8)]
    left_here(both, hs.at[0])
    left_here(both, hs.at[1])

    @pl.when(half == c)
    def _():
        left_here(inbuf.at[pl.ds(0, 15 * SHARE)], ags.at[0])
        left_here(b_recv.at[0], ps.at[1])
        left_here(fin.at[0, pl.ds(0, 3)], ps.at[2])
        left_here(b_send.at[pl.ds(0, 7 * SHARE)], ps.at[3])

    @pl.when(half != c)
    def _():
        left_here(inbuf, ags.at[0])
        left_here(b_recv.at[pl.ds(0, 2)], ps.at[1])
        left_here(fin.at[0], ps.at[2])


def body(
    residual,
    query_nope,
    query_rope,
    latent,
    rope_key,
    kv_gain,
    key_up,
    value_up,
    out_weight,
    post_gain,
    pre_gain,
    ffn_gain,
    up_value,
    up_gate,
    conv_value,
    conv_gate,
    down_weight,
):
    scale = (query_nope.shape[2] + query_rope.shape[2]) ** (-0.5)
    by_row, by_col = turn_tables()

    dma = pltpu.SemaphoreType.DMA
    vmem = pltpu.VMEM
    return pl.pallas_call(
        functools.partial(layer_kernel, scale),
        out_shape=jax.ShapeDtypeStruct((SHARE, D), BF16),
        in_specs=[pl.BlockSpec(memory_space=pl.ANY)] * 19,
        out_specs=pl.BlockSpec(memory_space=vmem),
        scratch_shapes=[
            vmem((KEYS, KW), BF16),
            vmem((NT, ROWS, QW), BF16),
            vmem((NC, NZ * ROWS, UP), BF16),
            vmem((NC, 256, D), BF16),
            vmem((ROWS, 256), BF16),
            vmem((NC, 128, D), BF16),
            vmem((256, KEYS), BF16),
            vmem((KEYS, 1024), F32),
            vmem((8, 1024), F32),
            vmem((256, 1024), F32),
            vmem((NT, 8, 128), F32),
            vmem((NT, 8, 128), F32),
            vmem((NT, 128, 128), BF16),
            vmem((NT, 128, 128), BF16),
            vmem((64, D), BF16),
            vmem((NX, SHARE, D), BF16),
            vmem((SHARE, D), BF16),
            vmem((TOK, D), BF16),
            vmem((NC, TOK + 16, UP), F32),
            vmem((TOK, D), BF16),
            vmem((NX, 64, D // 2), BF16),
            vmem((NY, ROWS, D // 2), BF16),
            vmem((64, D // 2), BF16),
            vmem((ROWS, D // 2), BF16),
            vmem((2, 4, SHARE, D // 2), BF16),
            vmem((SHARE, D), F32),
            vmem((SHARE, 256), BF16),
            vmem((64, ROWS), BF16),
            vmem((ROWS, 128), BF16),
            vmem((64, ROWS), BF16),
            vmem((8, 128), F32),
            vmem((2, GRID, 128), F32),
            vmem(up_value.shape, BF16),
            vmem(up_gate.shape, BF16),
            vmem(down_weight.shape[::-1], BF16),
            vmem((256 * NT, 128), BF16),
            vmem((256 * NT, 128), BF16),
            vmem((SHARE, D), BF16),
            vmem((2, 128), BF16),
            vmem((3, D // 128, 128), BF16),
            vmem((2,) + conv_value.shape, BF16),
            vmem((2, ROWS, 128), F32),
            vmem((ROWS, 128), F32),
            vmem((NY, 32, UP), BF16),
            vmem((NY, 32, 256), BF16),
            vmem((256 * NT, 128), F32),
            vmem((NX * 256, KW), BF16),
            vmem((4, 256, 256), BF16),
            vmem((NC, 8, UP), F32),
        ]
        + [dma((n,)) for n in (19, 1, 1, 18, 1, 1, 2, 2, 2, 2)]
        + [dma((2, NZ))]
        + [dma((n,)) for n in (2, 1, 1, 1, 1, 1, 1, 1, 1, 1, 1, 2, 2, 4, 4)],
        compiler_params=pltpu.CompilerParams(
            collective_id=0, has_side_effects=True, vmem_limit_bytes=60 * 1024 * 1024
        ),
        name="layer",
    )(
        latent,
        rope_key.T,
        query_nope[:, 0],
        query_rope[:, 0].T,
        by_row,
        by_col,
        up_value,
        up_gate,
        down_weight.T,
        out_weight,
        key_up.reshape(-1, key_up.shape[2]),
        value_up.reshape(-1, value_up.shape[2]),
        residual,
        kv_gain.reshape(-1, 128),
        post_gain.reshape(-1, 128),
        pre_gain.reshape(-1, 128),
        ffn_gain.reshape(-1, 128),
        conv_value,
        conv_gate,
    )


def solution(mesh):
    torus = Mesh(mesh.devices.reshape(NZ, NY, NX, NC), AXES)
    return jax.shard_map(
        body,
        mesh=torus,
        in_specs=(
            P(SP, None),
            P(SP, TP, None),
            P(SP, TP, None),
            P(SP, None),
            P(SP, None),
            P(),
            P(),
            P(),
            P(TP, None),
            P(),
            P(),
            P(),
            P(SP, TP),
            P(SP, TP),
            P(),
            P(),
            P(TP, SP),
        ),
        out_specs=P(SP + TP, None),
        check_vma=False,
    )
```

```python
import functools

import jax
import jax.numpy as jnp
import numpy as np
from jax import lax
from jax.experimental import pallas as pl
from jax.experimental.pallas import tpu as pltpu
from jax.sharding import Mesh
from jax.sharding import PartitionSpec as P

GRID = 64
AXES = ("z", "y", "x", "c")
SP = ("z", "y")
TP = ("x", "c")
MESH_IDS = pl.DeviceIdType.MESH
F32 = jnp.float32
BF16 = jnp.bfloat16

epsilon = 1e-06
rope_base = 10000.0

NZ, NY, NX, NC = 16, 4, 4, 2
NT = NX * NC
PLANE = NY * NT
D = 2048
ROWS = 128
SHARE = 16
KEYS = NZ * NY * SHARE
QW = 256
KW = 384
UP = 384
HID = 176
W_AT = {2: [0], 5: [1]}
W_NEAR = {0: [2], 1: [3]}
W_ATTN = {0: [4], 1: [5]}
W_MORE = ([6, 7], [8, 9], [10, 11, 12, 13, 14, 15, 16])
HOP = 3
QG = 512
NEAR_AT = 9
NEAR = (-4, 6)
TOK = 256


def rms_norm(values, gain):
    return (
        values * lax.rsqrt(jnp.mean(values * values, axis=-1, keepdims=True) + epsilon) * gain
    )


def turn_tables():
    pairs = 16
    frequency = rope_base ** (-np.arange(pairs) / pairs)
    sign = np.repeat([-1.0, 1.0], pairs)

    def both(steps, at):
        angles = np.tile(np.arange(steps)[:, None] * frequency, (1, 2))
        table = np.zeros((2, steps, 128))
        table[0, :, at : at + 32] = np.cos(angles)
        table[1, :, at : at + 32] = np.sin(angles) * sign
        return table

    by_row = both(ROWS // GRID * NZ * NY, 0).reshape(2, NZ * NY, ROWS // GRID, 128)
    by_row = by_row.transpose(1, 0, 2, 3).reshape(NZ * NY, 2 * ROWS // GRID, 128)
    by_row = np.pad(by_row, ((0, 0), (0, 8 - 2 * ROWS // GRID), (0, 0)))
    return by_row.astype(np.float32), both(GRID, 32).astype(np.float32)


def turned(values, cosine, sine):
    lane = lax.broadcasted_iota(jnp.int32, values.shape, 1)
    other = jnp.where((lane & 16) == 0, pltpu.roll(values, 112, 1), pltpu.roll(values, 16, 1))
    return values * cosine + other * sine


def in_one_row(ref):
    folded = ref[...].astype(F32)
    return jnp.concatenate([folded[i : i + 1] for i in range(folded.shape[0])], axis=1)


def as_rows(columns):
    both = jnp.concatenate([columns.astype(F32), jnp.zeros(columns.shape, F32)], axis=0)
    return both.T


def dot_nn(a, b):
    return jnp.dot(a, b, preferred_element_type=F32)


def dot_nt(a, b):
    return lax.dot_general(a, b, (((1,), (1,)), ((), ())), preferred_element_type=F32)


def side_lanes(v, g):
    rest = HID - 128
    pad = jnp.zeros(v.shape[:-1] + (64 - rest,), v.dtype)
    return [v[:, :128], g[:, :128], v[:, 128:], pad, g[:, 128:], pad]


def layer_kernel(
    scale,
    latent,
    rope_key,
    q_nope,
    q_rope,
    by_row,
    by_col,
    up_value,
    up_gate,
    down,
    ow,
    key_up,
    value_up,
    resid,
    kv_gain,
    post_gain,
    pre_gain,
    ffn_gain,
    conv_value,
    conv_gate,
    out,
    kvbuf,
    qbuf,
    wbuf,
    dbuf,
    d_stage,
    owbuf,
    kvt,
    s_scr,
    near_stats,
    near_mixed,
    st_send,
    stats,
    o_send,
    o_recv,
    r_send,
    r_recv,
    in_send,
    inbuf,
    up,
    p_send,
    a_recv,
    b_recv,
    a_send,
    b_send,
    fin,
    stream,
    latent_v,
    rope_key_v,
    q_nope_v,
    q_rope_v,
    by_row_v,
    by_col_v,
    up_value_v,
    up_gate_v,
    down_v,
    key_up_v,
    value_up_v,
    resid_v,
    kv_gain_v,
    gains,
    conv_v,
    turns,
    key_rows,
    w_loc,
    d_loc,
    wide,
    qf,
    vu,
    taps,
    loads,
    unused,
    kvs,
    kvr,
    qs,
    qr,
    wys,
    wyr,
    wzs,
    wps,
    wzr,
    wpr,
    ows,
    owr,
    sts,
    str_,
    os_,
    or_,
    rss,
    rsr,
    ags,
    agr,
    hs,
    hr,
    ps,
    pr,
):
    z, y, x, c = (lax.axis_index(a) for a in AXES)
    tp = x * NC + c
    plane = y * NT + tp
    half = lax.div(y, 2)

    def zz(k):
        return lax.rem(z + k + NZ, NZ)

    def push(src, dst, ss, rs, dev):
        return pltpu.make_async_remote_copy(
            src_ref=src, dst_ref=dst, send_sem=ss, recv_sem=rs, device_id=dev,
            device_id_type=MESH_IDS,
        )

    partner = (z, y, x, 1 - c)
    right, left = (zz(1), y, x, c), (zz(-1), y, x, c)
    cross = ((z + 2 * c - 1 + NZ) % NZ, y, x, 1 - c)

    def on_plane(j):
        p = lax.rem(plane + j, PLANE)
        return (z, lax.div(p, NT), lax.rem(lax.div(p, NC), NX), lax.rem(p, NC))

    def tp_peer(t):
        return (z, y, lax.div(t, NC), lax.rem(t, NC))

    def own(ref):
        return ref.at[pl.ds(pl.multiple_of(tp * SHARE, SHARE), SHARE)]

    local = {}

    def load(name, src, dst):
        local[name] = pltpu.make_async_copy(src, dst, loads.at[len(local)])
        local[name].start()

    load("latent", own(latent), latent_v)
    load("rope_key", rope_key, rope_key_v)
    load("by_row", by_row.at[z * NY + y], by_row_v)
    load("by_col", by_col, by_col_v)
    load("post", post_gain, gains.at[0])
    load("pre", pre_gain, gains.at[1])
    load("ffn", ffn_gain, gains.at[2])
    load("kv_gain", kv_gain, kv_gain_v)

    def ready(*names):
        for name in names:
            local[name].wait()

    barrier = pltpu.get_barrier_semaphore()
    for hop in range(1, HOP + 1):
        for dev in ((zz(hop), y, x, c), (zz(-hop), y, x, c)):
            pl.semaphore_signal(barrier, inc=1, device_id=dev, device_id_type=MESH_IDS)
    pl.semaphore_signal(barrier, inc=1, device_id=cross, device_id_type=MESH_IDS)

    for j in range(1, NY):
        dev = (z, lax.rem(y + j, NY), x, c)
        pl.semaphore_signal(barrier, inc=1, device_id=dev, device_id_type=MESH_IDS)
    for j in range(1, NT):
        dev = tp_peer(lax.rem(tp + j, NT))
        pl.semaphore_signal(barrier, inc=1, device_id=dev, device_id_type=MESH_IDS)

    def kv_slot(yy, d):
        start = pl.multiple_of(((d + 8) * NY + yy) * SHARE, SHARE)
        return kvbuf.at[pl.ds(start, SHARE)]

    def w_slot(kind, core, k):
        at = pl.ds(pl.multiple_of(k * ROWS, ROWS), ROWS)
        if kind == 0:
            return wbuf.at[core, at]
        return dbuf.at[core, pl.ds(0, HID), at]

    def w_part(kind, yy):
        if kind == 0:
            return wbuf.at[c, pl.ds(pl.multiple_of(z * ROWS + yy * 32, 32), 32)]
        return d_stage.at[pl.ds(pl.multiple_of(yy * 32, 32), 32)]

    load("q_nope", q_nope, q_nope_v)
    load("q_rope", q_rope, q_rope_v)
    load("up_value", up_value, up_value_v)
    load("up_gate", up_gate, up_gate_v)
    load("down", down, down_v)
    load("ow", ow, owbuf.at[c])
    load("key_up", key_up, key_up_v)
    load("value_up", value_up, value_up_v)
    load("resid", own(resid), resid_v)
    load("conv_value", conv_value, conv_v.at[0])
    load("conv_gate", conv_gate, conv_v.at[1])

    ready("latent", "rope_key", "by_row", "by_col", "kv_gain")
    for i in range(2):
        grid_rows = [
            by_row_v[2 * i + j : 2 * i + j + 1] + by_col_v[i] for j in range(ROWS // GRID)
        ]
        turns[i] = jnp.concatenate(grid_rows, axis=0)
    rows = pl.ds(pl.multiple_of(tp * SHARE, SHARE), SHARE)
    kv_slot(y, 0)[:, :256] = rms_norm(
        latent_v[...].astype(F32), in_one_row(kv_gain_v)
    ).astype(BF16)
    key_rows[...] = as_rows(rope_key_v[...])
    kv_slot(y, 0)[:, 256:] = turned(key_rows[rows], turns[0, rows], turns[1, rows]).astype(BF16)

    pl.semaphore_wait(barrier, 2 * HOP + NY + NT - 1)

    def go(copy):
        copy.start()

    def kv_to(d, hop, dev):
        seen = d - hop
        go(push(kv_slot(y, d), kv_slot(y, seen), kvs.at[0], kvr.at[seen + 8], dev))

    def kv_to_y(d):
        slot = kv_slot(y, d)
        for j in range(1, NY):
            dev = (z, lax.rem(y + j, NY), x, c)
            go(push(slot, slot, kvs.at[0], kvr.at[16 if NEAR[0] <= d < NEAR[1] else 17], dev))

    for hop in range(HOP, 0, -1):
        kv_to(0, hop, (zz(hop), y, x, c))
        kv_to(0, -hop, (zz(-hop), y, x, c))
    kv_to_y(0)
    ready("q_nope", "q_rope")
    qbuf[tp, :, :128] = q_nope_v[...]
    qbuf[tp, :, 128:] = turned(as_rows(q_rope_v[...]), turns[0], turns[1]).astype(BF16)
    for j in range(1, NT):
        t = lax.rem(tp + j, NT)
        go(push(qbuf.at[tp], qbuf.at[tp], qs.at[0], qr.at[0], tp_peer(t)))

    ready("up_value", "up_gate", "down")
    value, gate = up_value_v[...].astype(F32), up_gate_v[...].astype(F32)
    across = down_v[...].astype(F32)
    for yy in range(NY):
        at = slice(yy * HID, (yy + 1) * HID)
        parts = side_lanes(value[:, at], gate[:, at])
        w_loc[yy] = jnp.concatenate(parts, axis=1).astype(BF16)
        parts = [across[:, at], jnp.zeros((32, 256 - HID), F32)]
        d_loc[yy] = jnp.concatenate(parts, axis=1).astype(BF16)
    for j in range(1, NY):
        yy = lax.rem(y + j, NY)
        dev = (z, yy, x, c)
        go(push(w_loc.at[yy], w_part(0, y), wys.at[0], wyr.at[0], dev))
        go(push(d_loc.at[yy], w_part(1, y), wys.at[1], wyr.at[1], dev))
    w_part(0, y)[...] = w_loc[y]
    w_part(1, y)[...] = d_loc[y]
    dbuf[:, HID:] = jnp.zeros((NC, 256 - HID, D), BF16)
    ready("ow")
    go(push(owbuf.at[c], owbuf.at[c], ows.at[0], owr.at[0], partner))

    def w_send(kind, k, to_right, to_left):
        slot = w_slot(kind, c, k)
        if to_right:
            go(push(slot, slot, wzs.at[kind], wzr.at[kind, k], right))
        if to_left:
            go(push(slot, slot, wzs.at[kind], wzr.at[kind, k], left))

    def w_across(kind, k):
        slot = w_slot(kind, c, k)
        go(push(slot, slot, wps.at[kind], wpr.at[kind], partner))

    def w_wait(kind, k, dev):
        slot = w_slot(kind, c, k)
        push(slot, slot, wzs.at[kind], wzr.at[kind, k], dev).wait_recv()

    def w_start():
        for kind in range(2):
            landed((wbuf.at[c] if kind == 0 else d_stage).at[pl.ds(0, 96)], wyr.at[kind])
            if kind == 1:
                columns = pl.ds(pl.multiple_of(z * ROWS, ROWS), ROWS)
                dbuf[c, :HID, columns] = d_stage[...].astype(F32).T[:HID].astype(BF16)
            w_send(kind, z, True, True)
            w_across(kind, z)

    def w_go(steps):
        for event in steps:
            if event == 0:
                w_start()
                continue
            step, kind = (event + 1) // 2, (event + 1) % 2
            k = zz(-step)
            w_wait(kind, k, left)
            w_send(kind, k, step < 8, False)
            w_across(kind, k)
            if step < 8:
                k = zz(step)
                w_wait(kind, k, right)
                w_send(kind, k, False, step < 7)
                w_across(kind, k)

    def kv_wait(d):
        slot = kv_slot(y, d)
        push(slot, slot, kvs.at[0], kvr.at[d + 8], right).wait_recv()

    def landed(ref, sem):
        push(ref, ref, unused.at[0], sem, partner).wait_recv()

    def left_here(ref, sem):
        push(ref, ref, sem, unused.at[0], partner).wait_send()

    def fold_queries():
        landed(qbuf.at[pl.ds(0, NT - 1)], qr.at[0])
        ready("key_up")
        wide[...] = key_up_v[...].astype(F32)
        for h in range(NT):
            up_h = wide[pl.ds(h, 256, stride=NT)].astype(BF16)
            folded = dot_nt(qbuf[h, :, :128], up_h).astype(BF16)
            folded = folded.reshape(NX, NC, SHARE, 256)
            rope = qbuf[h, :, 128:].reshape(NX, NC, SHARE, 128)
            for core in range(NC):
                first = (h // 2 * NC + core) * 128 + h % 2 * 64
                r = slice(first, first + 64)
                qf[r, :256] = folded[:, core].reshape(64, 256)
                qf[r, 256:] = rope[:, core].reshape(64, 128)

    def split_values():
        ready("value_up")
        wide[...] = value_up_v[...].astype(F32)
        for h in range(NT):
            vu[h // 2, h % 2 * 128 : h % 2 * 128 + 128] = wide[pl.ds(h, 256, stride=NT)].T.astype(BF16)

    def weigh(queries, spans, top):
        for at in spans:
            s_scr[at, queries] = dot_nt(kvbuf[at], qf[queries])
            here = jnp.max(s_scr[at, queries], axis=0, keepdims=True)
            top = here if top is None else jnp.maximum(top, here)
        total, mixed = 0.0, 0.0
        for at in spans:
            weights = jnp.exp2((s_scr[at, queries] - top) * scale2)
            total += jnp.sum(weights, axis=0, keepdims=True)
            mixed += dot_nn(kvt[:, at], weights.astype(BF16))
        return top, total, mixed

    scale2 = scale * 1.4426950408889634
    first, last = ((d + 8) * NY * SHARE for d in NEAR)
    near, far = [slice(first, last)], [slice(0, first), slice(last, KEYS)]
    groups = [slice(i * QG, (i + 1) * QG) for i in range(1024 // QG)]

    def weigh_near():
        landed(kvbuf.at[pl.ds(0, (NEAR[1] - NEAR[0]) * 3 * SHARE)], kvr.at[16])
        for at in near:
            kvt[:, at] = kvbuf[at, :256].T
        for i, queries in enumerate(groups):
            top, total, mixed = weigh(queries, near, None)
            near_stats[0:1, queries] = top
            near_stats[1:2, queries] = total
            near_mixed[:, queries] = mixed
            if i in W_NEAR:
                w_go(W_NEAR[i])

    for d in range(1, 9):
        if d == 4:
            fold_queries()
        if d == 6:
            split_values()
        if d == NEAR_AT:
            weigh_near()
        kv_wait(-d)
        if d + HOP <= 8:
            kv_to(-d, HOP, (zz(HOP), y, x, c))
        if d < 8:
            kv_wait(d)
            if d + HOP <= 7:
                kv_to(d, -HOP, (zz(-HOP), y, x, c))
        kv_to_y(-d)
        if d < 8:
            kv_to_y(d)
        if d in W_AT:
            w_go(W_AT[d])
    if NEAR_AT == 9:
        weigh_near()
    landed(kvbuf.at[pl.ds(0, (NZ - NEAR[1] + NEAR[0]) * 3 * SHARE)], kvr.at[17])
    for at in far:
        kvt[:, at] = kvbuf[at, :256].T
    lane = lax.broadcasted_iota(jnp.int32, (128, 256), 1)
    for i in range(2):
        pair = (x // 2 + 1 + i) % 2
        queries = pl.ds(pl.multiple_of(pair * QG, QG), QG)
        top_near = near_stats[0:1, queries]
        top, total, mixed = weigh(queries, far, top_near)
        factor = jnp.exp2((top_near - top) * scale2)
        total += factor * near_stats[1:2, queries]
        mixed += factor * near_mixed[:, queries]
        for k in range(2):
            cut = slice(k * 256, k * 256 + 256)
            part = dot_nn(vu[2 * pair + k], mixed[:, cut].astype(BF16))
            part = jnp.where((lane & 64) == 0, part[:128], part[128:]).astype(BF16)
            for core in range(NC):
                t = pair * 4 + k * NC + core
                at = slice(core * 128, core * 128 + 128)
                o_send[t] = part[:, at]
                st_send[t, 0:1] = top[:, cut][:, at]
                st_send[t, 1:2] = total[:, cut][:, at]
        for k in range(4):
            t = pair * 4 + (k + tp) % 4

            @pl.when(t != tp)
            def _():
                go(push(st_send.at[t], stats.at[tp], sts.at[0], str_.at[0], tp_peer(t)))
                go(push(o_send.at[t], o_recv.at[tp], os_.at[0], or_.at[0], tp_peer(t)))

        if i in W_ATTN:
            w_go(W_ATTN[i])
    o_recv[tp] = o_send[tp]
    stats[tp] = st_send[tp]
    w_go(W_MORE[0])
    push(owbuf.at[1 - c], owbuf.at[1 - c], ows.at[0], owr.at[0], partner).wait_recv()
    landed(stats.at[pl.ds(0, NT - 1)], str_.at[0])
    landed(o_recv.at[pl.ds(0, NT - 1)], or_.at[0])
    top_all = stats[0, 0:1]
    for t in range(1, NT):
        top_all = jnp.maximum(top_all, stats[t, 0:1])
    total_all = jnp.zeros_like(top_all)
    attended = jnp.zeros((128, 128), F32)
    for t in range(NT):
        factor = jnp.exp2((stats[t, 0:1] - top_all) * scale2)
        total_all += factor * stats[t, 1:2]
        attended += factor * o_recv[t].astype(F32)
    attended = (attended / total_all).T.astype(BF16)
    r_send[...] = (
        dot_nn(attended[:64], owbuf[0]) + dot_nn(attended[64:], owbuf[1])
    ).astype(BF16)
    for j in range(1, NX):
        xx = lax.rem(x + j, NX)
        src = r_send.at[pl.ds(pl.multiple_of(xx * SHARE, SHARE), SHARE)]
        go(push(src, r_recv.at[x], rss.at[0], rsr.at[0], (z, y, xx, c)))
    r_recv[x] = r_send[pl.ds(pl.multiple_of(x * SHARE, SHARE), SHARE)]
    w_go(W_MORE[1])
    landed(r_recv.at[pl.ds(0, NX - 1)], rsr.at[0])
    ready("resid", "post", "pre", "ffn")
    summed = r_recv[0].astype(F32)
    for j in range(1, NX):
        summed += r_recv[j].astype(F32)
    summed = summed.astype(BF16).astype(F32)
    flow = (resid_v[...].astype(F32) + rms_norm(summed, in_one_row(gains.at[0]))).astype(BF16).astype(F32)
    stream[...] = flow
    in_send[...] = rms_norm(flow, in_one_row(gains.at[1])).astype(BF16)

    def in_slot(s):
        return inbuf.at[pl.ds(pl.multiple_of(s * SHARE, SHARE), SHARE)]

    mine = (y % 2) * NT + tp

    def ag_copy(j):
        chip = lax.rem(y * NX + x + j, NY * NX)
        dev = (z, lax.div(chip, NX), lax.rem(chip, NX), half)
        return push(in_send, in_slot(mine), ags.at[0], agr.at[0], dev)

    @pl.loop(1, NY * NX)
    def _(j):
        ag_copy(j).start()

    @pl.when(half == c)
    def _():
        in_slot(mine)[...] = in_send[...]

    @pl.when(half != c)
    def _():
        ag_copy(0).start()

    w_go(W_MORE[2])

    ready("conv_value", "conv_gate")
    last = conv_v.shape[2] - UP
    for core in range(NC):
        first = (x * NC + core) * NY * HID + y * HID
        base = jnp.minimum(first // 128 * 128, last)
        lanes = pl.ds(pl.multiple_of(base, 128), UP)
        back = UP - (first - base)
        v = pltpu.roll(conv_v[0, :, lanes].astype(F32), back, 1)
        g = pltpu.roll(conv_v[1, :, lanes].astype(F32), back, 1)
        taps[core, 0:3] = jnp.concatenate(side_lanes(v[:, :HID], g[:, :HID]), axis=1)

    landed(wbuf.at[1 - c], wpr.at[0])


    @pl.when(half == c)
    def _():
        landed(inbuf.at[pl.ds(0, 15 * SHARE)], agr.at[0])

    @pl.when(half != c)
    def _():
        landed(inbuf, agr.at[0])

    for core in range(NC):
        up[core, 8 : 8 + TOK] = dot_nn(inbuf[...], wbuf[core])

    low_dev = ((z + c) % NZ, y, x, 1 - c)
    high_dev = ((z + c - 1 + NZ) % NZ, y, x, 1 - c)
    go(push(up.at[:, pl.ds(TOK, 8)], up.at[:, pl.ds(0, 8)], hs.at[0], hr.at[0], low_dev))
    go(push(up.at[:, pl.ds(8, 8)], up.at[:, pl.ds(TOK + 8, 8)], hs.at[1], hr.at[1], high_dev))
    def hidden_rows(core, first, count):
        conv = (
            up[core, first + 7 : first + 7 + count] * taps[core, 0:1]
            + up[core, first + 8 : first + 8 + count] * taps[core, 1:2]
            + up[core, first + 9 : first + 9 + count] * taps[core, 2:3]
        )
        gate = conv[:, 128:256]
        near = gate / (1.0 + jnp.exp(-gate)) * conv[:, :128]
        gate = pltpu.roll(conv[:, 256:], 64, 1)
        far = gate / (1.0 + jnp.exp(-gate)) * conv[:, 256:]
        lane = lax.broadcasted_iota(jnp.int32, far.shape, 1)
        far = jnp.where(lane < 64, far, 0.0)
        return jnp.concatenate([near.astype(BF16), far.astype(BF16)], axis=1)

    def down_rows(hidden):
        return (dot_nn(hidden[0], dbuf[0]) + dot_nn(hidden[1], dbuf[1])).astype(BF16)

    inner = [hidden_rows(core, SHARE, TOK - 2 * SHARE) for core in range(NC)]
    landed(dbuf.at[1 - c, pl.ds(0, HID)], wpr.at[1])

    p_send[SHARE : TOK - SHARE] = down_rows(inner)

    left_cols, right_cols = pl.ds(0, D // 2), pl.ds(D // 2, D // 2)
    yl = lax.rem(y, 2)

    def along_x(s):
        to = lax.rem(lax.div(s, NC), NX)
        src = p_send.at[pl.ds(pl.multiple_of(s * SHARE, SHARE), SHARE), left_cols]
        at = pl.multiple_of((lax.div(s, NT) * NC + lax.rem(s, NC)) * SHARE, SHARE)
        dst = a_recv.at[x, pl.ds(at, SHARE)]
        return to, push(src, dst, ps.at[0], pr.at[0], (z, y, to, c))

    def along_y(k, first, count):
        at = pl.ds(pl.multiple_of(k * ROWS + first, SHARE), count)
        dst = b_recv.at[y, pl.ds(first, count)]
        dev = (z, 2 * c + k, x, c)
        return push(p_send.at[at, right_cols], dst, ps.at[1], pr.at[1], dev)

    for k, first in ((0, SHARE), (1, 0)):

        @pl.when(2 * c + k != y)
        def _():
            along_y(k, first, ROWS - SHARE).start()

    @pl.loop(0, 16)
    def _(j):
        s = lax.rem(mine + 2 + j, 16)
        to, copy = along_x(s)

        @pl.when((to != x) & (s > 0) & (s < 15))
        def _():
            copy.start()

    low, high = up.at[:, pl.ds(0, 8)], up.at[:, pl.ds(TOK + 8, 8)]
    push(low, low, hs.at[0], hr.at[0], low_dev).wait_recv()
    push(high, high, hs.at[1], hr.at[1], high_dev).wait_recv()

    @pl.when((z == 0) & (c == 0))
    def _():
        up[:, 0:8] = jnp.zeros((NC, 8, UP), F32)

    @pl.when((z == NZ - 1) & (c == 1))
    def _():
        up[:, TOK + 8 : TOK + 16] = jnp.zeros((NC, 8, UP), F32)

    outer = [
        jnp.concatenate(
            [hidden_rows(core, 0, SHARE), hidden_rows(core, TOK - SHARE, SHARE)], axis=0
        )
        for core in range(NC)
    ]
    edges = down_rows(outer)
    p_send[:SHARE] = edges[:SHARE]
    p_send[TOK - SHARE :] = edges[SHARE:]
    for k, first, s in ((0, 0, 0), (1, ROWS - SHARE, 15)):

        @pl.when(2 * c + k != y)
        def _():
            along_y(k, first, SHARE).start()

        to, copy = along_x(jnp.int32(s))

        @pl.when(to != x)
        def _():
            copy.start()

    def own_part(k, first, count, cols):
        at = pl.multiple_of(k * ROWS + first, SHARE)
        return p_send[pl.ds(at, count), cols].astype(F32)

    landed(a_recv.at[pl.ds(0, NX - 1)], pr.at[0])
    total = jnp.concatenate([own_part(k, x * 32, 32, left_cols) for k in range(2)], axis=0)
    for j in range(1, NX):
        total += a_recv[lax.rem(x + j, NX)].astype(F32)
    a_send[...] = total.astype(BF16)

    def a_owner(k, core):
        at = (k * NC + core) * SHARE
        dev = (z, 2 * c + k, x, core)
        return push(a_send.at[pl.ds(at, SHARE)], fin.at[0, y], ps.at[2], pr.at[2], dev)

    for k in range(2):
        for core in range(NC):

            @pl.when((2 * c + k != y) | (c != core))
            def _():
                a_owner(k, core).start()

    def b_owner(j):
        t = lax.rem(tp + j, NT)
        at = pl.multiple_of(t * SHARE, SHARE)
        return push(b_send.at[pl.ds(at, SHARE)], fin.at[1, x], ps.at[3], pr.at[3], tp_peer(t))

    @pl.when(half == c)
    def _():
        landed(b_recv.at[pl.ds(0, NY - 1)], pr.at[1])
        total = own_part(yl, 0, ROWS, right_cols)
        for j in range(1, NY):
            total += b_recv[lax.rem(y + j, NY)].astype(F32)
        b_send[...] = total.astype(BF16)
        for j in range(1, NT):
            b_owner(j).start()
        fin[1, x] = b_send[pl.ds(pl.multiple_of(tp * SHARE, SHARE), SHARE)]
        fin[0, y] = a_send[pl.ds(pl.multiple_of((yl * NC + c) * SHARE, SHARE), SHARE)]

    for kind in range(2):

        @pl.when(half == c)
        def _():
            landed(fin.at[kind, pl.ds(0, 3)], pr.at[2 + kind])

        @pl.when(half != c)
        def _():
            landed(fin.at[kind], pr.at[2 + kind])

    sums = []
    for kind in range(2):
        part = fin[kind, 0].astype(F32)
        for k in range(1, 4):
            part += fin[kind, k].astype(F32)
        sums.append(part)
    projected = jnp.concatenate(sums, axis=1).astype(BF16).astype(F32)
    out[...] = (stream[...] + rms_norm(projected, in_one_row(gains.at[2]))).astype(BF16)

    left_here(kvbuf.at[pl.ds(0, 63 * SHARE)], kvs.at[0])
    left_here(qbuf.at[pl.ds(0, NT - 1)], qs.at[0])
    left_here(wbuf.at[0, pl.ds(0, 96)], wys.at[0])
    left_here(d_stage.at[pl.ds(0, 96)], wys.at[1])
    left_here(owbuf.at[0], ows.at[0])
    left_here(wbuf.at[0, pl.ds(0, 15 * ROWS)], wzs.at[0])
    left_here(dbuf.at[0, pl.ds(0, HID), pl.ds(0, 15 * ROWS)], wzs.at[1])
    left_here(wbuf.at[0], wps.at[0])
    left_here(dbuf.at[0, pl.ds(0, HID)], wps.at[1])
    left_here(stats.at[pl.ds(0, NT - 1)], sts.at[0])
    left_here(o_recv.at[pl.ds(0, NT - 1)], os_.at[0])
    left_here(r_recv.at[pl.ds(0, NX - 1)], rss.at[0])
    left_here(a_recv.at[pl.ds(0, NX - 1)], ps.at[0])
    both = up.at[:, pl.ds(0, 8)]
    left_here(both, hs.at[0])
    left_here(both, hs.at[1])

    @pl.when(half == c)
    def _():
        left_here(inbuf.at[pl.ds(0, 15 * SHARE)], ags.at[0])
        left_here(b_recv.at[0], ps.at[1])
        left_here(fin.at[0, pl.ds(0, 3)], ps.at[2])
        left_here(b_send.at[pl.ds(0, 7 * SHARE)], ps.at[3])

    @pl.when(half != c)
    def _():
        left_here(inbuf, ags.at[0])
        left_here(b_recv.at[pl.ds(0, 2)], ps.at[1])
        left_here(fin.at[0], ps.at[2])


def body(
    residual,
    query_nope,
    query_rope,
    latent,
    rope_key,
    kv_gain,
    key_up,
    value_up,
    out_weight,
    post_gain,
    pre_gain,
    ffn_gain,
    up_value,
    up_gate,
    conv_value,
    conv_gate,
    down_weight,
):
    scale = (query_nope.shape[2] + query_rope.shape[2]) ** (-0.5)
    by_row, by_col = turn_tables()

    dma = pltpu.SemaphoreType.DMA
    vmem = pltpu.VMEM
    return pl.pallas_call(
        functools.partial(layer_kernel, scale),
        out_shape=jax.ShapeDtypeStruct((SHARE, D), BF16),
        in_specs=[pl.BlockSpec(memory_space=pl.ANY)] * 19,
        out_specs=pl.BlockSpec(memory_space=vmem),
        scratch_shapes=[
            vmem((KEYS, KW), BF16),
            vmem((NT, ROWS, QW), BF16),
            vmem((NC, NZ * ROWS, UP), BF16),
            vmem((NC, 256, D), BF16),
            vmem((ROWS, 256), BF16),
            vmem((NC, 128, D), BF16),
            vmem((256, KEYS), BF16),
            vmem((KEYS, 1024), F32),
            vmem((8, 1024), F32),
            vmem((256, 1024), F32),
            vmem((NT, 8, 128), F32),
            vmem((NT, 8, 128), F32),
            vmem((NT, 128, 128), BF16),
            vmem((NT, 128, 128), BF16),
            vmem((64, D), BF16),
            vmem((NX, SHARE, D), BF16),
            vmem((SHARE, D), BF16),
            vmem((TOK, D), BF16),
            vmem((NC, TOK + 16, UP), F32),
            vmem((TOK, D), BF16),
            vmem((NX, 64, D // 2), BF16),
            vmem((NY, ROWS, D // 2), BF16),
            vmem((64, D // 2), BF16),
            vmem((ROWS, D // 2), BF16),
            vmem((2, 4, SHARE, D // 2), BF16),
            vmem((SHARE, D), F32),
            vmem((SHARE, 256), BF16),
            vmem((64, ROWS), BF16),
            vmem((ROWS, 128), BF16),
            vmem((64, ROWS), BF16),
            vmem((8, 128), F32),
            vmem((2, GRID, 128), F32),
            vmem(up_value.shape, BF16),
            vmem(up_gate.shape, BF16),
            vmem(down_weight.shape[::-1], BF16),
            vmem((256 * NT, 128), BF16),
            vmem((256 * NT, 128), BF16),
            vmem((SHARE, D), BF16),
            vmem((2, 128), BF16),
            vmem((3, D // 128, 128), BF16),
            vmem((2,) + conv_value.shape, BF16),
            vmem((2, ROWS, 128), F32),
            vmem((ROWS, 128), F32),
            vmem((NY, 32, UP), BF16),
            vmem((NY, 32, 256), BF16),
            vmem((256 * NT, 128), F32),
            vmem((NX * 256, KW), BF16),
            vmem((4, 256, 256), BF16),
            vmem((NC, 8, UP), F32),
        ]
        + [dma((n,)) for n in (19, 1, 1, 18, 1, 1, 2, 2, 2, 2)]
        + [dma((2, NZ))]
        + [dma((n,)) for n in (2, 1, 1, 1, 1, 1, 1, 1, 1, 1, 1, 2, 2, 4, 4)],
        compiler_params=pltpu.CompilerParams(
            collective_id=0, has_side_effects=True, vmem_limit_bytes=60 * 1024 * 1024
        ),
        name="layer",
    )(
        latent,
        rope_key.T,
        query_nope[:, 0],
        query_rope[:, 0].T,
        by_row,
        by_col,
        up_value,
        up_gate,
        down_weight.T,
        out_weight,
        key_up.reshape(-1, key_up.shape[2]),
        value_up.reshape(-1, value_up.shape[2]),
        residual,
        kv_gain.reshape(-1, 128),
        post_gain.reshape(-1, 128),
        pre_gain.reshape(-1, 128),
        ffn_gain.reshape(-1, 128),
        conv_value,
        conv_gate,
    )


def solution(mesh):
    torus = Mesh(mesh.devices.reshape(NZ, NY, NX, NC), AXES)
    return jax.shard_map(
        body,
        mesh=torus,
        in_specs=(
            P(SP, None),
            P(SP, TP, None),
            P(SP, TP, None),
            P(SP, None),
            P(SP, None),
            P(),
            P(),
            P(),
            P(TP, None),
            P(),
            P(),
            P(),
            P(SP, TP),
            P(SP, TP),
            P(),
            P(),
            P(TP, SP),
        ),
        out_specs=P(SP + TP, None),
        check_vma=False,
    )
```

```python
import functools

import jax
import jax.numpy as jnp
import numpy as np
from jax import lax
from jax.experimental import pallas as pl
from jax.experimental.pallas import tpu as pltpu
from jax.sharding import Mesh
from jax.sharding import PartitionSpec as P

GRID = 64
AXES = ("z", "y", "x", "c")
SP = ("z", "y")
TP = ("x", "c")
MESH_IDS = pl.DeviceIdType.MESH
F32 = jnp.float32
BF16 = jnp.bfloat16

epsilon = 1e-06
rope_base = 10000.0

NZ, NY, NX, NC = 16, 4, 4, 2
NT = NX * NC
PLANE = NY * NT
D = 2048
ROWS = 128
SHARE = 16
KEYS = NZ * NY * SHARE
QW = 256
KW = 384
UP = 384
HID = 176
W_AT = {2: [0], 5: [1]}
W_NEAR = {0: [2], 1: [3]}
W_ATTN = {0: [4], 1: [5]}
W_MORE = ([6, 7], [8, 9], [10, 11, 12, 13, 14, 15, 16])
HOP = 3
QG = 512
NEAR_AT = 9
NEAR = (-4, 6)
TOK = 256


def rms_norm(values, gain):
    return (
        values * lax.rsqrt(jnp.mean(values * values, axis=-1, keepdims=True) + epsilon) * gain
    )


def turn_tables():
    pairs = 16
    frequency = rope_base ** (-np.arange(pairs) / pairs)
    sign = np.repeat([-1.0, 1.0], pairs)

    def both(steps, at):
        angles = np.tile(np.arange(steps)[:, None] * frequency, (1, 2))
        table = np.zeros((2, steps, 128))
        table[0, :, at : at + 32] = np.cos(angles)
        table[1, :, at : at + 32] = np.sin(angles) * sign
        return table

    by_row = both(ROWS // GRID * NZ * NY, 0).reshape(2, NZ * NY, ROWS // GRID, 128)
    by_row = by_row.transpose(1, 0, 2, 3).reshape(NZ * NY, 2 * ROWS // GRID, 128)
    by_row = np.pad(by_row, ((0, 0), (0, 8 - 2 * ROWS // GRID), (0, 0)))
    return by_row.astype(np.float32), both(GRID, 32).astype(np.float32)


def turned(values, cosine, sine):
    lane = lax.broadcasted_iota(jnp.int32, values.shape, 1)
    other = jnp.where((lane & 16) == 0, pltpu.roll(values, 112, 1), pltpu.roll(values, 16, 1))
    return values * cosine + other * sine


def in_one_row(ref):
    folded = ref[...].astype(F32)
    return jnp.concatenate([folded[i : i + 1] for i in range(folded.shape[0])], axis=1)


def as_rows(columns):
    both = jnp.concatenate([columns.astype(F32), jnp.zeros(columns.shape, F32)], axis=0)
    return both.T


def dot_nn(a, b):
    return jnp.dot(a, b, preferred_element_type=F32)


def dot_nt(a, b):
    return lax.dot_general(a, b, (((1,), (1,)), ((), ())), preferred_element_type=F32)


def side_lanes(v, g):
    rest = HID - 128
    pad = jnp.zeros(v.shape[:-1] + (64 - rest,), v.dtype)
    return [v[:, :128], g[:, :128], v[:, 128:], pad, g[:, 128:], pad]


def layer_kernel(
    scale,
    latent,
    rope_key,
    q_nope,
    q_rope,
    by_row,
    by_col,
    up_value,
    up_gate,
    down,
    ow,
    key_up,
    value_up,
    resid,
    kv_gain,
    post_gain,
    pre_gain,
    ffn_gain,
    conv_value,
    conv_gate,
    out,
    kvbuf,
    qbuf,
    wbuf,
    dbuf,
    d_stage,
    owbuf,
    kvt,
    s_scr,
    near_stats,
    near_mixed,
    st_send,
    stats,
    o_send,
    o_recv,
    r_send,
    r_recv,
    in_send,
    inbuf,
    up,
    p_send,
    a_recv,
    b_recv,
    a_send,
    b_send,
    fin,
    stream,
    latent_v,
    rope_key_v,
    q_nope_v,
    q_rope_v,
    by_row_v,
    by_col_v,
    up_value_v,
    up_gate_v,
    down_v,
    key_up_v,
    value_up_v,
    resid_v,
    kv_gain_v,
    gains,
    conv_v,
    turns,
    key_rows,
    w_loc,
    d_loc,
    wide,
    qf,
    vu,
    taps,
    loads,
    unused,
    kvs,
    kvr,
    qs,
    qr,
    wys,
    wyr,
    wzs,
    wps,
    wzr,
    wpr,
    ows,
    owr,
    sts,
    str_,
    os_,
    or_,
    rss,
    rsr,
    ags,
    agr,
    hs,
    hr,
    ps,
    pr,
):
    z, y, x, c = (lax.axis_index(a) for a in AXES)
    tp = x * NC + c
    plane = y * NT + tp
    half = lax.div(y, 2)

    def zz(k):
        return lax.rem(z + k + NZ, NZ)

    def push(src, dst, ss, rs, dev):
        return pltpu.make_async_remote_copy(
            src_ref=src, dst_ref=dst, send_sem=ss, recv_sem=rs, device_id=dev,
            device_id_type=MESH_IDS,
        )

    partner = (z, y, x, 1 - c)
    right, left = (zz(1), y, x, c), (zz(-1), y, x, c)
    cross = ((z + 2 * c - 1 + NZ) % NZ, y, x, 1 - c)

    def on_plane(j):
        p = lax.rem(plane + j, PLANE)
        return (z, lax.div(p, NT), lax.rem(lax.div(p, NC), NX), lax.rem(p, NC))

    def tp_peer(t):
        return (z, y, lax.div(t, NC), lax.rem(t, NC))

    def own(ref):
        return ref.at[pl.ds(pl.multiple_of(tp * SHARE, SHARE), SHARE)]

    local = {}

    def load(name, src, dst):
        local[name] = pltpu.make_async_copy(src, dst, loads.at[len(local)])
        local[name].start()

    load("latent", own(latent), latent_v)
    load("rope_key", rope_key, rope_key_v)
    load("by_row", by_row.at[z * NY + y], by_row_v)
    load("by_col", by_col, by_col_v)
    load("post", post_gain, gains.at[0])
    load("pre", pre_gain, gains.at[1])
    load("ffn", ffn_gain, gains.at[2])
    load("kv_gain", kv_gain, kv_gain_v)

    def ready(*names):
        for name in names:
            local[name].wait()

    barrier = pltpu.get_barrier_semaphore()
    for hop in range(1, HOP + 1):
        for dev in ((zz(hop), y, x, c), (zz(-hop), y, x, c)):
            pl.semaphore_signal(barrier, inc=1, device_id=dev, device_id_type=MESH_IDS)
    pl.semaphore_signal(barrier, inc=1, device_id=cross, device_id_type=MESH_IDS)

    for j in range(1, NY):
        dev = (z, lax.rem(y + j, NY), x, c)
        pl.semaphore_signal(barrier, inc=1, device_id=dev, device_id_type=MESH_IDS)
    for j in range(1, NT):
        dev = tp_peer(lax.rem(tp + j, NT))
        pl.semaphore_signal(barrier, inc=1, device_id=dev, device_id_type=MESH_IDS)

    def kv_slot(yy, d):
        start = pl.multiple_of(((d + 8) * NY + yy) * SHARE, SHARE)
        return kvbuf.at[pl.ds(start, SHARE)]

    def w_slot(kind, core, k):
        at = pl.ds(pl.multiple_of(k * ROWS, ROWS), ROWS)
        if kind == 0:
            return wbuf.at[core, at]
        return dbuf.at[core, pl.ds(0, HID), at]

    def w_part(kind, yy):
        if kind == 0:
            return wbuf.at[c, pl.ds(pl.multiple_of(z * ROWS + yy * 32, 32), 32)]
        return d_stage.at[pl.ds(pl.multiple_of(yy * 32, 32), 32)]

    load("q_nope", q_nope, q_nope_v)
    load("q_rope", q_rope, q_rope_v)
    load("up_value", up_value, up_value_v)
    load("up_gate", up_gate, up_gate_v)
    load("down", down, down_v)
    load("ow", ow, owbuf.at[c])
    load("key_up", key_up, key_up_v)
    load("value_up", value_up, value_up_v)
    load("resid", own(resid), resid_v)
    load("conv_value", conv_value, conv_v.at[0])
    load("conv_gate", conv_gate, conv_v.at[1])

    ready("latent", "rope_key", "by_row", "by_col", "kv_gain")
    for i in range(2):
        grid_rows = [
            by_row_v[2 * i + j : 2 * i + j + 1] + by_col_v[i] for j in range(ROWS // GRID)
        ]
        turns[i] = jnp.concatenate(grid_rows, axis=0)
    rows = pl.ds(pl.multiple_of(tp * SHARE, SHARE), SHARE)
    kv_slot(y, 0)[:, :256] = rms_norm(
        latent_v[...].astype(F32), in_one_row(kv_gain_v)
    ).astype(BF16)
    key_rows[...] = as_rows(rope_key_v[...])
    kv_slot(y, 0)[:, 256:] = turned(key_rows[rows], turns[0, rows], turns[1, rows]).astype(BF16)

    pl.semaphore_wait(barrier, 2 * HOP + NY + NT - 1)

    def go(copy):
        copy.start()

    def kv_to(d, hop, dev):
        seen = d - hop
        go(push(kv_slot(y, d), kv_slot(y, seen), kvs.at[0], kvr.at[seen + 8], dev))

    def kv_to_y(d):
        slot = kv_slot(y, d)
        for j in range(1, NY):
            dev = (z, lax.rem(y + j, NY), x, c)
            go(push(slot, slot, kvs.at[0], kvr.at[16 if NEAR[0] <= d < NEAR[1] else 17], dev))

    for hop in range(HOP, 0, -1):
        kv_to(0, hop, (zz(hop), y, x, c))
        kv_to(0, -hop, (zz(-hop), y, x, c))
    kv_to_y(0)
    ready("q_nope", "q_rope")
    qbuf[tp, :, :128] = q_nope_v[...]
    qbuf[tp, :, 128:] = turned(as_rows(q_rope_v[...]), turns[0], turns[1]).astype(BF16)
    for j in range(1, NT):
        t = lax.rem(tp + j, NT)
        go(push(qbuf.at[tp], qbuf.at[tp], qs.at[0], qr.at[0], tp_peer(t)))

    ready("up_value", "up_gate", "down")
    value, gate = up_value_v[...].astype(F32), up_gate_v[...].astype(F32)
    across = down_v[...].astype(F32)
    for yy in range(NY):
        at = slice(yy * HID, (yy + 1) * HID)
        parts = side_lanes(value[:, at], gate[:, at])
        w_loc[yy] = jnp.concatenate(parts, axis=1).astype(BF16)
        parts = [across[:, at], jnp.zeros((32, 256 - HID), F32)]
        d_loc[yy] = jnp.concatenate(parts, axis=1).astype(BF16)
    for j in range(1, NY):
        yy = lax.rem(y + j, NY)
        dev = (z, yy, x, c)
        go(push(w_loc.at[yy], w_part(0, y), wys.at[0], wyr.at[0], dev))
        go(push(d_loc.at[yy], w_part(1, y), wys.at[1], wyr.at[1], dev))
    w_part(0, y)[...] = w_loc[y]
    w_part(1, y)[...] = d_loc[y]
    dbuf[:, HID:] = jnp.zeros((NC, 256 - HID, D), BF16)
    ready("ow")
    go(push(owbuf.at[c], owbuf.at[c], ows.at[0], owr.at[0], partner))

    def w_send(kind, k, to_right, to_left):
        slot = w_slot(kind, c, k)
        if to_right:
            go(push(slot, slot, wzs.at[kind], wzr.at[kind, k], right))
        if to_left:
            go(push(slot, slot, wzs.at[kind], wzr.at[kind, k], left))

    def w_across(kind, k):
        slot = w_slot(kind, c, k)
        go(push(slot, slot, wps.at[kind], wpr.at[kind], partner))

    def w_wait(kind, k, dev):
        slot = w_slot(kind, c, k)
        push(slot, slot, wzs.at[kind], wzr.at[kind, k], dev).wait_recv()

    def w_start():
        for kind in range(2):
            landed((wbuf.at[c] if kind == 0 else d_stage).at[pl.ds(0, 96)], wyr.at[kind])
            if kind == 1:
                columns = pl.ds(pl.multiple_of(z * ROWS, ROWS), ROWS)
                dbuf[c, :HID, columns] = d_stage[...].astype(F32).T[:HID].astype(BF16)
            w_send(kind, z, True, True)
            w_across(kind, z)

    def w_go(steps):
        for event in steps:
            if event == 0:
                w_start()
                continue
            step, kind = (event + 1) // 2, (event + 1) % 2
            k = zz(-step)
            w_wait(kind, k, left)
            w_send(kind, k, step < 8, False)
            w_across(kind, k)
            if step < 8:
                k = zz(step)
                w_wait(kind, k, right)
                w_send(kind, k, False, step < 7)
                w_across(kind, k)

    def kv_wait(d):
        slot = kv_slot(y, d)
        push(slot, slot, kvs.at[0], kvr.at[d + 8], right).wait_recv()

    def landed(ref, sem):
        push(ref, ref, unused.at[0], sem, partner).wait_recv()

    def left_here(ref, sem):
        push(ref, ref, sem, unused.at[0], partner).wait_send()

    def fold_queries():
        landed(qbuf.at[pl.ds(0, NT - 1)], qr.at[0])
        ready("key_up")
        wide[...] = key_up_v[...].astype(F32)
        for h in range(NT):
            up_h = wide[pl.ds(h, 256, stride=NT)].astype(BF16)
            folded = dot_nt(qbuf[h, :, :128], up_h).astype(BF16)
            folded = folded.reshape(NX, NC, SHARE, 256)
            rope = qbuf[h, :, 128:].reshape(NX, NC, SHARE, 128)
            for core in range(NC):
                first = (h // 2 * NC + core) * 128 + h % 2 * 64
                r = slice(first, first + 64)
                qf[r, :256] = folded[:, core].reshape(64, 256)
                qf[r, 256:] = rope[:, core].reshape(64, 128)

    def split_values():
        ready("value_up")
        wide[...] = value_up_v[...].astype(F32)
        for h in range(NT):
            vu[h // 2, h % 2 * 128 : h % 2 * 128 + 128] = wide[pl.ds(h, 256, stride=NT)].T.astype(BF16)

    def weigh(queries, spans, top):
        for at in spans:
            s_scr[at, queries] = dot_nt(kvbuf[at], qf[queries])
            here = jnp.max(s_scr[at, queries], axis=0, keepdims=True)
            top = here if top is None else jnp.maximum(top, here)
        total, mixed = 0.0, 0.0
        for at in spans:
            weights = jnp.exp2((s_scr[at, queries] - top) * scale2)
            total += jnp.sum(weights, axis=0, keepdims=True)
            mixed += dot_nn(kvt[:, at], weights.astype(BF16))
        return top, total, mixed

    scale2 = scale * 1.4426950408889634
    first, last = ((d + 8) * NY * SHARE for d in NEAR)
    near, far = [slice(first, last)], [slice(0, first), slice(last, KEYS)]
    groups = [slice(i * QG, (i + 1) * QG) for i in range(1024 // QG)]

    def weigh_near():
        landed(kvbuf.at[pl.ds(0, (NEAR[1] - NEAR[0]) * 3 * SHARE)], kvr.at[16])
        for at in near:
            kvt[:, at] = kvbuf[at, :256].T
        for i, queries in enumerate(groups):
            top, total, mixed = weigh(queries, near, None)
            near_stats[0:1, queries] = top
            near_stats[1:2, queries] = total
            near_mixed[:, queries] = mixed
            if i in W_NEAR:
                w_go(W_NEAR[i])

    for d in range(1, 9):
        if d == 4:
            fold_queries()
        if d == 6:
            split_values()
        if d == NEAR_AT:
            weigh_near()
        kv_wait(-d)
        if d + HOP <= 8:
            kv_to(-d, HOP, (zz(HOP), y, x, c))
        if d < 8:
            kv_wait(d)
            if d + HOP <= 7:
                kv_to(d, -HOP, (zz(-HOP), y, x, c))
        kv_to_y(-d)
        if d < 8:
            kv_to_y(d)
        if d in W_AT:
            w_go(W_AT[d])
    if NEAR_AT == 9:
        weigh_near()
    landed(kvbuf.at[pl.ds(0, (NZ - NEAR[1] + NEAR[0]) * 3 * SHARE)], kvr.at[17])
    for at in far:
        kvt[:, at] = kvbuf[at, :256].T
    lane = lax.broadcasted_iota(jnp.int32, (128, 256), 1)
    for i in range(2):
        pair = (x // 2 + 1 + i) % 2
        queries = pl.ds(pl.multiple_of(pair * QG, QG), QG)
        top_near = near_stats[0:1, queries]
        top, total, mixed = weigh(queries, far, top_near)
        factor = jnp.exp2((top_near - top) * scale2)
        total += factor * near_stats[1:2, queries]
        mixed += factor * near_mixed[:, queries]
        for k in range(2):
            cut = slice(k * 256, k * 256 + 256)
            part = dot_nn(vu[2 * pair + k], mixed[:, cut].astype(BF16))
            part = jnp.where((lane & 64) == 0, part[:128], part[128:]).astype(BF16)
            for core in range(NC):
                t = pair * 4 + k * NC + core
                at = slice(core * 128, core * 128 + 128)
                o_send[t] = part[:, at]
                st_send[t, 0:1] = top[:, cut][:, at]
                st_send[t, 1:2] = total[:, cut][:, at]
        for k in range(4):
            t = pair * 4 + (k + tp) % 4

            @pl.when(t != tp)
            def _():
                go(push(st_send.at[t], stats.at[tp], sts.at[0], str_.at[0], tp_peer(t)))
                go(push(o_send.at[t], o_recv.at[tp], os_.at[0], or_.at[0], tp_peer(t)))

        if i in W_ATTN:
            w_go(W_ATTN[i])
    o_recv[tp] = o_send[tp]
    stats[tp] = st_send[tp]
    w_go(W_MORE[0])
    push(owbuf.at[1 - c], owbuf.at[1 - c], ows.at[0], owr.at[0], partner).wait_recv()
    landed(stats.at[pl.ds(0, NT - 1)], str_.at[0])
    landed(o_recv.at[pl.ds(0, NT - 1)], or_.at[0])
    top_all = stats[0, 0:1]
    for t in range(1, NT):
        top_all = jnp.maximum(top_all, stats[t, 0:1])
    total_all = jnp.zeros_like(top_all)
    attended = jnp.zeros((128, 128), F32)
    for t in range(NT):
        factor = jnp.exp2((stats[t, 0:1] - top_all) * scale2)
        total_all += factor * stats[t, 1:2]
        attended += factor * o_recv[t].astype(F32)
    attended = (attended / total_all).T.astype(BF16)
    r_send[...] = (
        dot_nn(attended[:64], owbuf[0]) + dot_nn(attended[64:], owbuf[1])
    ).astype(BF16)
    for j in range(1, NX):
        xx = lax.rem(x + j, NX)
        src = r_send.at[pl.ds(pl.multiple_of(xx * SHARE, SHARE), SHARE)]
        go(push(src, r_recv.at[x], rss.at[0], rsr.at[0], (z, y, xx, c)))
    r_recv[x] = r_send[pl.ds(pl.multiple_of(x * SHARE, SHARE), SHARE)]
    w_go(W_MORE[1])
    landed(r_recv.at[pl.ds(0, NX - 1)], rsr.at[0])
    ready("resid", "post", "pre", "ffn")
    summed = r_recv[0].astype(F32)
    for j in range(1, NX):
        summed += r_recv[j].astype(F32)
    summed = summed.astype(BF16).astype(F32)
    flow = (resid_v[...].astype(F32) + rms_norm(summed, in_one_row(gains.at[0]))).astype(BF16).astype(F32)
    stream[...] = flow
    in_send[...] = rms_norm(flow, in_one_row(gains.at[1])).astype(BF16)

    def in_slot(s):
        return inbuf.at[pl.ds(pl.multiple_of(s * SHARE, SHARE), SHARE)]

    mine = (y % 2) * NT + tp

    def ag_copy(j):
        chip = lax.rem(y * NX + x + j, NY * NX)
        dev = (z, lax.div(chip, NX), lax.rem(chip, NX), half)
        return push(in_send, in_slot(mine), ags.at[0], agr.at[0], dev)

    @pl.loop(1, NY * NX)
    def _(j):
        ag_copy(j).start()

    @pl.when(half == c)
    def _():
        in_slot(mine)[...] = in_send[...]

    @pl.when(half != c)
    def _():
        ag_copy(0).start()

    w_go(W_MORE[2])

    ready("conv_value", "conv_gate")
    last = conv_v.shape[2] - UP
    for core in range(NC):
        first = (x * NC + core) * NY * HID + y * HID
        base = jnp.minimum(first // 128 * 128, last)
        lanes = pl.ds(pl.multiple_of(base, 128), UP)
        back = UP - (first - base)
        v = pltpu.roll(conv_v[0, :, lanes].astype(F32), back, 1)
        g = pltpu.roll(conv_v[1, :, lanes].astype(F32), back, 1)
        taps[core, 0:3] = jnp.concatenate(side_lanes(v[:, :HID], g[:, :HID]), axis=1)

    landed(wbuf.at[1 - c], wpr.at[0])


    @pl.when(half == c)
    def _():
        landed(inbuf.at[pl.ds(0, 15 * SHARE)], agr.at[0])

    @pl.when(half != c)
    def _():
        landed(inbuf, agr.at[0])

    for core in range(NC):
        up[core, 8 : 8 + TOK] = dot_nn(inbuf[...], wbuf[core])

    low_dev = ((z + c) % NZ, y, x, 1 - c)
    high_dev = ((z + c - 1 + NZ) % NZ, y, x, 1 - c)
    go(push(up.at[:, pl.ds(TOK, 8)], up.at[:, pl.ds(0, 8)], hs.at[0], hr.at[0], low_dev))
    go(push(up.at[:, pl.ds(8, 8)], up.at[:, pl.ds(TOK + 8, 8)], hs.at[1], hr.at[1], high_dev))
    def hidden_rows(core, first, count):
        conv = (
            up[core, first + 7 : first + 7 + count] * taps[core, 0:1]
            + up[core, first + 8 : first + 8 + count] * taps[core, 1:2]
            + up[core, first + 9 : first + 9 + count] * taps[core, 2:3]
        )
        gate = conv[:, 128:256]
        near = gate / (1.0 + jnp.exp(-gate)) * conv[:, :128]
        gate = pltpu.roll(conv[:, 256:], 64, 1)
        far = gate / (1.0 + jnp.exp(-gate)) * conv[:, 256:]
        lane = lax.broadcasted_iota(jnp.int32, far.shape, 1)
        far = jnp.where(lane < 64, far, 0.0)
        return jnp.concatenate([near.astype(BF16), far.astype(BF16)], axis=1)

    def down_rows(hidden, cols):
        total = dot_nn(hidden[0], dbuf[0, :, cols]) + dot_nn(hidden[1], dbuf[1, :, cols])
        return total.astype(BF16)

    inner = [hidden_rows(core, SHARE, TOK - 2 * SHARE) for core in range(NC)]
    landed(dbuf.at[1 - c, pl.ds(0, HID)], wpr.at[1])

    p_send[SHARE : TOK - SHARE, D // 2 :] = down_rows(inner, slice(D // 2, D))

    left_cols, right_cols = pl.ds(0, D // 2), pl.ds(D // 2, D // 2)
    yl = lax.rem(y, 2)

    def along_x(s):
        to = lax.rem(lax.div(s, NC), NX)
        src = p_send.at[pl.ds(pl.multiple_of(s * SHARE, SHARE), SHARE), left_cols]
        at = pl.multiple_of((lax.div(s, NT) * NC + lax.rem(s, NC)) * SHARE, SHARE)
        dst = a_recv.at[x, pl.ds(at, SHARE)]
        return to, push(src, dst, ps.at[0], pr.at[0], (z, y, to, c))

    def along_y(k, first, count):
        at = pl.ds(pl.multiple_of(k * ROWS + first, SHARE), count)
        dst = b_recv.at[y, pl.ds(first, count)]
        dev = (z, 2 * c + k, x, c)
        return push(p_send.at[at, right_cols], dst, ps.at[1], pr.at[1], dev)

    for k, first in ((0, SHARE), (1, 0)):

        @pl.when(2 * c + k != y)
        def _():
            along_y(k, first, ROWS - SHARE).start()

    p_send[SHARE : TOK - SHARE, : D // 2] = down_rows(inner, slice(0, D // 2))

    @pl.loop(0, 16)
    def _(j):
        s = lax.rem(mine + 2 + j, 16)
        to, copy = along_x(s)

        @pl.when((to != x) & (s > 0) & (s < 15))
        def _():
            copy.start()

    low, high = up.at[:, pl.ds(0, 8)], up.at[:, pl.ds(TOK + 8, 8)]
    push(low, low, hs.at[0], hr.at[0], low_dev).wait_recv()
    push(high, high, hs.at[1], hr.at[1], high_dev).wait_recv()

    @pl.when((z == 0) & (c == 0))
    def _():
        up[:, 0:8] = jnp.zeros((NC, 8, UP), F32)

    @pl.when((z == NZ - 1) & (c == 1))
    def _():
        up[:, TOK + 8 : TOK + 16] = jnp.zeros((NC, 8, UP), F32)

    outer = [
        jnp.concatenate(
            [hidden_rows(core, 0, SHARE), hidden_rows(core, TOK - SHARE, SHARE)], axis=0
        )
        for core in range(NC)
    ]
    edges = down_rows(outer, slice(0, D))
    p_send[:SHARE] = edges[:SHARE]
    p_send[TOK - SHARE :] = edges[SHARE:]
    for k, first, s in ((0, 0, 0), (1, ROWS - SHARE, 15)):

        @pl.when(2 * c + k != y)
        def _():
            along_y(k, first, SHARE).start()

        to, copy = along_x(jnp.int32(s))

        @pl.when(to != x)
        def _():
            copy.start()

    def own_part(k, first, count, cols):
        at = pl.multiple_of(k * ROWS + first, SHARE)
        return p_send[pl.ds(at, count), cols].astype(F32)

    landed(a_recv.at[pl.ds(0, NX - 1)], pr.at[0])
    total = jnp.concatenate([own_part(k, x * 32, 32, left_cols) for k in range(2)], axis=0)
    for j in range(1, NX):
        total += a_recv[lax.rem(x + j, NX)].astype(F32)
    a_send[...] = total.astype(BF16)

    def a_owner(k, core):
        at = (k * NC + core) * SHARE
        dev = (z, 2 * c + k, x, core)
        return push(a_send.at[pl.ds(at, SHARE)], fin.at[0, y], ps.at[2], pr.at[2], dev)

    for k in range(2):
        for core in range(NC):

            @pl.when((2 * c + k != y) | (c != core))
            def _():
                a_owner(k, core).start()

    def b_owner(j):
        t = lax.rem(tp + j, NT)
        at = pl.multiple_of(t * SHARE, SHARE)
        return push(b_send.at[pl.ds(at, SHARE)], fin.at[1, x], ps.at[3], pr.at[3], tp_peer(t))

    @pl.when(half == c)
    def _():
        landed(b_recv.at[pl.ds(0, NY - 1)], pr.at[1])
        total = own_part(yl, 0, ROWS, right_cols)
        for j in range(1, NY):
            total += b_recv[lax.rem(y + j, NY)].astype(F32)
        b_send[...] = total.astype(BF16)
        for j in range(1, NT):
            b_owner(j).start()
        fin[1, x] = b_send[pl.ds(pl.multiple_of(tp * SHARE, SHARE), SHARE)]
        fin[0, y] = a_send[pl.ds(pl.multiple_of((yl * NC + c) * SHARE, SHARE), SHARE)]

    for kind in range(2):

        @pl.when(half == c)
        def _():
            landed(fin.at[kind, pl.ds(0, 3)], pr.at[2 + kind])

        @pl.when(half != c)
        def _():
            landed(fin.at[kind], pr.at[2 + kind])

    sums = []
    for kind in range(2):
        part = fin[kind, 0].astype(F32)
        for k in range(1, 4):
            part += fin[kind, k].astype(F32)
        sums.append(part)
    projected = jnp.concatenate(sums, axis=1).astype(BF16).astype(F32)
    out[...] = (stream[...] + rms_norm(projected, in_one_row(gains.at[2]))).astype(BF16)

    left_here(kvbuf.at[pl.ds(0, 63 * SHARE)], kvs.at[0])
    left_here(qbuf.at[pl.ds(0, NT - 1)], qs.at[0])
    left_here(wbuf.at[0, pl.ds(0, 96)], wys.at[0])
    left_here(d_stage.at[pl.ds(0, 96)], wys.at[1])
    left_here(owbuf.at[0], ows.at[0])
    left_here(wbuf.at[0, pl.ds(0, 15 * ROWS)], wzs.at[0])
    left_here(dbuf.at[0, pl.ds(0, HID), pl.ds(0, 15 * ROWS)], wzs.at[1])
    left_here(wbuf.at[0], wps.at[0])
    left_here(dbuf.at[0, pl.ds(0, HID)], wps.at[1])
    left_here(stats.at[pl.ds(0, NT - 1)], sts.at[0])
    left_here(o_recv.at[pl.ds(0, NT - 1)], os_.at[0])
    left_here(r_recv.at[pl.ds(0, NX - 1)], rss.at[0])
    left_here(a_recv.at[pl.ds(0, NX - 1)], ps.at[0])
    both = up.at[:, pl.ds(0, 8)]
    left_here(both, hs.at[0])
    left_here(both, hs.at[1])

    @pl.when(half == c)
    def _():
        left_here(inbuf.at[pl.ds(0, 15 * SHARE)], ags.at[0])
        left_here(b_recv.at[0], ps.at[1])
        left_here(fin.at[0, pl.ds(0, 3)], ps.at[2])
        left_here(b_send.at[pl.ds(0, 7 * SHARE)], ps.at[3])

    @pl.when(half != c)
    def _():
        left_here(inbuf, ags.at[0])
        left_here(b_recv.at[pl.ds(0, 2)], ps.at[1])
        left_here(fin.at[0], ps.at[2])


def body(
    residual,
    query_nope,
    query_rope,
    latent,
    rope_key,
    kv_gain,
    key_up,
    value_up,
    out_weight,
    post_gain,
    pre_gain,
    ffn_gain,
    up_value,
    up_gate,
    conv_value,
    conv_gate,
    down_weight,
):
    scale = (query_nope.shape[2] + query_rope.shape[2]) ** (-0.5)
    by_row, by_col = turn_tables()

    dma = pltpu.SemaphoreType.DMA
    vmem = pltpu.VMEM
    return pl.pallas_call(
        functools.partial(layer_kernel, scale),
        out_shape=jax.ShapeDtypeStruct((SHARE, D), BF16),
        in_specs=[pl.BlockSpec(memory_space=pl.ANY)] * 19,
        out_specs=pl.BlockSpec(memory_space=vmem),
        scratch_shapes=[
            vmem((KEYS, KW), BF16),
            vmem((NT, ROWS, QW), BF16),
            vmem((NC, NZ * ROWS, UP), BF16),
            vmem((NC, 256, D), BF16),
            vmem((ROWS, 256), BF16),
            vmem((NC, 128, D), BF16),
            vmem((256, KEYS), BF16),
            vmem((KEYS, 1024), F32),
            vmem((8, 1024), F32),
            vmem((256, 1024), F32),
            vmem((NT, 8, 128), F32),
            vmem((NT, 8, 128), F32),
            vmem((NT, 128, 128), BF16),
            vmem((NT, 128, 128), BF16),
            vmem((64, D), BF16),
            vmem((NX, SHARE, D), BF16),
            vmem((SHARE, D), BF16),
            vmem((TOK, D), BF16),
            vmem((NC, TOK + 16, UP), F32),
            vmem((TOK, D), BF16),
            vmem((NX, 64, D // 2), BF16),
            vmem((NY, ROWS, D // 2), BF16),
            vmem((64, D // 2), BF16),
            vmem((ROWS, D // 2), BF16),
            vmem((2, 4, SHARE, D // 2), BF16),
            vmem((SHARE, D), F32),
            vmem((SHARE, 256), BF16),
            vmem((64, ROWS), BF16),
            vmem((ROWS, 128), BF16),
            vmem((64, ROWS), BF16),
            vmem((8, 128), F32),
            vmem((2, GRID, 128), F32),
            vmem(up_value.shape, BF16),
            vmem(up_gate.shape, BF16),
            vmem(down_weight.shape[::-1], BF16),
            vmem((256 * NT, 128), BF16),
            vmem((256 * NT, 128), BF16),
            vmem((SHARE, D), BF16),
            vmem((2, 128), BF16),
            vmem((3, D // 128, 128), BF16),
            vmem((2,) + conv_value.shape, BF16),
            vmem((2, ROWS, 128), F32),
            vmem((ROWS, 128), F32),
            vmem((NY, 32, UP), BF16),
            vmem((NY, 32, 256), BF16),
            vmem((256 * NT, 128), F32),
            vmem((NX * 256, KW), BF16),
            vmem((4, 256, 256), BF16),
            vmem((NC, 8, UP), F32),
        ]
        + [dma((n,)) for n in (19, 1, 1, 18, 1, 1, 2, 2, 2, 2)]
        + [dma((2, NZ))]
        + [dma((n,)) for n in (2, 1, 1, 1, 1, 1, 1, 1, 1, 1, 1, 2, 2, 4, 4)],
        compiler_params=pltpu.CompilerParams(
            collective_id=0, has_side_effects=True, vmem_limit_bytes=60 * 1024 * 1024
        ),
        name="layer",
    )(
        latent,
        rope_key.T,
        query_nope[:, 0],
        query_rope[:, 0].T,
        by_row,
        by_col,
        up_value,
        up_gate,
        down_weight.T,
        out_weight,
        key_up.reshape(-1, key_up.shape[2]),
        value_up.reshape(-1, value_up.shape[2]),
        residual,
        kv_gain.reshape(-1, 128),
        post_gain.reshape(-1, 128),
        pre_gain.reshape(-1, 128),
        ffn_gain.reshape(-1, 128),
        conv_value,
        conv_gate,
    )


def solution(mesh):
    torus = Mesh(mesh.devices.reshape(NZ, NY, NX, NC), AXES)
    return jax.shard_map(
        body,
        mesh=torus,
        in_specs=(
            P(SP, None),
            P(SP, TP, None),
            P(SP, TP, None),
            P(SP, None),
            P(SP, None),
            P(),
            P(),
            P(),
            P(TP, None),
            P(),
            P(),
            P(),
            P(SP, TP),
            P(SP, TP),
            P(),
            P(),
            P(TP, SP),
        ),
        out_specs=P(SP + TP, None),
        check_vma=False,
    )
```
